256 devices in a mesh: sp: 32 (over z, y), fs: 4 (over x), tp: 2 (over core).
Axes of the slice: x: 4, y: 4, z: 8, core: 2. Of those that a mesh axis runs over, the one named last changes fastest.
Arguments:
- tokens: bfloat16 [4, 4096, 2048], P('fs', ('sp', 'tp')), may hold values from -6 to 6
- norm_gain: float32 [2048], replicated, may hold values from 0.1 to 1.9
- drive_weight: bfloat16 [2048, 1024], P('fs', 'tp'), may hold values from -0.125 to 0.125
- query_weight: bfloat16 [2048, 1024], P('fs', 'tp'), may hold values from -1 to 1
- key_weight: bfloat16 [2048, 1024], P('fs', 'tp'), may hold values from -1 to 1
- value_weight: bfloat16 [2048, 1024], P('fs', 'tp'), may hold values from -0.5 to 0.5
- key_offset: bfloat16 [8, 4, 4096], P('tp', 'fs', 'sp'), may hold values from -16 to 0
- log_step: float32 [64], P('tp'), may hold values from -4.7 to -1.2
- lambda_real: float32 [64, 64], P('tp'), as said below
- lambda_imag: float32 [64, 64], P('tp'), may hold values from 1 to 201
- input_map: float32 [2, 64, 64, 16], P(None, 'tp'), may hold values from -2 to 2
- output_map: float32 [2, 64, 16, 64], P(None, 'tp'), may hold values from -0.5 to 0.5
- skip_gain: float32 [1024], P('tp'), may hold values from -5 to 5
- forget: float32 [64, 4, 4096], P('tp', 'fs', 'sp'), may hold values from -0.52 to 0
- initial_state: float32 [2, 4, 64, 64], P(None, 'fs', 'tp'), may hold values from -24 to 24
- scan_out_weight: bfloat16 [1024, 2048], P('tp', 'fs'), may hold values from -0.125 to 0.125
- attend_out_weight: bfloat16 [1024, 2048], P('tp', 'fs'), may hold values from -0.125 to 0.125
Outputs:
- layer_out: bfloat16 [4, 4096, 2048], P('fs', ('sp', 'tp'))
The draws below stay inside these ranges and needn't reach their ends.
Inputs may be any that keep to these rules, and one draw needn't show every extreme that they name: lambda_real[g, n] * exp(log_step[g]) lies between -1/30 and 0 for every group g and state n.
All inputs are finite; a program needn't handle non-finite values.
Results may differ from the reference program's by a relative error of at most 0.009.
Values may be sent and summed in bfloat16 or wider, within the bound.
A program may use at most 128 MiB of HBM per device.

```python
import math
import jax
import jax.numpy as jnp
from jax import lax

D = 2048
BRANCH_W = 1024
HEAD_DIM = 128
HEADS = 8
GROUP_W = 16
GROUPS = 64
STATE_N = 64
TOK_DEV = 128
LENGTH = 4096
SEQUENCE_COUNT = 4
N_TP = 2


def spike_mask(key, leading_part, item_count):
    spots = jax.random.randint(key, leading_part + (item_count,), 0, LENGTH)
    places = jnp.arange(LENGTH, dtype=jnp.int32)
    return jnp.any(places[None, None, :, None] == spots[:, :, None, :], axis=-1)


def draw_tokens(key, part):
    key_sequence = jax.random.split(jax.random.fold_in(key, 11), 4)
    full_shape = (SEQUENCE_COUNT, LENGTH, D)
    noise = jnp.clip(jax.random.normal(key_sequence[0], full_shape, jnp.float32), -4.0, 4.0)
    direction = jnp.where(jax.random.bernoulli(key_sequence[1], 0.5, (SEQUENCE_COUNT, 1, D)), 1.0, -1.0)
    row_sign = jnp.where(jax.random.bernoulli(key_sequence[2], 0.5, (SEQUENCE_COUNT, LENGTH, 1)), 1.0, -1.0)
    block_total = LENGTH // TOK_DEV
    amplitude = jnp.exp(jax.random.uniform(key_sequence[3], (SEQUENCE_COUNT, block_total, 1), jnp.float32, math.log(0.15), math.log(2.0)))
    amplitude = jnp.repeat(amplitude, TOK_DEV, axis=1)
    return (noise + row_sign * amplitude * direction).astype(jnp.bfloat16)


def paired_weights(key):
    key_sequence = jax.random.split(jax.random.fold_in(key, 13), 2)
    first = jnp.clip(jax.random.normal(key_sequence[0], (D, BRANCH_W), jnp.float32), -6.0, 6.0) * D ** (-0.5)
    second = jnp.clip(jax.random.normal(key_sequence[1], (D, BRANCH_W), jnp.float32), -6.0, 6.0) * D ** (-0.5)
    return (first, 0.35 * first + 0.93675 * second)


def draw_query_weight(key, part):
    return paired_weights(key)[0].astype(jnp.bfloat16)


def draw_key_weight(key, part):
    return paired_weights(key)[1].astype(jnp.bfloat16)


def draw_key_offset(key, part):
    head_number = BRANCH_W // HEAD_DIM
    key_sequence = jax.random.split(jax.random.fold_in(key, 7), 7)
    fast_count = head_number // 2
    fast = jax.random.permutation(key_sequence[0], head_number) < fast_count
    quick_rate = jnp.exp(jax.random.uniform(key_sequence[1], (head_number,), jnp.float32, math.log(0.001), math.log(1.0 / 30.0)))
    slow_rate = jnp.exp(jax.random.uniform(key_sequence[2], (head_number,), jnp.float32, math.log(0.1), math.log(0.6))) / LENGTH
    ground_level = jnp.log(jnp.where(fast, quick_rate, slow_rate)) - 0.5
    block_total = LENGTH // TOK_DEV
    block_multiplier = jax.random.uniform(key_sequence[3], (head_number, SEQUENCE_COUNT, block_total), jnp.float32, math.log(0.5), math.log(2.0))
    block_multiplier = jnp.repeat(block_multiplier, TOK_DEV, axis=2)
    random_shake = jax.random.uniform(key_sequence[4], (head_number, SEQUENCE_COUNT, LENGTH), jnp.float32, -0.7, 0.7)
    struck_mask = spike_mask(key_sequence[5], (head_number, SEQUENCE_COUNT), 3)
    share_fraction = jax.random.uniform(key_sequence[6], (head_number, SEQUENCE_COUNT, LENGTH), jnp.float32, 0.2, 0.4)
    spike_level = jnp.log(share_fraction / (1.0 - share_fraction))
    value_gathered_full = jnp.where(struck_mask, spike_level, ground_level[:, None, None] + block_multiplier + random_shake)
    return value_gathered_full.astype(jnp.bfloat16)


def decay_pair(key):
    group_count_total = BRANCH_W // GROUP_W
    key_sequence = jax.random.split(jax.random.fold_in(key, 3), 4)
    log_steps = jax.random.uniform(key_sequence[0], (group_count_total,), jnp.float32, math.log(0.01), math.log(0.3))
    fast_count = group_count_total // 2
    fast = jax.random.permutation(key_sequence[1], group_count_total) < fast_count
    quick_rate = jnp.exp(jax.random.uniform(key_sequence[2], (group_count_total, STATE_N), jnp.float32, math.log(0.001), math.log(1.0 / 30.0)))
    slow_rate = jnp.exp(jax.random.uniform(key_sequence[3], (group_count_total, STATE_N), jnp.float32, math.log(0.05), math.log(0.4))) / LENGTH
    rate_all = jnp.where(fast[:, None], quick_rate, slow_rate)
    return (log_steps, -rate_all / jnp.exp(log_steps)[:, None])


def draw_log_step(key, part):
    return decay_pair(key)[0]


def draw_lambda_real(key, part):
    return decay_pair(key)[1]


def draw_forget(key, part):
    group_count_total = BRANCH_W // GROUP_W
    key_sequence = jax.random.split(jax.random.fold_in(key, 5), 4)
    base_rate = jax.random.uniform(key_sequence[0], (group_count_total, SEQUENCE_COUNT, LENGTH), jnp.float32, 0.05, 0.5) / LENGTH
    block_total = LENGTH // TOK_DEV
    block_multiplier = jnp.exp(jax.random.uniform(key_sequence[1], (group_count_total, SEQUENCE_COUNT, block_total), jnp.float32, math.log(0.5), math.log(2.0)))
    block_multiplier = jnp.repeat(block_multiplier, TOK_DEV, axis=2)
    struck_mask = spike_mask(key_sequence[2], (group_count_total, SEQUENCE_COUNT), 2)
    share_fraction = jax.random.uniform(key_sequence[3], (group_count_total, SEQUENCE_COUNT, LENGTH), jnp.float32, 0.2, 0.4)
    return jnp.where(struck_mask, jnp.log1p(-share_fraction), -base_rate * block_multiplier)


def block_scale(stream_key, extent, pieces, low, largest):
    def one(axis_at, blocks):
        draws = jax.random.uniform(jax.random.fold_in(jax.random.fold_in(stream_key, 6), axis_at), (blocks,), jnp.float32, low / len(pieces), largest / len(pieces))
        return jnp.repeat(jnp.exp(draws), extent[axis_at] // blocks).reshape((-1,) + (1,) * (len(extent) - axis_at - 1))

    level = one(*pieces[0])
    for cut in pieces[1:]:
        level = level * one(*cut)
    return level


def scatter_about(key, dims, spread, bound, cuts=(), kind=jnp.bfloat16):
    level = block_scale(key, dims, cuts, -0.22, 0.18) if cuts else 1.0
    array = jax.random.normal(key, dims, jnp.float32) * spread * level
    return jnp.minimum(jnp.maximum(array, -bound), bound).astype(kind)


def setup_inputs(seed: int = 0) -> dict:
    arg_keys = jax.random.split(jax.random.key(seed), 18)
    return {
        "tokens": draw_tokens(jax.random.fold_in(arg_keys[17], 71), 0),
        "norm_gain": jnp.clip(1.0 + 0.18 * jax.random.normal(arg_keys[1], (D,), jnp.float32), 0.1, 1.9),
        "drive_weight": scatter_about(arg_keys[2], (D, BRANCH_W), D ** -0.5, 0.125, ((0, 4), (1, 2))),
        "query_weight": draw_query_weight(jax.random.fold_in(arg_keys[17], 71), 0),
        "key_weight": draw_key_weight(jax.random.fold_in(arg_keys[17], 71), 0),
        "value_weight": scatter_about(arg_keys[5], (D, BRANCH_W), (D // 16) ** -0.5, 0.5, ((0, 4), (1, 2))),
        "key_offset": draw_key_offset(jax.random.fold_in(arg_keys[17], 71), 0),
        "log_step": draw_log_step(jax.random.fold_in(arg_keys[17], 71), 0),
        "lambda_real": draw_lambda_real(jax.random.fold_in(arg_keys[17], 71), 0),
        "lambda_imag": jnp.clip(1.0 + 200.0 * jax.random.uniform(arg_keys[9], (GROUPS, STATE_N), jnp.float32) ** block_scale(arg_keys[9], (GROUPS, STATE_N), ((0, 2),), -0.2, 0.2), 1.0, 201.0),
        "input_map": scatter_about(arg_keys[10], (2, GROUPS, STATE_N, GROUP_W), (GROUP_W // 2) ** -0.5, 2.0, ((1, 2),), jnp.float32),
        "output_map": scatter_about(arg_keys[11], (2, GROUPS, GROUP_W, STATE_N), (2 * STATE_N) ** -0.5, 0.5, ((1, 2),), jnp.float32),
        "skip_gain": scatter_about(arg_keys[12], (BRANCH_W,), 1.0, 5.0, ((0, 2),), jnp.float32),
        "forget": draw_forget(jax.random.fold_in(arg_keys[17], 71), 0),
        "initial_state": scatter_about(arg_keys[14], (2, SEQUENCE_COUNT, GROUPS, STATE_N), 4.0, 24.0, ((1, 4), (2, 2)), jnp.float32),
        "scan_out_weight": scatter_about(arg_keys[15], (BRANCH_W, D), (2 * BRANCH_W) ** -0.5, 0.125, ((0, 2), (1, 4))),
        "attend_out_weight": scatter_about(arg_keys[16], (BRANCH_W, D), (2 * BRANCH_W) ** -0.5, 0.125, ((0, 2), (1, 4))),
    }


epsilon = 1e-06

def reference(tokens, norm_gain, drive_weight, query_weight, key_weight, value_weight, key_offset, log_step, lambda_real, lambda_imag, input_map, output_map, skip_gain, forget, initial_state, scan_out_weight, attend_out_weight):
    highest = lax.Precision.HIGHEST
    flat_rows = tokens.reshape(SEQUENCE_COUNT * LENGTH, D).astype(jnp.float32)
    normed = (flat_rows * lax.rsqrt(lax.optimization_barrier(jnp.mean(flat_rows * flat_rows, axis=1, keepdims=True)) + epsilon) * norm_gain[None]).astype(jnp.bfloat16)

    def project(matrix):
        return jnp.dot(normed, matrix, preferred_element_type=jnp.float32).astype(jnp.bfloat16)
    drive_rows = project(drive_weight)
    queries = project(query_weight)
    keys_all = project(key_weight)
    values_all = project(value_weight)
    step_size = jnp.exp(log_step)[:, None]
    log_gain = lambda_real * step_size
    rotate = lambda_imag * step_size
    magnitude = jnp.exp(log_gain)
    bar_real = magnitude * jnp.cos(rotate)
    bar_imag = magnitude * jnp.sin(rotate)
    divisor = lambda_real * lambda_real + lambda_imag * lambda_imag
    shifted = bar_real - 1.0
    factor_real = (shifted * lambda_real + bar_imag * lambda_imag) / divisor
    factor_imag = (bar_imag * lambda_real - shifted * lambda_imag) / divisor
    map_real = factor_real[:, :, None] * input_map[0] - factor_imag[:, :, None] * input_map[1]
    map_imag = factor_real[:, :, None] * input_map[1] + factor_imag[:, :, None] * input_map[0]
    inputs = drive_rows.astype(jnp.float32).reshape(SEQUENCE_COUNT, LENGTH, GROUPS, GROUP_W)

    def one_sequence(element):
        seq_inputs, seq_forget, seq_init = element

        def advance(running, item_pair):
            in_now, forget_now = item_pair
            keep_rate = jnp.exp(forget_now)[:, None]
            new_real = keep_rate * (bar_real * running[0] - bar_imag * running[1]) + jnp.einsum('gc,gnc->gn', in_now, map_real, precision=highest)
            new_imag = keep_rate * (bar_real * running[1] + bar_imag * running[0]) + jnp.einsum('gc,gnc->gn', in_now, map_imag, precision=highest)
            readout = jnp.einsum('gn,gcn->gc', new_real, output_map[0], precision=highest) - jnp.einsum('gn,gcn->gc', new_imag, output_map[1], precision=highest)
            return ((new_real, new_imag), readout)
        _, read_rows = lax.scan(advance, (seq_init[0], seq_init[1]), (seq_inputs, seq_forget.T))
        return read_rows
    readouts = lax.map(one_sequence, (inputs, jnp.transpose(forget, (1, 0, 2)), jnp.transpose(initial_state, (1, 0, 2, 3))))
    readouts = readouts + skip_gain.reshape(GROUPS, GROUP_W)[None, None] * inputs
    scan_out = jax.nn.gelu(readouts).reshape(SEQUENCE_COUNT * LENGTH, BRANCH_W).astype(jnp.bfloat16)
    blocks = LENGTH // TOK_DEV
    shape_five = (SEQUENCE_COUNT, blocks, TOK_DEV, HEADS, HEAD_DIM)
    query_five = queries.reshape(shape_five)
    key_five = keys_all.reshape(shape_five)
    value_five = values_all.reshape(shape_five)
    offset_four = key_offset.reshape(HEADS, SEQUENCE_COUNT, blocks, TOK_DEV)
    ladder = jnp.arange(TOK_DEV, dtype=jnp.int32)

    def one_block(item_index):
        seq_id = item_index // blocks
        block_id = item_index % blocks
        query_block = query_five[seq_id, block_id].astype(jnp.float32)
        query_place = block_id * TOK_DEV + ladder

        def turn(distance, running):
            summed_now, fallen = running
            source = block_id - distance
            key_block = key_five[seq_id, source].astype(jnp.float32)
            value_block = value_five[seq_id, source].astype(jnp.float32)
            offset_block = offset_four[:, seq_id, source].astype(jnp.float32)
            scores = jnp.einsum('qhd,khd->qhk', query_block, key_block) * HEAD_DIM ** (-0.5) + offset_block[None]
            key_place = source * TOK_DEV + ladder
            visible = key_place[None, None, :] < query_place[:, None, None]
            escape_log = jnp.where(visible, jax.nn.log_sigmoid(-scores), 0.0)
            behind_log = lax.cumsum(escape_log, axis=2, reverse=True) - escape_log
            weight = jnp.where(visible, jnp.exp(jax.nn.log_sigmoid(scores) + behind_log), 0.0)
            weight = lax.optimization_barrier(weight.astype(jnp.bfloat16)).astype(jnp.float32)
            portion = jnp.einsum('qhk,khd->qhd', weight, value_block)
            return (summed_now + jnp.exp(fallen)[:, :, None] * portion, fallen + lax.optimization_barrier(jnp.sum(escape_log, axis=2)))
        empty_state = (jnp.zeros((TOK_DEV, HEADS, HEAD_DIM), jnp.float32), jnp.zeros((TOK_DEV, HEADS), jnp.float32))
        result_now, _ = lax.fori_loop(0, block_id + 1, turn, empty_state)
        return result_now.astype(jnp.bfloat16)
    attended = lax.map(one_block, jnp.arange(SEQUENCE_COUNT * blocks, dtype=jnp.int32))
    attend_out = attended.reshape(SEQUENCE_COUNT * LENGTH, BRANCH_W)
    share_width = BRANCH_W // N_TP
    summed = jnp.zeros((SEQUENCE_COUNT * LENGTH, D), jnp.float32)
    for part_index in range(N_TP):
        column_low = part_index * share_width
        column_high = column_low + share_width
        partial_value = jnp.dot(scan_out[:, column_low:column_high], scan_out_weight[column_low:column_high], preferred_element_type=jnp.float32)
        partial_value = partial_value + jnp.dot(attend_out[:, column_low:column_high], attend_out_weight[column_low:column_high], preferred_element_type=jnp.float32)
        rounded = lax.optimization_barrier(partial_value.astype(jnp.bfloat16))
        summed = summed + rounded.astype(jnp.float32)
    return summed.astype(jnp.bfloat16).reshape(SEQUENCE_COUNT, LENGTH, D)
```

```python
import math

import jax
import jax.numpy as jnp
from jax import lax
from jax.experimental import pallas as pl
from jax.experimental.pallas import tpu as pltpu
from jax.sharding import Mesh
from jax.sharding import PartitionSpec as P

SP_TP = ("sp_0", "sp_1", "tp")
SP = ("sp_0", "sp_1")
EPSILON = 1e-06
LOG2E = 1.4426950408889634
NZ, NY, NX, NT = 8, 4, 4, 2
BF16, F32 = jnp.bfloat16, jnp.float32
VMEM = pl.BlockSpec(memory_space=pltpu.VMEM)
MESH_ID = pl.DeviceIdType.MESH


def remote(src, dst, send_sem, recv_sem, where):
    return pltpu.make_async_remote_copy(
        src_ref=src, dst_ref=dst, send_sem=send_sem, recv_sem=recv_sem,
        device_id=where, device_id_type=MESH_ID,
    )


def greet(peers):
    barrier = pltpu.get_barrier_semaphore()
    for peer in peers:
        pl.semaphore_signal(barrier, inc=1, device_id=peer, device_id_type=MESH_ID)


def await_greetings(count):
    pl.semaphore_wait(pltpu.get_barrier_semaphore(), count)


def plane_peers(x, y, t):
    peers = [
        {"fs": (x + dx) % NX, "tp": (t + dt) % NT}
        for dx in range(NX) for dt in range(NT) if (dx, dt) != (0, 0)
    ]
    peers += [
        {"fs": (x + dx) % NX, "sp_1": (y + dy) % NY} for dx in range(NX) for dy in range(1, NY)
    ]
    return peers


def high_low(value):
    high = value.astype(BF16)
    return high, (value - high.astype(F32)).astype(BF16)


def project_kernel(
    tok, gain, w_drive, w_query, w_key, w_value, packed,
    proj, packed_out,
    normed, rows_in, part_out, part_in, packed_in,
    s_rows, r_rows, s_part, r_part, s_packed, r_packed,
):
    y, x, t = (lax.axis_index(a) for a in ("sp_1", "fs", "tp"))
    greet(plane_peers(x, y, t))
    values = tok[...].astype(F32)
    scale = lax.rsqrt(jnp.mean(values * values, axis=1, keepdims=True) + EPSILON)
    rounded = (values * scale * gain[...]).astype(BF16)
    width = rounded.shape[1] // NX
    for k in range(NX):
        normed[k] = rounded[:, k * width : (k + 1) * width]
    half = rounded.shape[0]
    mine = pl.ds(pl.multiple_of(t * half, half), half)
    rows_in[x, mine, :] = normed[x]
    packed_in[y] = packed[y]
    await_greetings(19)
    row_copies = {}
    for dx in (1, 3, 2, 0):
        for dt in range(NT):
            if (dx, dt) != (0, 0):
                to = (x + dx) % NX
                row_copies[dx, dt] = remote(
                    normed.at[to], rows_in.at[x, mine], s_rows.at[dx, dt], r_rows.at[dx, dt],
                    {"fs": to, "tp": (t + dt) % NT},
                )
                row_copies[dx, dt].start()
    packed_copies = []
    for dy in range(1, NY):
        to = (y + dy) % NY
        copy = remote(
            packed.at[to], packed_in.at[y], s_packed.at[dy], r_packed.at[dy], {"sp_1": to}
        )
        copy.start()
        packed_copies.append(copy)
    part_copies = {}
    for dx in (0, 1, 3, 2):
        seq = (x + NX - dx) % NX
        for dt in range(NT):
            if (dx, dt) != (0, 0):
                row_copies[dx, dt].wait_recv()
        rows = rows_in[seq]
        for kind, weight in enumerate((w_drive, w_query, w_key, w_value)):
            product = jnp.dot(rows, weight[...], preferred_element_type=F32).astype(BF16)
            for k in range(NY):
                part_out[dx, k, kind] = product[:, k * 128 : (k + 1) * 128]
        for dy in (1, 3, 2, 0):
            if (dx, dy) != (0, 0):
                to = (y + dy) % NY
                part_copies[dx, dy] = remote(
                    part_out.at[dx, to], part_in.at[dx, dy], s_part.at[dx, dy], r_part.at[dx, dy],
                    {"fs": seq, "sp_1": to},
                )
                part_copies[dx, dy].start()
    part_in[0, 0] = part_out[0, y]
    for copy in packed_copies:
        copy.wait()
    packed_out[...] = packed_in[...]
    for dy in range(NY):
        for dx in range(NX):
            if (dx, dy) != (0, 0):
                part_copies[dx, dy].wait_recv()
        block = (y + NY - dy) % NY
        for kind in range(4):
            total = part_in[0, dy, kind].astype(F32)
            for dx in range(1, NX):
                total = total + part_in[dx, dy, kind].astype(F32)
            proj[kind, block] = total.astype(BF16)
    for copy in row_copies.values():
        copy.wait_send()
    for copy in part_copies.values():
        copy.wait_send()


def project(tok, gain, weights, packed):
    return pl.pallas_call(
        project_kernel,
        out_shape=(
            jax.ShapeDtypeStruct((4, NY, 128, 128), BF16),
            jax.ShapeDtypeStruct((NY, 16, 128), F32),
        ),
        in_specs=[VMEM] * 7,
        out_specs=(VMEM, VMEM),
        scratch_shapes=[
            pltpu.VMEM((NX, 64, 512), BF16),
            pltpu.VMEM((NX, 128, 512), BF16),
            pltpu.VMEM((NX, NY, 4, 128, 128), BF16),
            pltpu.VMEM((NX, NY, 4, 128, 128), BF16),
            pltpu.VMEM((NY, 16, 128), F32),
            pltpu.SemaphoreType.DMA((NX, NT)),
            pltpu.SemaphoreType.DMA((NX, NT)),
            pltpu.SemaphoreType.DMA((NX, NY)),
            pltpu.SemaphoreType.DMA((NX, NY)),
            pltpu.SemaphoreType.DMA((NY,)),
            pltpu.SemaphoreType.DMA((NY,)),
        ],
        compiler_params=pltpu.CompilerParams(
            collective_id=0, has_side_effects=True, vmem_limit_bytes=40 << 20
        ),
        name="project",
    )(tok, gain, *weights, packed)


def attend_pair(query, key, value, offset, fallen, ladder, visible):
    score = lax.dot_general(query, key, (((1,), (1,)), ((), ())), preferred_element_type=F32)
    score = score * (LOG2E * 128**-0.5) + offset
    soft = jnp.maximum(score, 0.0) + LOG2E * jnp.log(1.0 + jnp.exp2(-jnp.abs(score)))
    if visible is not None:
        soft = jnp.where(visible, soft, 0.0)
    sums = jnp.dot(
        jnp.concatenate(high_low(soft), axis=1), ladder, preferred_element_type=F32
    )
    behind = sums[:, :128] if fallen is None else sums[:, :128] + fallen
    weight = jnp.exp2(score + behind)
    if visible is not None:
        weight = jnp.where(visible, weight, 0.0)
    portion = jnp.dot(weight.astype(BF16), value, preferred_element_type=F32)
    total = sums[:, 128:] if fallen is None else sums[:, 128:] + fallen
    return portion, total


def turned(gain, state):
    return gain[0] * state + gain[1] * pltpu.roll(state, 64, 1)


def powers_times(left, right):
    return (
        left[0] * right[0] - left[1] * right[1],
        left[1] * right[0] + left[0] * right[1],
    )


def mix_kernel(
    proj, packed, params, maps,
    attend_out, scan_out,
    right_in, left_in, offset_own, offset_in, state_own, state_in, acc, tot, ladder,
    into_map, out_map, fwd_p, fwd_q, inv_p, inv_q, held, ends, decay,
    s_right, r_right, s_left, r_left, s_offset, r_offset, s_state, r_state,
):
    z, y = lax.axis_index("sp_0"), lax.axis_index("sp_1")
    greet([{"sp_0": (z + dz) % NZ} for dz in range(1, NZ)])
    up, down = {"sp_0": (z + 1) % NZ}, {"sp_0": (z + NZ - 1) % NZ}
    for b in range(NY):
        offset_own[b : b + 1, :] = packed[b, 8:9, :]
        offset_in[0, b : b + 1, :] = packed[b, 8:9, :]
    offset_own[4:8, :] = jnp.zeros((4, 128), F32)
    await_greetings(NZ - 1)
    copies = []

    def send(src, dst, s_sem, r_sem, where):
        copy = remote(src, dst, s_sem, r_sem, where)
        copy.start()
        copies.append(copy)
        return copy

    right, left = {}, {}
    for part in range(2):
        right[1, part] = send(
            proj.at[2 + part], right_in.at[0, part], s_right.at[0, part], r_right.at[0, part], up
        )
        left[1, part] = send(
            proj.at[2 + part], left_in.at[0, part], s_left.at[0, part], r_left.at[0, part], down
        )
    offset_copies = [
        send(
            offset_own, offset_in.at[dz], s_offset.at[dz], r_offset.at[dz], {"sp_0": (z + dz) % NZ}
        )
        for dz in range(1, NZ)
    ]

    row = lax.broadcasted_iota(jnp.int32, (128, 128), 0)
    lane = lax.broadcasted_iota(jnp.int32, (128, 128), 1)

    sign = jnp.where(lane[:8] < 64, -1.0, 1.0)
    lam_real, lam_imag, log_step, initial, skip = (params[y, k] for k in range(5))
    step = jnp.exp(log_step)
    log_gain, rotate = lam_real * step, lam_imag * step
    cosine, sine, magnitude = jnp.cos(rotate), jnp.sin(rotate), jnp.exp(log_gain)
    bar_real, bar_imag = magnitude * cosine, magnitude * sine
    divisor = lam_real * lam_real + lam_imag * lam_imag
    shifted = bar_real - 1.0
    factor_real = (shifted * lam_real + bar_imag * lam_imag) / divisor
    factor_imag = (bar_imag * lam_real - shifted * lam_imag) / divisor * sign
    shrink = jnp.exp(-log_gain)
    gain = (bar_real, sign * bar_imag)
    inverse = (shrink * cosine, -sign * shrink * sine)
    gains, inverses = [gain], [inverse]
    for _ in range(9):
        gains.append(powers_times(gains[-1], gains[-1]))
    for _ in range(6):
        inverses.append(powers_times(inverses[-1], inverses[-1]))
    gain_block, gain_all = gains[7], gains[9]
    gain_last = powers_times(gain_block, inverse)
    into_map[...] = jnp.zeros_like(into_map)
    out_map[...] = jnp.zeros_like(out_map)
    for g in range(8):
        cols, swapped = pl.ds(g * 128, 128), pl.ds(1024 + g * 128, 128)
        raw = maps[y, 0, g]
        entry = factor_real[g : g + 1] * raw + factor_imag[g : g + 1] * pltpu.roll(raw, 64, 1)
        other = pltpu.roll(entry, 64, 1)
        for at in (g * 16, 128 + g * 16):
            into_map[at : at + 16, cols] = entry.astype(BF16)
            into_map[at : at + 16, swapped] = other.astype(BF16)
        raw = maps[y, 1, g]
        out_map[g * 16 : g * 16 + 16, cols] = (raw * -sign[:1]).astype(BF16)
        out_map[g * 16 : g * 16 + 16, swapped] = (pltpu.roll(raw, 64, 1) * -sign[:1]).astype(BF16)
        for table_p, table_q, steps in ((fwd_p, fwd_q, gains), (inv_p, inv_q, inverses)):
            real, imag = jnp.ones((8, 128), F32), jnp.zeros((8, 128), F32)
            for bit in range(3):
                by = tuple(part[g : g + 1] for part in steps[bit])
                new = powers_times((real, imag), by)
                chosen = (row[:8] & (1 << bit)) != 0
                real, imag = jnp.where(chosen, new[0], real), jnp.where(chosen, new[1], imag)
            table_p[:8, cols] = real
            table_q[:8, cols] = imag
            for bit in range(3, 7):
                n = 1 << bit
                by = tuple(part[g : g + 1] for part in steps[bit])
                new = powers_times((table_p[:n, cols], table_q[:n, cols]), by)
                table_p[n : 2 * n, cols] = new[0]
                table_q[n : 2 * n, cols] = new[1]
    until = jnp.where(lane <= row, 1.0, 0.0)
    until_half = until.astype(BF16)
    falls = []
    local = jnp.zeros((8, 128), F32)
    fall_all = jnp.zeros((8, 1), F32)
    for b in range(NY):
        forget = packed[b, :8, :]
        spread = jnp.concatenate(
            [jnp.broadcast_to(forget[g : g + 1], (16, 128)) for g in range(8)], axis=0
        )
        fall = lax.dot_general(
            until, spread, (((1,), (1,)), ((), ())), preferred_element_type=F32,
            precision=lax.Precision.HIGHEST,
        )
        decay[b] = fall
        driven = proj[0, b].astype(F32) * jnp.exp(-fall)
        entered = jnp.dot(
            jnp.concatenate(high_low(driven), axis=1), into_map[...], preferred_element_type=F32
        )
        unturned = entered[:, :1024] * inv_p[...] + entered[:, 1024:] * inv_q[...]
        high, low = high_low(unturned)
        held[b] = jnp.dot(until_half, high, preferred_element_type=F32) + jnp.dot(
            until_half, low, preferred_element_type=F32
        )
        for g in range(8):
            ends[b, g : g + 1, :] = held[b, 127:128, g * 128 : (g + 1) * 128]
        total = jnp.sum(forget, axis=1, keepdims=True)
        falls.append(jnp.exp(total))
        fall_all = fall_all + total
        ends[b] = falls[b] * turned(gain_last, ends[b])
        local = falls[b] * turned(gain_block, local) + ends[b]
    state_own[:8, :] = local
    state_own[8:, :] = jnp.broadcast_to(fall_all, (8, 128))
    state_copies = [
        send(
            state_own, state_in.at[dz], s_state.at[dz], r_state.at[dz], {"sp_0": (z + dz) % NZ}
        )
        for dz in range(1, NZ)
    ]

    ladder_row = lax.broadcasted_iota(jnp.int32, (256, 256), 0) % 128
    ladder_lane = lax.broadcasted_iota(jnp.int32, (256, 256), 1)
    ladder[...] = jnp.where((ladder_lane >= 128) | (ladder_row >= ladder_lane), -1.0, 0.0).astype(
        BF16
    )
    for q in range(NY):
        portion_sum, fallen = None, None
        for k in range(q, -1, -1):
            portion, fallen = attend_pair(
                proj[1, q], proj[2, k], proj[3, k], offset_in[0, k : k + 1, :], fallen,
                ladder[...], lane < row if k == q else None,
            )
            portion_sum = portion if portion_sum is None else portion_sum + portion
        acc[0, q] = portion_sum
        tot[0, q] = fallen

    for copy in offset_copies:
        copy.wait_recv()

    def attend_chunk(dz, key_at, value_at):
        @pl.when(z >= dz)
        def _():
            for q in range(NY):
                acc[dz, q] = jnp.zeros((128, 128), F32)
                tot[dz, q] = jnp.zeros((128, 128), F32)

            def one(turn, carry):
                k = NY - 1 - turn
                key, value = key_at(k), value_at(k)
                offset = offset_in[dz, pl.ds(k, 1), :]
                for q in range(NY):
                    portion, fallen = attend_pair(
                        proj[1, q], key, value, offset, tot[dz, q], ladder[...], None
                    )
                    acc[dz, q] += portion
                    tot[dz, q] = fallen
                return carry

            lax.fori_loop(0, NY, one, 0)

    for i in range(1, 4):
        for part in range(2):
            right[i, part].wait_recv()
            if i < 3 or part == 0:
                right[i + 1, part] = send(
                    right_in.at[i - 1, part], right_in.at[i, part],
                    s_right.at[i, part], r_right.at[i, part], up,
                )
            left[i, part].wait_recv()
            if i < 3 or part == 1:
                left[i + 1, part] = send(
                    left_in.at[i - 1, part], left_in.at[i, part],
                    s_left.at[i, part], r_left.at[i, part], down,
                )
        attend_chunk(i, lambda k: right_in[i - 1, 0, k], lambda k: right_in[i - 1, 1, k])
        attend_chunk(8 - i, lambda k: left_in[i - 1, 0, k], lambda k: left_in[i - 1, 1, k])
    right[4, 0].wait_recv()
    left[4, 1].wait_recv()
    attend_chunk(4, lambda k: right_in[3, 0, k], lambda k: left_in[3, 1, k])
    for dz in range(1, NZ):
        @pl.when(z >= dz)
        def _():
            for q in range(NY):
                fallen = tot[0, q]
                acc[0, q] += jnp.exp2(fallen) * acc[dz, q]
                tot[0, q] = fallen + tot[dz, q]

    for q in range(NY):
        attend_out[q] = acc[0, q].astype(BF16)

    for copy in state_copies:
        copy.wait_recv()
    carry = initial
    for source in range(NZ - 1):
        back = jnp.maximum(z - source, 1)
        arrived = state_in[back]
        moved = jnp.exp(arrived[8:]) * turned(gain_all, carry) + arrived[:8]
        carry = jnp.where(source < z, moved, carry)
    for b in range(NY):
        entering = turned(gain, carry)
        whole = jnp.concatenate(
            [
                held[b, :, g * 128 : (g + 1) * 128] + entering[g : g + 1]
                for g in range(8)
            ],
            axis=1,
        )
        turned_states = jnp.concatenate(
            [(whole * fwd_p[...]).astype(BF16), (whole * fwd_q[...]).astype(BF16)], axis=1
        )
        read = lax.dot_general(
            turned_states, out_map[...], (((1,), (1,)), ((), ())), preferred_element_type=F32
        )
        read = read * jnp.exp(decay[b]) + skip[:1] * proj[0, b].astype(F32)
        inner = math.sqrt(2.0 / math.pi) * (read + 0.044715 * (read * read * read))
        scan_out[b] = (0.5 * read * (1.0 + jnp.tanh(inner))).astype(BF16)
        carry = falls[b] * turned(gain_block, carry) + ends[b]
    for copy in copies:
        copy.wait_send()


def mix(proj, packed, params, maps):
    return pl.pallas_call(
        mix_kernel,
        out_shape=(
            jax.ShapeDtypeStruct((NY, 128, 128), BF16),
            jax.ShapeDtypeStruct((NY, 128, 128), BF16),
        ),
        in_specs=[VMEM] * 4,
        out_specs=(VMEM, VMEM),
        scratch_shapes=[
            pltpu.VMEM((4, 2, NY, 128, 128), BF16),
            pltpu.VMEM((4, 2, NY, 128, 128), BF16),
            pltpu.VMEM((8, 128), F32),
            pltpu.VMEM((NZ, 8, 128), F32),
            pltpu.VMEM((16, 128), F32),
            pltpu.VMEM((NZ, 16, 128), F32),
            pltpu.VMEM((NZ, NY, 128, 128), F32),
            pltpu.VMEM((NZ, NY, 128, 128), F32),
            pltpu.VMEM((256, 256), BF16),
            pltpu.VMEM((256, 2048), BF16),
            pltpu.VMEM((128, 2048), BF16),
            pltpu.VMEM((128, 1024), F32),
            pltpu.VMEM((128, 1024), F32),
            pltpu.VMEM((128, 1024), F32),
            pltpu.VMEM((128, 1024), F32),
            pltpu.VMEM((NY, 128, 1024), F32),
            pltpu.VMEM((NY, 8, 128), F32),
            pltpu.VMEM((NY, 128, 128), F32),
            pltpu.SemaphoreType.DMA((4, 2)),
            pltpu.SemaphoreType.DMA((4, 2)),
            pltpu.SemaphoreType.DMA((4, 2)),
            pltpu.SemaphoreType.DMA((4, 2)),
            pltpu.SemaphoreType.DMA((NZ,)),
            pltpu.SemaphoreType.DMA((NZ,)),
            pltpu.SemaphoreType.DMA((NZ,)),
            pltpu.SemaphoreType.DMA((NZ,)),
        ],
        compiler_params=pltpu.CompilerParams(
            collective_id=1, has_side_effects=True, vmem_limit_bytes=48 << 20
        ),
        name="mix",
    )(proj, packed, params, maps)


def finish_kernel(
    attend, scan, w_attend, w_scan,
    out,
    attend_in, scan_in, part_out, part_in,
    s_attend, r_attend, s_scan, r_scan, s_part, r_part,
):
    y, x, t = (lax.axis_index(a) for a in ("sp_1", "fs", "tp"))
    greet(plane_peers(x, y, t))
    attend_in[0, 0] = attend[y]
    scan_in[0, 0] = scan[y]
    await_greetings(19)
    copies, arriving = [], {}
    for dx in (0, 1, 3, 2):
        for dy in (1, 3, 2, 0):
            if (dx, dy) != (0, 0):
                to = (y + dy) % NY
                where = {"fs": (x + dx) % NX, "sp_1": to}
                pair = (
                    remote(
                        scan.at[to], scan_in.at[dx, dy], s_scan.at[dx, dy], r_scan.at[dx, dy],
                        where,
                    ),
                    remote(
                        attend.at[to], attend_in.at[dx, dy], s_attend.at[dx, dy],
                        r_attend.at[dx, dy], where,
                    ),
                )
                for copy in pair:
                    copy.start()
                    copies.append(copy)
                arriving[dx, dy] = pair
    part_copies = {}
    for dx in (0, 1, 3, 2):
        total = None
        for dy in range(NY):
            for copy in arriving.get((dx, dy), ()):
                copy.wait_recv()
            head = (y + NY - dy) % NY
            rows = pl.ds(pl.multiple_of(head * 128, 128), 128)
            product = jnp.dot(
                attend_in[dx, dy], w_attend[rows, :], preferred_element_type=F32
            ) + jnp.dot(scan_in[dx, dy], w_scan[rows, :], preferred_element_type=F32)
            total = product if total is None else total + product
        rounded = total.astype(BF16)
        for k in range(NT):
            part_out[dx, k] = rounded[k * 64 : (k + 1) * 64]
        for dt in range(NT):
            if (dx, dt) != (0, 0):
                to = (t + dt) % NT
                part_copies[dx, dt] = remote(
                    part_out.at[dx, to], part_in.at[dx, dt], s_part.at[dx, dt], r_part.at[dx, dt],
                    {"fs": (x + NX - dx) % NX, "tp": to},
                )
                part_copies[dx, dt].start()
    part_in[0, 0] = part_out[0, t]
    for dx in (0, 1, 3, 2):
        for dt in range(NT):
            if (dx, dt) != (0, 0):
                part_copies[dx, dt].wait_recv()
        columns = pl.ds(pl.multiple_of((x + dx) % NX * 512, 512), 512)
        out[:, columns] = (part_in[dx, 0].astype(F32) + part_in[dx, 1].astype(F32)).astype(BF16)
    for copy in copies:
        copy.wait_send()
    for copy in part_copies.values():
        copy.wait_send()


def finish(attend, scan, w_attend, w_scan):
    return pl.pallas_call(
        finish_kernel,
        out_shape=jax.ShapeDtypeStruct((64, 2048), BF16),
        in_specs=[VMEM] * 4,
        out_specs=VMEM,
        scratch_shapes=[
            pltpu.VMEM((NX, NY, 128, 128), BF16),
            pltpu.VMEM((NX, NY, 128, 128), BF16),
            pltpu.VMEM((NX, NT, 64, 512), BF16),
            pltpu.VMEM((NX, NT, 64, 512), BF16),
            pltpu.SemaphoreType.DMA((NX, NY)),
            pltpu.SemaphoreType.DMA((NX, NY)),
            pltpu.SemaphoreType.DMA((NX, NY)),
            pltpu.SemaphoreType.DMA((NX, NY)),
            pltpu.SemaphoreType.DMA((NX, NT)),
            pltpu.SemaphoreType.DMA((NX, NT)),
        ],
        compiler_params=pltpu.CompilerParams(
            collective_id=2, has_side_effects=True, vmem_limit_bytes=40 << 20
        ),
        name="finish",
    )(attend, scan, w_attend, w_scan)


def on_device(
    tokens, norm_gain, drive_weight, query_weight, key_weight, value_weight, key_offset, log_step,
    lambda_real, lambda_imag, input_map, output_map, skip_gain, forget, initial_state,
    scan_out_weight, attend_out_weight,
):
    packed = jnp.concatenate(
        [
            forget[:, 0, :].reshape(NY, 8, 128),
            (key_offset[:, 0, :].astype(F32) * LOG2E).reshape(NY, 1, 128),
            jnp.zeros((NY, 7, 128), F32),
        ],
        axis=1,
    )

    def twice(array):
        return jnp.concatenate([array, array], axis=-1).reshape(NY, 8, 128)

    params = jnp.stack(
        [
            twice(lambda_real),
            twice(lambda_imag),
            jnp.broadcast_to(log_step.reshape(NY, 8, 1), (NY, 8, 128)),
            jnp.concatenate([initial_state[0, 0], initial_state[1, 0]], axis=-1).reshape(
                NY, 8, 128
            ),
            jnp.broadcast_to(skip_gain.reshape(NY, 1, 128), (NY, 8, 128)),
        ],
        axis=1,
    )
    maps = jnp.stack(
        [
            jnp.concatenate([input_map[0], input_map[1]], axis=1)
            .transpose(0, 2, 1)
            .reshape(NY, 8, 16, 128),
            jnp.concatenate([output_map[0], output_map[1]], axis=2).reshape(NY, 8, 16, 128),
        ],
        axis=1,
    )
    weights = (drive_weight, query_weight, key_weight, value_weight)
    proj, packed_all = project(tokens[0], norm_gain[None], weights, packed)
    attend, scan = mix(proj, packed_all, params, maps)
    return finish(attend, scan, attend_out_weight, scan_out_weight)[None]


def solution(mesh):
    split = Mesh(
        mesh.devices.reshape(NZ, NY, mesh.shape["fs"], mesh.shape["tp"]),
        ("sp_0", "sp_1", "fs", "tp"),
    )
    in_specs = (
        P("fs", SP_TP, None),
        P(),
        P("fs", "tp"),
        P("fs", "tp"),
        P("fs", "tp"),
        P("fs", "tp"),
        P("tp", "fs", SP),
        P("tp"),
        P("tp", None),
        P("tp", None),
        P(None, "tp", None, None),
        P(None, "tp", None, None),
        P("tp"),
        P("tp", "fs", SP),
        P(None, "fs", "tp", None),
        P("tp", "fs"),
        P("tp", "fs"),
    )
    return jax.shard_map(
        on_device, mesh=split, in_specs=in_specs, out_specs=P("fs", SP_TP, None), check_vma=False
    )
```

```python
import math

import jax
import jax.numpy as jnp
from jax import lax
from jax.experimental import pallas as pl
from jax.experimental.pallas import tpu as pltpu
from jax.sharding import Mesh
from jax.sharding import PartitionSpec as P

SP_TP = ("sp_0", "sp_1", "tp")
SP = ("sp_0", "sp_1")
EPSILON = 1e-06
LOG2E = 1.4426950408889634
NZ, NY, NX, NT = 8, 4, 4, 2
BF16, F32 = jnp.bfloat16, jnp.float32
VMEM = pl.BlockSpec(memory_space=pltpu.VMEM)
MESH_ID = pl.DeviceIdType.MESH


def remote(src, dst, send_sem, recv_sem, where):
    return pltpu.make_async_remote_copy(
        src_ref=src, dst_ref=dst, send_sem=send_sem, recv_sem=recv_sem,
        device_id=where, device_id_type=MESH_ID,
    )


def greet(peers):
    barrier = pltpu.get_barrier_semaphore()
    for peer in peers:
        pl.semaphore_signal(barrier, inc=1, device_id=peer, device_id_type=MESH_ID)


def await_greetings(count):
    pl.semaphore_wait(pltpu.get_barrier_semaphore(), count)


def plane_peers(x, y, t):
    peers = [
        {"fs": (x + dx) % NX, "tp": (t + dt) % NT}
        for dx in range(NX) for dt in range(NT) if (dx, dt) != (0, 0)
    ]
    peers += [
        {"fs": (x + dx) % NX, "sp_1": (y + dy) % NY} for dx in range(NX) for dy in range(1, NY)
    ]
    return peers


def high_low(value):
    high = value.astype(BF16)
    return high, (value - high.astype(F32)).astype(BF16)


def attend_pair(query, key, value, offset, fallen, ladder, visible):
    score = lax.dot_general(query, key, (((1,), (1,)), ((), ())), preferred_element_type=F32)
    score = score * (LOG2E * 128**-0.5) + offset
    soft = jnp.maximum(score, 0.0) + LOG2E * jnp.log(1.0 + jnp.exp2(-jnp.abs(score)))
    if visible is not None:
        soft = jnp.where(visible, soft, 0.0)
    sums = jnp.dot(
        jnp.concatenate(high_low(soft), axis=1), ladder, preferred_element_type=F32
    )
    behind = sums[:, :128] if fallen is None else sums[:, :128] + fallen
    weight = jnp.exp2(score + behind)
    if visible is not None:
        weight = jnp.where(visible, weight, 0.0)
    portion = jnp.dot(weight.astype(BF16), value, preferred_element_type=F32)
    total = sums[:, 128:] if fallen is None else sums[:, 128:] + fallen
    return portion, total


def turned(gain, state):
    return gain[0] * state + gain[1] * pltpu.roll(state, 64, 1)


def powers_times(left, right):
    return (
        left[0] * right[0] - left[1] * right[1],
        left[1] * right[0] + left[0] * right[1],
    )


def layer_kernel(
    tok, gain_ref, w_drive, w_query, w_key, w_value, packed, params, maps, w_attend, w_scan,
    out,
    normed, rows_in, keyed_w, query_w, drive_w, packed_in, driven_in, queries,
    own_in, right_in, left_in, far_in, offset_own, offset_in, state_own, state_in, acc, tot,
    ladder, into_map, out_map, fwd_p, fwd_q, inv_p, inv_q, held, ends, decay,
    attend_own, scan_own, attend_in, scan_in, part_out, part_in,
    s_rows, r_rows, s_half, r_half, s_weight, r_weight, s_packed, r_packed,
    s_right, r_right, s_left, r_left, s_offset, r_offset, s_state, r_state,
    s_attend, r_attend, s_scan, r_scan, s_part, r_part,
):
    z, y, x, t = (lax.axis_index(a) for a in ("sp_0", "sp_1", "fs", "tp"))
    greet(plane_peers(x, y, t) + [{"sp_0": (z + dz) % NZ} for dz in range(1, NZ)])
    row = lax.broadcasted_iota(jnp.int32, (128, 128), 0)
    lane = lax.broadcasted_iota(jnp.int32, (128, 128), 1)
    up, down = {"sp_0": (z + 1) % NZ}, {"sp_0": (z + NZ - 1) % NZ}
    sent = []

    def send(copy):
        copy.start()
        sent.append(copy)
        return copy

    values = tok[...].astype(F32)
    scale = lax.rsqrt(jnp.mean(values * values, axis=1, keepdims=True) + EPSILON)
    normed[...] = (values * scale * gain_ref[...]).astype(BF16)
    await_greetings(26)

    order = (0, 1, 3, 2)
    mine = pl.ds(pl.multiple_of(t * 64, 64), 64)
    sibling = {"tp": 1 - t}

    def row_copy(j):
        return remote(
            normed, rows_in.at[j, mine], s_rows.at[j], r_rows.at[j],
            {"sp_1": (y + order[j]) % NY},
        )

    def half_copy(j):
        return remote(
            rows_in.at[j, mine] if j else normed, rows_in.at[j, mine], s_half.at[j], r_half.at[j],
            sibling,
        )

    column = pl.ds(pl.multiple_of(y * 128, 128), 128)
    depth = pl.ds(pl.multiple_of(x * 512, 512), 512)
    sources = (w_key, w_value, w_query, w_drive)
    targets = (
        keyed_w.at[depth, :128], keyed_w.at[depth, 128:], query_w.at[depth], drive_w.at[depth]
    )

    def weight_copy(kind, dx):
        return remote(
            sources[kind].at[:, column], targets[kind], s_weight.at[kind, dx],
            r_weight.at[kind, dx], {"fs": (x + dx) % NX},
        )

    send(half_copy(0))
    for j in (1, 2, 3):
        send(row_copy(j))
    for kind in range(4):
        for dx in (1, 3, 2):
            send(weight_copy(kind, dx))
    packed_copies = [
        send(
            remote(
                packed.at[(y + dy) % NY], packed_in.at[y], s_packed.at[dy], r_packed.at[dy],
                {"sp_1": (y + dy) % NY},
            )
        )
        for dy in range(1, NY)
    ]
    packed_in[y] = packed[y]
    rows_in[0, mine] = normed[...]
    keyed_w[depth, :128] = w_key[:, column]
    keyed_w[depth, 128:] = w_value[:, column]
    query_w[depth] = w_query[:, column]
    drive_w[depth] = w_drive[:, column]

    sign = jnp.where(lane[:8] < 64, -1.0, 1.0)
    lam_real, lam_imag, log_step, initial, skip = (params[y, k] for k in range(5))
    step = jnp.exp(log_step)
    log_gain, rotate = lam_real * step, lam_imag * step
    cosine, sine, magnitude = jnp.cos(rotate), jnp.sin(rotate), jnp.exp(log_gain)
    bar_real, bar_imag = magnitude * cosine, magnitude * sine
    divisor = lam_real * lam_real + lam_imag * lam_imag
    shifted = bar_real - 1.0
    factor_real = (shifted * lam_real + bar_imag * lam_imag) / divisor
    factor_imag = (bar_imag * lam_real - shifted * lam_imag) / divisor * sign
    shrink = jnp.exp(-log_gain)
    gain = (bar_real, sign * bar_imag)
    inverse = (shrink * cosine, -sign * shrink * sine)
    gains, inverses = [gain], [inverse]
    for _ in range(9):
        gains.append(powers_times(gains[-1], gains[-1]))
    for _ in range(6):
        inverses.append(powers_times(inverses[-1], inverses[-1]))
    gain_block, gain_all = gains[7], gains[9]
    gain_last = powers_times(gain_block, inverse)
    into_map[...] = jnp.zeros_like(into_map)
    out_map[...] = jnp.zeros_like(out_map)
    for g in range(8):
        cols, swapped = pl.ds(g * 128, 128), pl.ds(1024 + g * 128, 128)
        raw = maps[y, 0, g]
        entry = factor_real[g : g + 1] * raw + factor_imag[g : g + 1] * pltpu.roll(raw, 64, 1)
        turned_entry = pltpu.roll(entry, 64, 1)
        for at in (g * 16, 128 + g * 16):
            into_map[at : at + 16, cols] = entry.astype(BF16)
            into_map[at : at + 16, swapped] = turned_entry.astype(BF16)
        raw = maps[y, 1, g]
        out_map[g * 16 : g * 16 + 16, cols] = (raw * -sign[:1]).astype(BF16)
        out_map[g * 16 : g * 16 + 16, swapped] = (pltpu.roll(raw, 64, 1) * -sign[:1]).astype(BF16)
        for table_p, table_q, steps in ((fwd_p, fwd_q, gains), (inv_p, inv_q, inverses)):
            real, imag = jnp.ones((8, 128), F32), jnp.zeros((8, 128), F32)
            for bit in range(3):
                by = tuple(part[g : g + 1] for part in steps[bit])
                new = powers_times((real, imag), by)
                chosen = (row[:8] & (1 << bit)) != 0
                real, imag = jnp.where(chosen, new[0], real), jnp.where(chosen, new[1], imag)
            table_p[:8, cols] = real
            table_q[:8, cols] = imag
            for bit in range(3, 7):
                n = 1 << bit
                by = tuple(part[g : g + 1] for part in steps[bit])
                new = powers_times((table_p[:n, cols], table_q[:n, cols]), by)
                table_p[n : 2 * n, cols] = new[0]
                table_q[n : 2 * n, cols] = new[1]
    ladder_row = lax.broadcasted_iota(jnp.int32, (256, 256), 0) % 128
    ladder_lane = lax.broadcasted_iota(jnp.int32, (256, 256), 1)
    ladder[...] = jnp.where((ladder_lane >= 128) | (ladder_row >= ladder_lane), -1.0, 0.0).astype(
        BF16
    )

    def block_of(j):
        dy = j + j // 2 * (5 - 2 * j)
        return (y + NY - dy) % NY

    def right_copy(i, j):
        b = block_of(j)
        return remote(
            own_in.at[b] if i == 1 else right_in.at[i - 2, b],
            far_in.at[b] if i == 4 else right_in.at[i - 1, b],
            s_right.at[i - 1, j], r_right.at[i - 1, j], up,
        )

    def left_copy(i, j):
        b = block_of(j)
        return remote(
            own_in.at[b] if i == 1 else left_in.at[i - 2, b],
            far_in.at[b] if i == 4 else left_in.at[i - 1, b],
            s_left.at[i - 1, j], r_left.at[i - 1, j], down,
        )

    def own_keys(first, last):
        product = jnp.dot(
            rows_in[first:last].reshape((last - first) * 128, 2048), keyed_w[...],
            preferred_element_type=F32,
        ).astype(BF16)
        for j in range(first, last):
            own_in[block_of(j)] = product[(j - first) * 128 : (j - first + 1) * 128]
            right_copy(1, j).start()
            left_copy(1, j).start()

    for j in (1, 2):
        row_copy(j).wait_recv()
        send(half_copy(j))
    for copy in packed_copies:
        copy.wait_recv()
    for b in range(NY):
        offset_own[b : b + 1, :] = packed_in[b, 8:9, :]
        offset_in[0, b : b + 1, :] = packed_in[b, 8:9, :]
    offset_own[4:8, :] = jnp.zeros((4, 128), F32)
    offset_copies = [
        send(
            remote(
                offset_own, offset_in.at[dz], s_offset.at[dz], r_offset.at[dz],
                {"sp_0": (z + dz) % NZ},
            )
        )
        for dz in range(1, NZ)
    ]
    for kind in (0, 1):
        for dx in (1, 3, 2):
            weight_copy(kind, dx).wait_recv()
    for j in (0, 1, 2):
        half_copy(j).wait_recv()
    own_keys(0, 3)
    row_copy(3).wait_recv()
    send(half_copy(3))
    half_copy(3).wait_recv()
    own_keys(3, 4)
    until = jnp.where(lane <= row, 1.0, 0.0)
    until_half = until.astype(BF16)
    falls = []
    for b in range(NY):
        forget = packed_in[b, :8, :]
        spread = jnp.concatenate(
            [jnp.broadcast_to(forget[g : g + 1], (16, 128)) for g in range(8)], axis=0
        )
        decay[b] = lax.dot_general(
            until, spread, (((1,), (1,)), ((), ())), preferred_element_type=F32,
            precision=lax.Precision.HIGHEST,
        )
        falls.append(jnp.sum(forget, axis=1, keepdims=True))
    for dx in (1, 3, 2):
        weight_copy(2, dx).wait_recv()
    product = jnp.dot(
        rows_in[...].reshape(512, 2048), query_w[...], preferred_element_type=F32
    ).astype(BF16)
    for j in range(NY):
        queries[block_of(j)] = product[j * 128 : (j + 1) * 128]

    def arrive(i, j):
        right_copy(i, j).wait_recv()
        left_copy(i, j).wait_recv()
        if i < 3:
            right_copy(i + 1, j).start()
            left_copy(i + 1, j).start()
            return

        @pl.when(j < 2)
        def _():
            right_copy(4, j).start()

        @pl.when(j >= 2)
        def _():
            left_copy(4, j).start()

    for j in range(NY):
        arrive(1, j)

    for q in range(NY):
        portion_sum, fallen = None, None
        for k in range(q, -1, -1):
            portion, fallen = attend_pair(
                queries[q], own_in[k, :, :128], own_in[k, :, 128:], offset_in[0, k : k + 1, :],
                fallen, ladder[...], lane < row if k == q else None,
            )
            portion_sum = portion if portion_sum is None else portion_sum + portion
        acc[0, q] = portion_sum
        tot[0, q] = fallen
    for copy in offset_copies:
        copy.wait_recv()

    for dx in (1, 3, 2):
        weight_copy(3, dx).wait_recv()
    product = jnp.dot(
        rows_in[...].reshape(512, 2048), drive_w[...], preferred_element_type=F32
    ).astype(BF16)
    for j in range(NY):
        driven_in[block_of(j)] = product[j * 128 : (j + 1) * 128]
    local = jnp.zeros((8, 128), F32)
    fall_all = jnp.zeros((8, 1), F32)
    for b in range(NY):
        driven = driven_in[b].astype(F32) * jnp.exp(-decay[b])
        entered = jnp.dot(
            jnp.concatenate(high_low(driven), axis=1), into_map[...], preferred_element_type=F32
        )
        unturned = entered[:, :1024] * inv_p[...] + entered[:, 1024:] * inv_q[...]
        high, low = high_low(unturned)
        held[b] = jnp.dot(until_half, high, preferred_element_type=F32) + jnp.dot(
            until_half, low, preferred_element_type=F32
        )
        for g in range(8):
            ends[b, g : g + 1, :] = held[b, 127:128, g * 128 : (g + 1) * 128]
        fall_all = fall_all + falls[b]
        falls[b] = jnp.exp(falls[b])
        ends[b] = falls[b] * turned(gain_last, ends[b])
        local = falls[b] * turned(gain_block, local) + ends[b]
        arrive(2, b)
    state_own[:8, :] = local
    state_own[8:, :] = jnp.broadcast_to(fall_all, (8, 128))
    state_copies = [
        send(
            remote(
                state_own, state_in.at[dz], s_state.at[dz], r_state.at[dz],
                {"sp_0": (z + dz) % NZ},
            )
        )
        for dz in range(1, NZ)
    ]

    def attend_block(dz, pairs, k):
        offset = offset_in[dz, pl.ds(k, 1), :]
        for q in range(NY):
            portion, fallen = attend_pair(
                queries[q], pairs[k, :, :128], pairs[k, :, 128:], offset, tot[dz, q],
                ladder[...], None,
            )
            acc[dz, q] += portion
            tot[dz, q] = fallen

    def attend_step(i):
        chunks = [(i, right_in.at[i - 1]), (8 - i, left_in.at[i - 1])] if i < 4 else [(4, far_in)]
        for dz, _ in chunks:
            @pl.when(z >= dz)
            def _():
                acc[dz] = jnp.zeros((NY, 128, 128), F32)
                tot[dz] = jnp.zeros((NY, 128, 128), F32)

        def one(turn, carry):
            if i < 2:
                arrive(i + 2, turn)
            elif i == 2:
                @pl.when(turn < 2)
                def _():
                    right_copy(4, turn).wait_recv()

                @pl.when(turn >= 2)
                def _():
                    left_copy(4, turn).wait_recv()

            for dz, pairs in chunks:
                @pl.when(z >= dz)
                def _():
                    attend_block(dz, pairs, NY - 1 - turn)

            return carry

        lax.fori_loop(0, NY, one, 0)

    attend_step(1)
    attend_step(2)

    for copy in state_copies:
        copy.wait_recv()
    carry = initial
    for source in range(NZ - 1):
        arrived = state_in[jnp.maximum(z - source, 1)]
        moved = jnp.exp(arrived[8:]) * turned(gain_all, carry) + arrived[:8]
        carry = jnp.where(source < z, moved, carry)
    for b in range(NY):
        entering = turned(gain, carry)
        whole = jnp.concatenate(
            [held[b, :, g * 128 : (g + 1) * 128] + entering[g : g + 1] for g in range(8)], axis=1
        )
        turned_states = jnp.concatenate(
            [(whole * fwd_p[...]).astype(BF16), (whole * fwd_q[...]).astype(BF16)], axis=1
        )
        read = lax.dot_general(
            turned_states, out_map[...], (((1,), (1,)), ((), ())), preferred_element_type=F32
        )
        read = read * jnp.exp(decay[b]) + skip[:1] * driven_in[b].astype(F32)
        inner = math.sqrt(2.0 / math.pi) * (read + 0.044715 * (read * read * read))
        scan_own[b] = (0.5 * read * (1.0 + jnp.tanh(inner))).astype(BF16)
        carry = falls[b] * turned(gain_block, carry) + ends[b]

    def spread_copies(own, landing, s_sem, r_sem):
        return {
            (dx, dy): remote(
                own.at[(y + dy) % NY], landing.at[dx, dy], s_sem.at[dx, dy], r_sem.at[dx, dy],
                {"fs": (x + dx) % NX, "sp_1": (y + dy) % NY},
            )
            for dx in order for dy in (1, 3, 2, 0) if (dx, dy) != (0, 0)
        }

    scan_copies = spread_copies(scan_own, scan_in, s_scan, r_scan)
    for copy in scan_copies.values():
        send(copy)
    scan_in[0, 0] = scan_own[y]
    attend_step(3)
    attend_step(4)
    for dz in range(1, NZ):
        @pl.when(z >= dz)
        def _():
            for q in range(NY):
                fallen = tot[0, q]
                acc[0, q] += jnp.exp2(fallen) * acc[dz, q]
                tot[0, q] = fallen + tot[dz, q]

    for q in range(NY):
        attend_own[q] = acc[0, q].astype(BF16)
    attend_copies = spread_copies(attend_own, attend_in, s_attend, r_attend)
    for copy in attend_copies.values():
        send(copy)
    attend_in[0, 0] = attend_own[y]

    part_copies = {}
    for dx in order:
        total = None
        for dy in range(NY):
            if (dx, dy) != (0, 0):
                scan_copies[dx, dy].wait_recv()
                attend_copies[dx, dy].wait_recv()
            head = (y + NY - dy) % NY
            head_rows = pl.ds(pl.multiple_of(head * 128, 128), 128)
            product = jnp.dot(
                attend_in[dx, dy], w_attend[head_rows, :], preferred_element_type=F32
            ) + jnp.dot(scan_in[dx, dy], w_scan[head_rows, :], preferred_element_type=F32)
            total = product if total is None else total + product
        rounded = total.astype(BF16)
        for k in range(NT):
            part_out[dx, k] = rounded[k * 64 : (k + 1) * 64]
        for dt in range(NT):
            if (dx, dt) != (0, 0):
                to = (t + dt) % NT
                part_copies[dx, dt] = send(
                    remote(
                        part_out.at[dx, to], part_in.at[dx, dt], s_part.at[dx, dt],
                        r_part.at[dx, dt], {"fs": (x + NX - dx) % NX, "tp": to},
                    )
                )
    part_in[0, 0] = part_out[0, t]
    for dx in order:
        for dt in range(NT):
            if (dx, dt) != (0, 0):
                part_copies[dx, dt].wait_recv()
        columns = pl.ds(pl.multiple_of((x + dx) % NX * 512, 512), 512)
        out[:, columns] = (part_in[dx, 0].astype(F32) + part_in[dx, 1].astype(F32)).astype(BF16)
    for copy in sent:
        copy.wait_send()
    for i in range(1, 5):
        for j in range(NY):
            if i < 4 or j < 2:
                right_copy(i, j).wait_send()
            if i < 4 or j >= 2:
                left_copy(i, j).wait_send()


def layer(*operands):
    def sems(*shape):
        return [pltpu.SemaphoreType.DMA(shape)] * 2

    return pl.pallas_call(
        layer_kernel,
        out_shape=jax.ShapeDtypeStruct((64, 2048), BF16),
        in_specs=[VMEM] * 11,
        out_specs=VMEM,
        scratch_shapes=[
            pltpu.VMEM((64, 2048), BF16),
            pltpu.VMEM((NY, 128, 2048), BF16),
            pltpu.VMEM((2048, 256), BF16),
            pltpu.VMEM((2048, 128), BF16),
            pltpu.VMEM((2048, 128), BF16),
            pltpu.VMEM((NY, 16, 128), F32),
            pltpu.VMEM((NY, 128, 128), BF16),
            pltpu.VMEM((NY, 128, 128), BF16),
            pltpu.VMEM((NY, 128, 256), BF16),
            pltpu.VMEM((3, NY, 128, 256), BF16),
            pltpu.VMEM((3, NY, 128, 256), BF16),
            pltpu.VMEM((NY, 128, 256), BF16),
            pltpu.VMEM((8, 128), F32),
            pltpu.VMEM((NZ, 8, 128), F32),
            pltpu.VMEM((16, 128), F32),
            pltpu.VMEM((NZ, 16, 128), F32),
            pltpu.VMEM((NZ, NY, 128, 128), F32),
            pltpu.VMEM((NZ, NY, 128, 128), F32),
            pltpu.VMEM((256, 256), BF16),
            pltpu.VMEM((256, 2048), BF16),
            pltpu.VMEM((128, 2048), BF16),
            pltpu.VMEM((128, 1024), F32),
            pltpu.VMEM((128, 1024), F32),
            pltpu.VMEM((128, 1024), F32),
            pltpu.VMEM((128, 1024), F32),
            pltpu.VMEM((NY, 128, 1024), F32),
            pltpu.VMEM((NY, 8, 128), F32),
            pltpu.VMEM((NY, 128, 128), F32),
            pltpu.VMEM((NY, 128, 128), BF16),
            pltpu.VMEM((NY, 128, 128), BF16),
            pltpu.VMEM((NX, NY, 128, 128), BF16),
            pltpu.VMEM((NX, NY, 128, 128), BF16),
            pltpu.VMEM((NX, NT, 64, 512), BF16),
            pltpu.VMEM((NX, NT, 64, 512), BF16),
            *sems(NY), *sems(NY), *sems(4, NX), *sems(NY), *sems(4, NY), *sems(4, NY), *sems(NZ),
            *sems(NZ), *sems(NX, NY), *sems(NX, NY), *sems(NX, NT),
        ],
        compiler_params=pltpu.CompilerParams(
            collective_id=0, has_side_effects=True, vmem_limit_bytes=56 << 20
        ),
        name="layer",
    )(*operands)


def on_device(
    tokens, norm_gain, drive_weight, query_weight, key_weight, value_weight, key_offset, log_step,
    lambda_real, lambda_imag, input_map, output_map, skip_gain, forget, initial_state,
    scan_out_weight, attend_out_weight,
):
    packed = jnp.concatenate(
        [
            forget[:, 0, :].reshape(NY, 8, 128),
            (key_offset[:, 0, :].astype(F32) * LOG2E).reshape(NY, 1, 128),
            jnp.zeros((NY, 7, 128), F32),
        ],
        axis=1,
    )

    def twice(array):
        return jnp.concatenate([array, array], axis=-1).reshape(NY, 8, 128)

    params = jnp.stack(
        [
            twice(lambda_real),
            twice(lambda_imag),
            jnp.broadcast_to(log_step.reshape(NY, 8, 1), (NY, 8, 128)),
            jnp.concatenate([initial_state[0, 0], initial_state[1, 0]], axis=-1).reshape(
                NY, 8, 128
            ),
            jnp.broadcast_to(skip_gain.reshape(NY, 1, 128), (NY, 8, 128)),
        ],
        axis=1,
    )
    maps = jnp.stack(
        [
            jnp.concatenate([input_map[0], input_map[1]], axis=1)
            .transpose(0, 2, 1)
            .reshape(NY, 8, 16, 128),
            jnp.concatenate([output_map[0], output_map[1]], axis=2).reshape(NY, 8, 16, 128),
        ],
        axis=1,
    )
    weights = (drive_weight, query_weight, key_weight, value_weight)
    return layer(
        tokens[0], norm_gain[None], *weights, packed, params, maps, attend_out_weight,
        scan_out_weight,
    )[None]


def solution(mesh):
    split = Mesh(
        mesh.devices.reshape(NZ, NY, mesh.shape["fs"], mesh.shape["tp"]),
        ("sp_0", "sp_1", "fs", "tp"),
    )
    in_specs = (
        P("fs", SP_TP, None),
        P(),
        P("fs", "tp"),
        P("fs", "tp"),
        P("fs", "tp"),
        P("fs", "tp"),
        P("tp", "fs", SP),
        P("tp"),
        P("tp", None),
        P("tp", None),
        P(None, "tp", None, None),
        P(None, "tp", None, None),
        P("tp"),
        P("tp", "fs", SP),
        P(None, "fs", "tp", None),
        P("tp", "fs"),
        P("tp", "fs"),
    )
    return jax.shard_map(
        on_device, mesh=split, in_specs=in_specs, out_specs=P("fs", SP_TP, None), check_vma=False
    )
```

```python
import math

import jax
import jax.numpy as jnp
from jax import lax
from jax.experimental import pallas as pl
from jax.experimental.pallas import tpu as pltpu
from jax.sharding import Mesh
from jax.sharding import PartitionSpec as P

SP_TP = ("sp_0", "sp_1", "tp")
SP = ("sp_0", "sp_1")
EPSILON = 1e-06
LOG2E = 1.4426950408889634
NZ, NY, NX, NT = 8, 4, 4, 2
BF16, F32 = jnp.bfloat16, jnp.float32
VMEM = pl.BlockSpec(memory_space=pltpu.VMEM)
MESH_ID = pl.DeviceIdType.MESH


def remote(src, dst, send_sem, recv_sem, where):
    return pltpu.make_async_remote_copy(
        src_ref=src, dst_ref=dst, send_sem=send_sem, recv_sem=recv_sem,
        device_id=where, device_id_type=MESH_ID,
    )


def greet(peers):
    barrier = pltpu.get_barrier_semaphore()
    for peer in peers:
        pl.semaphore_signal(barrier, inc=1, device_id=peer, device_id_type=MESH_ID)


def await_greetings(count):
    pl.semaphore_wait(pltpu.get_barrier_semaphore(), count)


def plane_peers(x, y, t):
    peers = [
        {"fs": (x + dx) % NX, "tp": (t + dt) % NT}
        for dx in range(NX) for dt in range(NT) if (dx, dt) != (0, 0)
    ]
    peers += [
        {"fs": (x + dx) % NX, "sp_1": (y + dy) % NY} for dx in range(NX) for dy in range(1, NY)
    ]
    return peers


def high_low(value):
    high = value.astype(BF16)
    return high, (value - high.astype(F32)).astype(BF16)


def attend_pair(query, key, value, offset, fallen, ladder, visible):
    score = lax.dot_general(query, key, (((1,), (1,)), ((), ())), preferred_element_type=F32)
    score = score * (LOG2E * 128**-0.5) + offset
    soft = jnp.maximum(score, 0.0) + LOG2E * jnp.log(1.0 + jnp.exp2(-jnp.abs(score)))
    if visible is not None:
        soft = jnp.where(visible, soft, 0.0)
    sums = jnp.dot(
        jnp.concatenate(high_low(soft), axis=1), ladder, preferred_element_type=F32
    )
    behind = sums[:, :128] if fallen is None else sums[:, :128] + fallen
    weight = jnp.exp2(score + behind)
    if visible is not None:
        weight = jnp.where(visible, weight, 0.0)
    portion = jnp.dot(weight.astype(BF16), value, preferred_element_type=F32)
    total = sums[:, 128:] if fallen is None else sums[:, 128:] + fallen
    return portion, total


def turned(gain, state):
    return gain[0] * state + gain[1] * pltpu.roll(state, 64, 1)


def powers_times(left, right):
    return (
        left[0] * right[0] - left[1] * right[1],
        left[1] * right[0] + left[0] * right[1],
    )


def layer_kernel(
    *refs,
):
    operands, outs, held_here, rest = refs[:17], refs[17:19], refs[19:36], refs[36:]
    run_layer(operands, outs, held_here, *rest)


def run_layer(
    operands, outs, held_here, s_operand,
    normed, rows_in, keyed_w, query_w, drive_w, packed, packed_in, driven_in, queries,
    own_in, right_in, left_in, far_in, offset_own, offset_in, state_own, state_in, acc, tot,
    ladder, into_map, out_map, fwd_p, fwd_q, inv_p, inv_q, held, ends, decay,
    attend_own, scan_own, attend_in, scan_in, part_out, part_in,
    s_rows, r_rows, s_half, r_half, s_weight, r_weight, s_packed, r_packed,
    s_right, r_right, s_left, r_left, s_offset, r_offset, s_state, r_state,
    s_attend, r_attend, s_scan, r_scan, s_part, r_part,
):
    (
        tok, gain_ref, w_drive, w_query, w_key, w_value, key_offset, log_step_ref, lambda_real,
        lambda_imag, input_map, output_map, skip_ref, forget_ref, initial_ref, w_attend, w_scan,
    ) = held_here
    fetches = [
        pltpu.make_async_copy(src, dst, s_operand.at[k])
        for k, (src, dst) in enumerate(zip(operands, held_here))
    ]
    for fetch in fetches:
        fetch.start()
    z, y, x, t = (lax.axis_index(a) for a in ("sp_0", "sp_1", "fs", "tp"))
    greet(plane_peers(x, y, t) + [{"sp_0": (z + dz) % NZ} for dz in range(1, NZ)])
    row = lax.broadcasted_iota(jnp.int32, (128, 128), 0)
    lane = lax.broadcasted_iota(jnp.int32, (128, 128), 1)
    up, down = {"sp_0": (z + 1) % NZ}, {"sp_0": (z + NZ - 1) % NZ}
    sent = []

    def send(copy):
        copy.start()
        sent.append(copy)
        return copy

    for k in (0, 1, 6, 13):
        fetches[k].wait()
    packed[:, :8, :] = forget_ref[...]
    packed[:, 8:, :] = jnp.zeros((NY, 8, 128), F32)
    offsets = key_offset[...].astype(F32) * LOG2E
    for k in range(NY):
        packed[k, 8:9, :] = offsets[k : k + 1]
    values = tok[...].astype(F32)
    scale = lax.rsqrt(jnp.mean(values * values, axis=1, keepdims=True) + EPSILON)
    normed[...] = (values * scale * gain_ref[...]).astype(BF16)
    for k in (2, 3, 4, 5):
        fetches[k].wait()
    await_greetings(26)

    order = (0, 1, 3, 2)
    mine = pl.ds(pl.multiple_of(t * 64, 64), 64)
    sibling = {"tp": 1 - t}

    def row_copy(j):
        return remote(
            normed, rows_in.at[j, mine], s_rows.at[j], r_rows.at[j],
            {"sp_1": (y + order[j]) % NY},
        )

    def half_copy(j):
        return remote(
            rows_in.at[j, mine] if j else normed, rows_in.at[j, mine], s_half.at[j], r_half.at[j],
            sibling,
        )

    column = pl.ds(pl.multiple_of(y * 128, 128), 128)
    depth = pl.ds(pl.multiple_of(x * 512, 512), 512)
    sources = (w_key, w_value, w_query, w_drive)
    targets = (
        keyed_w.at[depth, :128], keyed_w.at[depth, 128:], query_w.at[depth], drive_w.at[depth]
    )

    def weight_copy(kind, dx):
        return remote(
            sources[kind].at[:, column], targets[kind], s_weight.at[kind, dx],
            r_weight.at[kind, dx], {"fs": (x + dx) % NX},
        )

    send(half_copy(0))
    for j in (1, 2, 3):
        send(row_copy(j))
    for kind in range(4):
        for dx in (1, 3, 2):
            send(weight_copy(kind, dx))
    packed_copies = [
        send(
            remote(
                packed.at[(y + dy) % NY], packed_in.at[y], s_packed.at[dy], r_packed.at[dy],
                {"sp_1": (y + dy) % NY},
            )
        )
        for dy in range(1, NY)
    ]
    packed_in[y] = packed[y]
    rows_in[0, mine] = normed[...]
    keyed_w[depth, :128] = w_key[:, column]
    keyed_w[depth, 128:] = w_value[:, column]
    query_w[depth] = w_query[:, column]
    drive_w[depth] = w_drive[:, column]

    for k in (7, 8, 9, 10, 11, 12, 14, 15, 16):
        fetches[k].wait()
    sign = jnp.where(lane[:8] < 64, -1.0, 1.0)
    groups = pl.ds(pl.multiple_of(y * 8, 8), 8)

    def side_by_side(left, right):
        return jnp.concatenate([left, right], axis=1)

    lam_real = side_by_side(lambda_real[groups, :], lambda_real[groups, :])
    lam_imag = side_by_side(lambda_imag[groups, :], lambda_imag[groups, :])
    initial = side_by_side(initial_ref[0, groups, :], initial_ref[1, groups, :])
    spot = lax.broadcasted_iota(jnp.int32, (8, 32), 1) - lax.broadcasted_iota(
        jnp.int32, (8, 32), 0
    )
    step = jnp.exp(
        jnp.sum(jnp.where(spot == y * 8, log_step_ref[...], 0.0), axis=1, keepdims=True)
    )
    log_gain, rotate = lam_real * step, lam_imag * step
    cosine, sine, magnitude = jnp.cos(rotate), jnp.sin(rotate), jnp.exp(log_gain)
    bar_real, bar_imag = magnitude * cosine, magnitude * sine
    divisor = lam_real * lam_real + lam_imag * lam_imag
    shifted = bar_real - 1.0
    factor_real = (shifted * lam_real + bar_imag * lam_imag) / divisor
    factor_imag = (bar_imag * lam_real - shifted * lam_imag) / divisor * sign
    shrink = jnp.exp(-log_gain)
    gain = (bar_real, sign * bar_imag)
    inverse = (shrink * cosine, -sign * shrink * sine)
    gains, inverses = [gain], [inverse]
    for _ in range(9):
        gains.append(powers_times(gains[-1], gains[-1]))
    for _ in range(6):
        inverses.append(powers_times(inverses[-1], inverses[-1]))
    gain_block, gain_all = gains[7], gains[9]
    gain_last = powers_times(gain_block, inverse)
    into_map[...] = jnp.zeros_like(into_map)
    out_map[...] = jnp.zeros_like(out_map)
    for g in range(8):
        cols, swapped = pl.ds(g * 128, 128), pl.ds(1024 + g * 128, 128)
        raw = side_by_side(input_map[0, y * 8 + g], input_map[1, y * 8 + g])
        entry = factor_real[g : g + 1] * raw + factor_imag[g : g + 1] * pltpu.roll(raw, 64, 1)
        turned_entry = pltpu.roll(entry, 64, 1)
        for at in (g * 16, 128 + g * 16):
            into_map[at : at + 16, cols] = entry.astype(BF16)
            into_map[at : at + 16, swapped] = turned_entry.astype(BF16)
        raw = side_by_side(output_map[0, y * 8 + g], output_map[1, y * 8 + g])
        out_map[g * 16 : g * 16 + 16, cols] = (raw * -sign[:1]).astype(BF16)
        out_map[g * 16 : g * 16 + 16, swapped] = (pltpu.roll(raw, 64, 1) * -sign[:1]).astype(BF16)
        for table_p, table_q, steps in ((fwd_p, fwd_q, gains), (inv_p, inv_q, inverses)):
            real, imag = jnp.ones((8, 128), F32), jnp.zeros((8, 128), F32)
            for bit in range(3):
                by = tuple(part[g : g + 1] for part in steps[bit])
                new = powers_times((real, imag), by)
                chosen = (row[:8] & (1 << bit)) != 0
                real, imag = jnp.where(chosen, new[0], real), jnp.where(chosen, new[1], imag)
            table_p[:8, cols] = real
            table_q[:8, cols] = imag
            for bit in range(3, 7):
                n = 1 << bit
                by = tuple(part[g : g + 1] for part in steps[bit])
                new = powers_times((table_p[:n, cols], table_q[:n, cols]), by)
                table_p[n : 2 * n, cols] = new[0]
                table_q[n : 2 * n, cols] = new[1]
    ladder_row = lax.broadcasted_iota(jnp.int32, (256, 256), 0) % 128
    ladder_lane = lax.broadcasted_iota(jnp.int32, (256, 256), 1)
    ladder[...] = jnp.where((ladder_lane >= 128) | (ladder_row >= ladder_lane), -1.0, 0.0).astype(
        BF16
    )

    def block_of(j):
        dy = j + j // 2 * (5 - 2 * j)
        return (y + NY - dy) % NY

    def right_copy(i, j):
        b = block_of(j)
        return remote(
            own_in.at[b] if i == 1 else right_in.at[i - 2, b],
            far_in.at[b] if i == 4 else right_in.at[i - 1, b],
            s_right.at[i - 1, j], r_right.at[i - 1, j], up,
        )

    def left_copy(i, j):
        b = block_of(j)
        return remote(
            own_in.at[b] if i == 1 else left_in.at[i - 2, b],
            far_in.at[b] if i == 4 else left_in.at[i - 1, b],
            s_left.at[i - 1, j], r_left.at[i - 1, j], down,
        )

    def own_keys(first, last):
        product = jnp.dot(
            rows_in[first:last].reshape((last - first) * 128, 2048), keyed_w[...],
            preferred_element_type=F32,
        ).astype(BF16)
        for j in range(first, last):
            own_in[block_of(j)] = product[(j - first) * 128 : (j - first + 1) * 128]
            right_copy(1, j).start()
            left_copy(1, j).start()

    for j in (1, 2):
        row_copy(j).wait_recv()
        send(half_copy(j))
    for copy in packed_copies:
        copy.wait_recv()
    for b in range(NY):
        offset_own[b : b + 1, :] = packed_in[b, 8:9, :]
        offset_in[0, b : b + 1, :] = packed_in[b, 8:9, :]
    offset_own[4:8, :] = jnp.zeros((4, 128), F32)
    offset_copies = [
        send(
            remote(
                offset_own, offset_in.at[dz], s_offset.at[dz], r_offset.at[dz],
                {"sp_0": (z + dz) % NZ},
            )
        )
        for dz in range(1, NZ)
    ]
    for kind in (0, 1):
        for dx in (1, 3, 2):
            weight_copy(kind, dx).wait_recv()
    for j in (0, 1, 2):
        half_copy(j).wait_recv()
    own_keys(0, 3)
    row_copy(3).wait_recv()
    send(half_copy(3))
    half_copy(3).wait_recv()
    own_keys(3, 4)
    until = jnp.where(lane <= row, 1.0, 0.0)
    until_half = until.astype(BF16)
    falls = []
    for b in range(NY):
        forget = packed_in[b, :8, :]
        spread = jnp.concatenate(
            [jnp.broadcast_to(forget[g : g + 1], (16, 128)) for g in range(8)], axis=0
        )
        decay[b] = lax.dot_general(
            until, spread, (((1,), (1,)), ((), ())), preferred_element_type=F32,
            precision=lax.Precision.HIGHEST,
        )
        falls.append(jnp.sum(forget, axis=1, keepdims=True))
    for dx in (1, 3, 2):
        weight_copy(2, dx).wait_recv()
    product = jnp.dot(
        rows_in[...].reshape(512, 2048), query_w[...], preferred_element_type=F32
    ).astype(BF16)
    for j in range(NY):
        queries[block_of(j)] = product[j * 128 : (j + 1) * 128]

    def arrive(i, j):
        right_copy(i, j).wait_recv()
        left_copy(i, j).wait_recv()
        if i < 3:
            right_copy(i + 1, j).start()
            left_copy(i + 1, j).start()
            return

        @pl.when(j < 2)
        def _():
            right_copy(4, j).start()

        @pl.when(j >= 2)
        def _():
            left_copy(4, j).start()

    for j in range(NY):
        arrive(1, j)

    for q in range(NY):
        portion_sum, fallen = None, None
        for k in range(q, -1, -1):
            portion, fallen = attend_pair(
                queries[q], own_in[k, :, :128], own_in[k, :, 128:], offset_in[0, k : k + 1, :],
                fallen, ladder[...], lane < row if k == q else None,
            )
            portion_sum = portion if portion_sum is None else portion_sum + portion
        acc[0, q] = portion_sum
        tot[0, q] = fallen
    for copy in offset_copies:
        copy.wait_recv()

    for dx in (1, 3, 2):
        weight_copy(3, dx).wait_recv()
    product = jnp.dot(
        rows_in[...].reshape(512, 2048), drive_w[...], preferred_element_type=F32
    ).astype(BF16)
    for j in range(NY):
        driven_in[block_of(j)] = product[j * 128 : (j + 1) * 128]
    local = jnp.zeros((8, 128), F32)
    fall_all = jnp.zeros((8, 1), F32)
    for b in range(NY):
        driven = driven_in[b].astype(F32) * jnp.exp(-decay[b])
        entered = jnp.dot(
            jnp.concatenate(high_low(driven), axis=1), into_map[...], preferred_element_type=F32
        )
        unturned = entered[:, :1024] * inv_p[...] + entered[:, 1024:] * inv_q[...]
        high, low = high_low(unturned)
        held[b] = jnp.dot(until_half, high, preferred_element_type=F32) + jnp.dot(
            until_half, low, preferred_element_type=F32
        )
        for g in range(8):
            ends[b, g : g + 1, :] = held[b, 127:128, g * 128 : (g + 1) * 128]
        fall_all = fall_all + falls[b]
        falls[b] = jnp.exp(falls[b])
        ends[b] = falls[b] * turned(gain_last, ends[b])
        local = falls[b] * turned(gain_block, local) + ends[b]
        arrive(2, b)
    state_own[:8, :] = local
    state_own[8:, :] = jnp.broadcast_to(fall_all, (8, 128))
    state_copies = [
        send(
            remote(
                state_own, state_in.at[dz], s_state.at[dz], r_state.at[dz],
                {"sp_0": (z + dz) % NZ},
            )
        )
        for dz in range(1, NZ)
    ]

    def attend_block(dz, pairs, k):
        offset = offset_in[dz, pl.ds(k, 1), :]
        for q in range(NY):
            portion, fallen = attend_pair(
                queries[q], pairs[k, :, :128], pairs[k, :, 128:], offset, tot[dz, q],
                ladder[...], None,
            )
            acc[dz, q] += portion
            tot[dz, q] = fallen

    def attend_step(i):
        chunks = [(i, right_in.at[i - 1]), (8 - i, left_in.at[i - 1])] if i < 4 else [(4, far_in)]
        for dz, _ in chunks:
            @pl.when(z >= dz)
            def _():
                acc[dz] = jnp.zeros((NY, 128, 128), F32)
                tot[dz] = jnp.zeros((NY, 128, 128), F32)

        def one(turn, carry):
            if i < 2:
                arrive(i + 2, turn)
            elif i == 2:
                @pl.when(turn < 2)
                def _():
                    right_copy(4, turn).wait_recv()

                @pl.when(turn >= 2)
                def _():
                    left_copy(4, turn).wait_recv()

            for dz, pairs in chunks:
                @pl.when(z >= dz)
                def _():
                    attend_block(dz, pairs, NY - 1 - turn)

            return carry

        lax.fori_loop(0, NY, one, 0)

    attend_step(1)
    attend_step(2)

    for copy in state_copies:
        copy.wait_recv()
    carry = initial
    for source in range(NZ - 1):
        arrived = state_in[jnp.maximum(z - source, 1)]
        moved = jnp.exp(arrived[8:]) * turned(gain_all, carry) + arrived[:8]
        carry = jnp.where(source < z, moved, carry)
    for b in range(NY):
        entering = turned(gain, carry)
        whole = jnp.concatenate(
            [held[b, :, g * 128 : (g + 1) * 128] + entering[g : g + 1] for g in range(8)], axis=1
        )
        turned_states = jnp.concatenate(
            [(whole * fwd_p[...]).astype(BF16), (whole * fwd_q[...]).astype(BF16)], axis=1
        )
        read = lax.dot_general(
            turned_states, out_map[...], (((1,), (1,)), ((), ())), preferred_element_type=F32
        )
        read = read * jnp.exp(decay[b]) + skip_ref[pl.ds(y, 1), :] * driven_in[b].astype(F32)
        inner = math.sqrt(2.0 / math.pi) * (read + 0.044715 * (read * read * read))
        scan_own[b] = (0.5 * read * (1.0 + jnp.tanh(inner))).astype(BF16)
        carry = falls[b] * turned(gain_block, carry) + ends[b]

    def spread_copies(own, landing, s_sem, r_sem):
        return {
            (dx, dy): remote(
                own.at[(y + dy) % NY], landing.at[dx, dy], s_sem.at[dx, dy], r_sem.at[dx, dy],
                {"fs": (x + dx) % NX, "sp_1": (y + dy) % NY},
            )
            for dx in order for dy in (1, 3, 2, 0) if (dx, dy) != (0, 0)
        }

    scan_copies = spread_copies(scan_own, scan_in, s_scan, r_scan)
    for copy in scan_copies.values():
        send(copy)
    scan_in[0, 0] = scan_own[y]
    attend_step(3)
    attend_step(4)
    for dz in range(1, NZ):
        @pl.when(z >= dz)
        def _():
            for q in range(NY):
                fallen = tot[0, q]
                acc[0, q] += jnp.exp2(fallen) * acc[dz, q]
                tot[0, q] = fallen + tot[dz, q]

    for q in range(NY):
        attend_own[q] = acc[0, q].astype(BF16)
    attend_copies = spread_copies(attend_own, attend_in, s_attend, r_attend)
    for copy in attend_copies.values():
        send(copy)
    attend_in[0, 0] = attend_own[y]

    part_copies = {}
    for dx in order:
        total = None
        for dy in range(NY):
            if (dx, dy) != (0, 0):
                scan_copies[dx, dy].wait_recv()
                attend_copies[dx, dy].wait_recv()
            head = (y + NY - dy) % NY
            head_rows = pl.ds(pl.multiple_of(head * 128, 128), 128)
            product = jnp.dot(
                attend_in[dx, dy], w_attend[head_rows, :], preferred_element_type=F32
            ) + jnp.dot(scan_in[dx, dy], w_scan[head_rows, :], preferred_element_type=F32)
            total = product if total is None else total + product
        rounded = total.astype(BF16)
        for k in range(NT):
            part_out[dx, k] = rounded[k * 64 : (k + 1) * 64]
        for dt in range(NT):
            if (dx, dt) != (0, 0):
                to = (t + dt) % NT
                part_copies[dx, dt] = send(
                    remote(
                        part_out.at[dx, to], part_in.at[dx, dt], s_part.at[dx, dt],
                        r_part.at[dx, dt], {"fs": (x + NX - dx) % NX, "tp": to},
                    )
                )
    part_in[0, 0] = part_out[0, t]
    for dx in order:
        for dt in range(NT):
            if (dx, dt) != (0, 0):
                part_copies[dx, dt].wait_recv()
        columns = pl.ds(pl.multiple_of((x + dx) % NX * 512, 512), 512)
        for dt in range(NT):
            outs[dt][:, columns] = part_in[dx, dt]
    for copy in sent:
        copy.wait_send()
    for i in range(1, 5):
        for j in range(NY):
            if i < 4 or j < 2:
                right_copy(i, j).wait_send()
            if i < 4 or j >= 2:
                left_copy(i, j).wait_send()


def layer(*operands):
    def sems(*shape):
        return [pltpu.SemaphoreType.DMA(shape)] * 2

    return pl.pallas_call(
        layer_kernel,
        out_shape=[jax.ShapeDtypeStruct((64, 2048), BF16)] * NT,
        in_specs=[pl.BlockSpec(memory_space=pl.ANY)] * 17,
        out_specs=[VMEM] * NT,
        scratch_shapes=[
            *(pltpu.VMEM(operand.shape, operand.dtype) for operand in operands),
            pltpu.SemaphoreType.DMA((17,)),
            pltpu.VMEM((64, 2048), BF16),
            pltpu.VMEM((NY, 128, 2048), BF16),
            pltpu.VMEM((2048, 256), BF16),
            pltpu.VMEM((2048, 128), BF16),
            pltpu.VMEM((2048, 128), BF16),
            pltpu.VMEM((NY, 16, 128), F32),
            pltpu.VMEM((NY, 16, 128), F32),
            pltpu.VMEM((NY, 128, 128), BF16),
            pltpu.VMEM((NY, 128, 128), BF16),
            pltpu.VMEM((NY, 128, 256), BF16),
            pltpu.VMEM((3, NY, 128, 256), BF16),
            pltpu.VMEM((3, NY, 128, 256), BF16),
            pltpu.VMEM((NY, 128, 256), BF16),
            pltpu.VMEM((8, 128), F32),
            pltpu.VMEM((NZ, 8, 128), F32),
            pltpu.VMEM((16, 128), F32),
            pltpu.VMEM((NZ, 16, 128), F32),
            pltpu.VMEM((NZ, NY, 128, 128), F32),
            pltpu.VMEM((NZ, NY, 128, 128), F32),
            pltpu.VMEM((256, 256), BF16),
            pltpu.VMEM((256, 2048), BF16),
            pltpu.VMEM((128, 2048), BF16),
            pltpu.VMEM((128, 1024), F32),
            pltpu.VMEM((128, 1024), F32),
            pltpu.VMEM((128, 1024), F32),
            pltpu.VMEM((128, 1024), F32),
            pltpu.VMEM((NY, 128, 1024), F32),
            pltpu.VMEM((NY, 8, 128), F32),
            pltpu.VMEM((NY, 128, 128), F32),
            pltpu.VMEM((NY, 128, 128), BF16),
            pltpu.VMEM((NY, 128, 128), BF16),
            pltpu.VMEM((NX, NY, 128, 128), BF16),
            pltpu.VMEM((NX, NY, 128, 128), BF16),
            pltpu.VMEM((NX, NT, 64, 512), BF16),
            pltpu.VMEM((NX, NT, 64, 512), BF16),
            *sems(NY), *sems(NY), *sems(4, NX), *sems(NY), *sems(4, NY), *sems(4, NY), *sems(NZ),
            *sems(NZ), *sems(NX, NY), *sems(NX, NY), *sems(NX, NT),
        ],
        compiler_params=pltpu.CompilerParams(
            collective_id=0, has_side_effects=True, vmem_limit_bytes=60 << 20
        ),
        name="layer",
    )(*operands)


def on_device(
    tokens, norm_gain, drive_weight, query_weight, key_weight, value_weight, key_offset, log_step,
    lambda_real, lambda_imag, input_map, output_map, skip_gain, forget, initial_state,
    scan_out_weight, attend_out_weight,
):
    parts = layer(
        tokens[0],
        norm_gain[None],
        drive_weight,
        query_weight,
        key_weight,
        value_weight,
        key_offset[:, 0, :],
        log_step[None],
        lambda_real,
        lambda_imag,
        input_map.transpose(0, 1, 3, 2),
        output_map,
        skip_gain.reshape(NY, 128),
        forget.reshape(NY, 8, 128),
        initial_state[:, 0],
        attend_out_weight,
        scan_out_weight,
    )
    return (parts[0].astype(F32) + parts[1].astype(F32)).astype(BF16)[None]


def solution(mesh):
    split = Mesh(
        mesh.devices.reshape(NZ, NY, mesh.shape["fs"], mesh.shape["tp"]),
        ("sp_0", "sp_1", "fs", "tp"),
    )
    in_specs = (
        P("fs", SP_TP, None),
        P(),
        P("fs", "tp"),
        P("fs", "tp"),
        P("fs", "tp"),
        P("fs", "tp"),
        P("tp", "fs", SP),
        P("tp"),
        P("tp", None),
        P("tp", None),
        P(None, "tp", None, None),
        P(None, "tp", None, None),
        P("tp"),
        P("tp", "fs", SP),
        P(None, "fs", "tp", None),
        P("tp", "fs"),
        P("tp", "fs"),
    )
    return jax.shard_map(
        on_device, mesh=split, in_specs=in_specs, out_specs=P("fs", SP_TP, None), check_vma=False
    )
```

```python
import math

import jax
import jax.numpy as jnp
from jax import lax
from jax.experimental import pallas as pl
from jax.experimental.pallas import tpu as pltpu
from jax.sharding import Mesh
from jax.sharding import PartitionSpec as P

SP_TP = ("sp_0", "sp_1", "tp")
SP = ("sp_0", "sp_1")
EPSILON = 1e-06
LOG2E = 1.4426950408889634
NZ, NY, NX, NT = 8, 4, 4, 2
BF16, F32 = jnp.bfloat16, jnp.float32
VMEM = pl.BlockSpec(memory_space=pltpu.VMEM)
MESH_ID = pl.DeviceIdType.MESH


def remote(src, dst, send_sem, recv_sem, where):
    return pltpu.make_async_remote_copy(
        src_ref=src, dst_ref=dst, send_sem=send_sem, recv_sem=recv_sem,
        device_id=where, device_id_type=MESH_ID,
    )


def greet(peers):
    barrier = pltpu.get_barrier_semaphore()
    for peer in peers:
        pl.semaphore_signal(barrier, inc=1, device_id=peer, device_id_type=MESH_ID)


def await_greetings(count):
    pl.semaphore_wait(pltpu.get_barrier_semaphore(), count)


def plane_peers(x, y, t):
    peers = [
        {"fs": (x + dx) % NX, "tp": (t + dt) % NT}
        for dx in range(NX) for dt in range(NT) if (dx, dt) != (0, 0)
    ]
    peers += [
        {"fs": (x + dx) % NX, "sp_1": (y + dy) % NY} for dx in range(NX) for dy in range(1, NY)
    ]
    return peers


def high_low(value):
    high = value.astype(BF16)
    return high, (value - high.astype(F32)).astype(BF16)


def attend_chunk(query, pairs, offset, ladder, visible=None):
    keys, values = pairs[:, :128], pairs[:, 128:]
    score = lax.dot_general(query, keys, (((1,), (1,)), ((), ())), preferred_element_type=F32)
    score = score + offset
    soft = jnp.maximum(score, LOG2E * jnp.log(1.0 + jnp.exp2(jnp.minimum(score, 126.0))))
    if visible is not None:
        soft = jnp.where(visible, soft, 0.0)
    soft = soft.astype(BF16)
    last = jnp.dot(soft[:, 256:], ladder[:, :256], preferred_element_type=F32)
    first = jnp.dot(soft[:, :256], ladder[:, :256], preferred_element_type=F32) + jnp.dot(
        soft[:, 256:], ladder[:, 256:], preferred_element_type=F32
    )
    weight = jnp.exp2(score + jnp.concatenate([first, last], axis=1))
    if visible is not None:
        weight = jnp.where(visible, weight, 0.0)
    return jnp.dot(weight.astype(BF16), values, preferred_element_type=F32), first[:, :128]


def turned(gain, state):
    return gain[0] * state + gain[1] * pltpu.roll(state, 64, 1)


def powers_times(left, right):
    return (
        left[0] * right[0] - left[1] * right[1],
        left[1] * right[0] + left[0] * right[1],
    )


def layer_kernel(
    *refs,
):
    operands, outs, held_here, rest = refs[:17], refs[17:19], refs[19:36], refs[36:]
    run_layer(operands, outs, held_here, *rest)


def run_layer(
    operands, outs, held_here, s_operand,
    normed, rows_in, keyed_w, query_w, drive_w, packed, packed_in, driven_in, queries,
    own_in, right_in, left_in, far_in, offset_own, offset_in, state_own, state_in, acc, tot,
    ladder, into_map, out_map, fwd_p, fwd_q, inv_p, inv_q, held, ends, decay,
    attend_own, scan_own, attend_in, scan_in, part_out, part_in,
    s_rows, r_rows, s_half, r_half, s_weight, r_weight, s_packed, r_packed,
    s_right, r_right, s_left, r_left, s_offset, r_offset, s_state, r_state,
    s_attend, r_attend, s_scan, r_scan, s_part, r_part,
):
    (
        tok, gain_ref, w_drive, w_query, w_key, w_value, key_offset, log_step_ref, lambda_real,
        lambda_imag, input_map, output_map, skip_ref, forget_ref, initial_ref, w_attend, w_scan,
    ) = held_here
    fetches = [
        pltpu.make_async_copy(src, dst, s_operand.at[k])
        for k, (src, dst) in enumerate(zip(operands, held_here))
    ]
    for fetch in fetches:
        fetch.start()
    z, y, x, t = (lax.axis_index(a) for a in ("sp_0", "sp_1", "fs", "tp"))
    greet(plane_peers(x, y, t) + [{"sp_0": (z + dz) % NZ} for dz in range(1, NZ)])
    row = lax.broadcasted_iota(jnp.int32, (128, 128), 0)
    lane = lax.broadcasted_iota(jnp.int32, (128, 128), 1)
    up, down = {"sp_0": (z + 1) % NZ}, {"sp_0": (z + NZ - 1) % NZ}
    sent = []

    def send(copy):
        copy.start()
        sent.append(copy)
        return copy

    for k in (0, 1, 6, 13):
        fetches[k].wait()
    packed[:, :8, :] = forget_ref[...]
    packed[:, 8:, :] = jnp.zeros((NY, 8, 128), F32)
    offsets = key_offset[...].astype(F32) * LOG2E
    for k in range(NY):
        packed[k, 8:9, :] = offsets[k : k + 1]
    values = tok[...].astype(F32)
    scale = lax.rsqrt(jnp.mean(values * values, axis=1, keepdims=True) + EPSILON)
    normed[...] = (values * scale * gain_ref[...]).astype(BF16)
    for k in (2, 3, 4, 5):
        fetches[k].wait()
    await_greetings(26)

    order = (0, 1, 3, 2)
    mine = pl.ds(pl.multiple_of(t * 64, 64), 64)
    sibling = {"tp": 1 - t}

    def row_copy(j):
        return remote(
            normed, rows_in.at[j, mine], s_rows.at[j], r_rows.at[j],
            {"sp_1": (y + order[j]) % NY},
        )

    def half_copy(j):
        return remote(
            rows_in.at[j, mine] if j else normed, rows_in.at[j, mine], s_half.at[j], r_half.at[j],
            sibling,
        )

    column = pl.ds(pl.multiple_of(y * 128, 128), 128)
    depth = pl.ds(pl.multiple_of(x * 512, 512), 512)
    sources = (w_key, w_value, w_query, w_drive)
    targets = (
        keyed_w.at[depth, :128], keyed_w.at[depth, 128:], query_w.at[depth], drive_w.at[depth]
    )

    def weight_copy(kind, dx):
        return remote(
            sources[kind].at[:, column], targets[kind], s_weight.at[kind, dx],
            r_weight.at[kind, dx], {"fs": (x + dx) % NX},
        )

    packed_copies = [
        send(
            remote(
                packed.at[(y + dy) % NY], packed_in.at[y], s_packed.at[dy], r_packed.at[dy],
                {"sp_1": (y + dy) % NY},
            )
        )
        for dy in range(1, NY)
    ]
    send(half_copy(0))
    for j in (1, 2, 3):
        send(row_copy(j))
    for kind in range(4):
        for dx in (1, 3, 2):
            send(weight_copy(kind, dx))
    packed_in[y] = packed[y]
    rows_in[0, mine] = normed[...]
    keyed_w[depth, :128] = w_key[:, column]
    keyed_w[depth, 128:] = w_value[:, column]
    query_w[depth] = w_query[:, column]
    drive_w[depth] = w_drive[:, column]

    for k in (7, 8, 9, 10, 11, 12, 14, 15, 16):
        fetches[k].wait()
    sign = jnp.where(lane[:8] < 64, -1.0, 1.0)
    groups = pl.ds(pl.multiple_of(y * 8, 8), 8)

    def side_by_side(left, right):
        return jnp.concatenate([left, right], axis=1)

    lam_real = side_by_side(lambda_real[groups, :], lambda_real[groups, :])
    lam_imag = side_by_side(lambda_imag[groups, :], lambda_imag[groups, :])
    initial = side_by_side(initial_ref[0, groups, :], initial_ref[1, groups, :])
    spot = lax.broadcasted_iota(jnp.int32, (8, 32), 1) - lax.broadcasted_iota(
        jnp.int32, (8, 32), 0
    )
    step = jnp.exp(
        jnp.sum(jnp.where(spot == y * 8, log_step_ref[...], 0.0), axis=1, keepdims=True)
    )
    log_gain, rotate = lam_real * step, lam_imag * step
    cosine, sine, magnitude = jnp.cos(rotate), jnp.sin(rotate), jnp.exp(log_gain)
    bar_real, bar_imag = magnitude * cosine, magnitude * sine
    divisor = lam_real * lam_real + lam_imag * lam_imag
    shifted = bar_real - 1.0
    factor_real = (shifted * lam_real + bar_imag * lam_imag) / divisor
    factor_imag = (bar_imag * lam_real - shifted * lam_imag) / divisor * sign
    shrink = jnp.exp(-log_gain)
    gain = (bar_real, sign * bar_imag)
    inverse = (shrink * cosine, -sign * shrink * sine)
    gains, inverses = [gain], [inverse]
    for _ in range(9):
        gains.append(powers_times(gains[-1], gains[-1]))
    for _ in range(6):
        inverses.append(powers_times(inverses[-1], inverses[-1]))
    gain_block, gain_all = gains[7], gains[9]
    gain_last = powers_times(gain_block, inverse)
    into_map[...] = jnp.zeros_like(into_map)
    out_map[...] = jnp.zeros_like(out_map)
    for g in range(8):
        cols, swapped = pl.ds(g * 128, 128), pl.ds(1024 + g * 128, 128)
        raw = side_by_side(input_map[0, y * 8 + g], input_map[1, y * 8 + g])
        entry = factor_real[g : g + 1] * raw + factor_imag[g : g + 1] * pltpu.roll(raw, 64, 1)
        turned_entry = pltpu.roll(entry, 64, 1)
        for at in (g * 16, 128 + g * 16):
            into_map[at : at + 16, cols] = entry.astype(BF16)
            into_map[at : at + 16, swapped] = turned_entry.astype(BF16)
        raw = side_by_side(output_map[0, y * 8 + g], output_map[1, y * 8 + g])
        out_map[g * 16 : g * 16 + 16, cols] = (raw * -sign[:1]).astype(BF16)
        out_map[g * 16 : g * 16 + 16, swapped] = (pltpu.roll(raw, 64, 1) * -sign[:1]).astype(BF16)
        for table_p, table_q, steps in ((fwd_p, fwd_q, gains), (inv_p, inv_q, inverses)):
            real, imag = jnp.ones((8, 128), F32), jnp.zeros((8, 128), F32)
            for bit in range(3):
                by = tuple(part[g : g + 1] for part in steps[bit])
                new = powers_times((real, imag), by)
                chosen = (row[:8] & (1 << bit)) != 0
                real, imag = jnp.where(chosen, new[0], real), jnp.where(chosen, new[1], imag)
            table_p[:8, cols] = real
            table_q[:8, cols] = imag
            for bit in range(3, 7):
                n = 1 << bit
                by = tuple(part[g : g + 1] for part in steps[bit])
                new = powers_times((table_p[:n, cols], table_q[:n, cols]), by)
                table_p[n : 2 * n, cols] = new[0]
                table_q[n : 2 * n, cols] = new[1]
    ladder_row = lax.broadcasted_iota(jnp.int32, (256, 512), 0)
    ladder_lane = lax.broadcasted_iota(jnp.int32, (256, 512), 1)
    ladder[...] = jnp.where((ladder_lane >= 256) | (ladder_row >= ladder_lane), -1.0, 0.0).astype(
        BF16
    )

    def block_of(j):
        dy = j + j // 2 * (5 - 2 * j)
        return (y + NY - dy) % NY

    def right_copy(i, j):
        b = block_of(j)
        return remote(
            own_in.at[b] if i == 1 else right_in.at[i - 2, b],
            far_in.at[b] if i == 4 else right_in.at[i - 1, b],
            s_right.at[i - 1, j], r_right.at[i - 1, j], up,
        )

    def left_copy(i, j):
        b = block_of(j)
        return remote(
            own_in.at[b] if i == 1 else left_in.at[i - 2, b],
            far_in.at[b] if i == 4 else left_in.at[i - 1, b],
            s_left.at[i - 1, j], r_left.at[i - 1, j], down,
        )

    for copy in packed_copies:
        copy.wait_recv()
    for b in range(NY):
        offset_own[b : b + 1, :] = packed_in[b, 8:9, :]
        offset_in[0, b : b + 1, :] = packed_in[b, 8:9, :]
    offset_own[4:8, :] = jnp.zeros((4, 128), F32)
    offset_copies = [
        send(
            remote(
                offset_own, offset_in.at[dz], s_offset.at[dz], r_offset.at[dz],
                {"sp_0": (z + dz) % NZ},
            )
        )
        for dz in range(1, NZ)
    ]
    for j in (1, 2, 3):
        row_copy(j).wait_recv()
        send(half_copy(j))
    for kind in (0, 1):
        for dx in (1, 3, 2):
            weight_copy(kind, dx).wait_recv()
    for j in range(NY):
        half_copy(j).wait_recv()
    product = jnp.dot(
        rows_in[...].reshape(512, 2048), keyed_w[...], preferred_element_type=F32
    ).astype(BF16)
    for j in range(NY):
        own_in[block_of(j)] = product[j * 128 : (j + 1) * 128]
        right_copy(1, j).start()
        left_copy(1, j).start()
    until = jnp.where(lane <= row, 1.0, 0.0)
    until_half = until.astype(BF16)
    falls = []
    for b in range(NY):
        forget = packed_in[b, :8, :]
        spread = jnp.concatenate(
            [jnp.broadcast_to(forget[g : g + 1], (16, 128)) for g in range(8)], axis=0
        )
        decay[b] = lax.dot_general(
            until, spread, (((1,), (1,)), ((), ())), preferred_element_type=F32,
            precision=lax.Precision.HIGHEST,
        )
        falls.append(jnp.sum(forget, axis=1, keepdims=True))
    for dx in (1, 3, 2):
        weight_copy(2, dx).wait_recv()
    product = jnp.dot(
        rows_in[...].reshape(512, 2048), query_w[...], preferred_element_type=F32
    )
    product = (product * (LOG2E * 128**-0.5)).astype(BF16)
    for j in range(NY):
        queries[block_of(j)] = product[j * 128 : (j + 1) * 128]

    def arrive(i):
        for j in range(NY):
            if i < 4 or j < 2:
                right_copy(i, j).wait_recv()
                if i < 3 or i == 3 and j < 2:
                    right_copy(i + 1, j).start()
            if i < 4 or j >= 2:
                left_copy(i, j).wait_recv()
                if i < 3 or i == 3 and j >= 2:
                    left_copy(i + 1, j).start()

    def offset_row(dz):
        return jnp.concatenate([offset_in[dz, b : b + 1, :] for b in range(NY)], axis=1)

    def attend_far(dz, pairs):
        @pl.when(z >= dz)
        def _():
            acc[dz], tot[dz] = attend_chunk(
                queries[...].reshape(512, 128), pairs[...].reshape(512, 256), offset_row(dz),
                ladder[...],
            )

    def attend_step(i):
        attend_far(i, right_in.at[i - 1])
        attend_far(8 - i, left_in.at[i - 1])

    acc[0], tot[0] = attend_chunk(
        queries[...].reshape(512, 128), own_in[...].reshape(512, 256), offset_row(0), ladder[...],
        lax.broadcasted_iota(jnp.int32, (512, 512), 1)
        < lax.broadcasted_iota(jnp.int32, (512, 512), 0),
    )
    arrive(1)
    for copy in offset_copies:
        copy.wait_recv()
    attend_step(1)

    for dx in (1, 3, 2):
        weight_copy(3, dx).wait_recv()
    product = jnp.dot(
        rows_in[...].reshape(512, 2048), drive_w[...], preferred_element_type=F32
    ).astype(BF16)
    for j in range(NY):
        driven_in[block_of(j)] = product[j * 128 : (j + 1) * 128]
    local = jnp.zeros((8, 128), F32)
    fall_all = jnp.zeros((8, 1), F32)
    for b in range(NY):
        driven = driven_in[b].astype(F32) * jnp.exp(-decay[b])
        entered = jnp.dot(
            jnp.concatenate(high_low(driven), axis=1), into_map[...], preferred_element_type=F32
        )
        unturned = entered[:, :1024] * inv_p[...] + entered[:, 1024:] * inv_q[...]
        high, low = high_low(unturned)
        held[b] = jnp.dot(until_half, high, preferred_element_type=F32) + jnp.dot(
            until_half, low, preferred_element_type=F32
        )
        for g in range(8):
            ends[b, g : g + 1, :] = held[b, 127:128, g * 128 : (g + 1) * 128]
        fall_all = fall_all + falls[b]
        falls[b] = jnp.exp(falls[b])
        ends[b] = falls[b] * turned(gain_last, ends[b])
        local = falls[b] * turned(gain_block, local) + ends[b]
    state_own[:8, :] = local
    state_own[8:, :] = jnp.broadcast_to(fall_all, (8, 128))
    state_copies = [
        send(
            remote(
                state_own, state_in.at[dz], s_state.at[dz], r_state.at[dz],
                {"sp_0": (z + dz) % NZ},
            )
        )
        for dz in range(1, NZ)
    ]

    arrive(2)
    attend_step(2)
    arrive(3)

    for copy in state_copies:
        copy.wait_recv()
    carry = initial
    for source in range(NZ - 1):
        arrived = state_in[jnp.maximum(z - source, 1)]
        moved = jnp.exp(arrived[8:]) * turned(gain_all, carry) + arrived[:8]
        carry = jnp.where(source < z, moved, carry)
    for b in range(NY):
        entering = turned(gain, carry)
        whole = jnp.concatenate(
            [held[b, :, g * 128 : (g + 1) * 128] + entering[g : g + 1] for g in range(8)], axis=1
        )
        turned_states = jnp.concatenate(
            [(whole * fwd_p[...]).astype(BF16), (whole * fwd_q[...]).astype(BF16)], axis=1
        )
        read = lax.dot_general(
            turned_states, out_map[...], (((1,), (1,)), ((), ())), preferred_element_type=F32
        )
        read = read * jnp.exp(decay[b]) + skip_ref[pl.ds(y, 1), :] * driven_in[b].astype(F32)
        inner = math.sqrt(2.0 / math.pi) * (read + 0.044715 * (read * read * read))
        scan_own[b] = (0.5 * read * (1.0 + jnp.tanh(inner))).astype(BF16)
        carry = falls[b] * turned(gain_block, carry) + ends[b]

    def spread_copies(own, landing, s_sem, r_sem):
        return {
            (dx, dy): remote(
                own.at[(y + dy) % NY], landing.at[dx, dy], s_sem.at[dx, dy], r_sem.at[dx, dy],
                {"fs": (x + dx) % NX, "sp_1": (y + dy) % NY},
            )
            for dx in order for dy in (1, 3, 2, 0) if (dx, dy) != (0, 0)
        }

    scan_copies = spread_copies(scan_own, scan_in, s_scan, r_scan)
    for copy in scan_copies.values():
        send(copy)
    scan_in[0, 0] = scan_own[y]
    attend_step(3)
    arrive(4)
    attend_far(4, far_in)
    for dz in range(1, NZ):
        @pl.when(z >= dz)
        def _():
            fallen = tot[0, :, :1]
            acc[0] += jnp.exp2(fallen) * acc[dz]
            tot[0, :, :1] = fallen + tot[dz, :, :1]

    attend_own[...] = acc[0].astype(BF16).reshape(NY, 128, 128)
    attend_copies = spread_copies(attend_own, attend_in, s_attend, r_attend)
    for copy in attend_copies.values():
        send(copy)
    attend_in[0, 0] = attend_own[y]

    part_copies = {}
    for dx in order:
        total = None
        for dy in range(NY):
            if (dx, dy) != (0, 0):
                scan_copies[dx, dy].wait_recv()
                attend_copies[dx, dy].wait_recv()
            head = (y + NY - dy) % NY
            head_rows = pl.ds(pl.multiple_of(head * 128, 128), 128)
            product = jnp.dot(
                attend_in[dx, dy], w_attend[head_rows, :], preferred_element_type=F32
            ) + jnp.dot(scan_in[dx, dy], w_scan[head_rows, :], preferred_element_type=F32)
            total = product if total is None else total + product
        rounded = total.astype(BF16)
        for k in range(NT):
            part_out[dx, k] = rounded[k * 64 : (k + 1) * 64]
        for dt in range(NT):
            if (dx, dt) != (0, 0):
                to = (t + dt) % NT
                part_copies[dx, dt] = send(
                    remote(
                        part_out.at[dx, to], part_in.at[dx, dt], s_part.at[dx, dt],
                        r_part.at[dx, dt], {"fs": (x + NX - dx) % NX, "tp": to},
                    )
                )
    part_in[0, 0] = part_out[0, t]
    for dx in order:
        for dt in range(NT):
            if (dx, dt) != (0, 0):
                part_copies[dx, dt].wait_recv()
        columns = pl.ds(pl.multiple_of((x + dx) % NX * 512, 512), 512)
        for dt in range(NT):
            outs[dt][:, columns] = part_in[dx, dt]
    for copy in sent:
        copy.wait_send()
    for i in range(1, 5):
        for j in range(NY):
            if i < 4 or j < 2:
                right_copy(i, j).wait_send()
            if i < 4 or j >= 2:
                left_copy(i, j).wait_send()


def layer(*operands):
    def sems(*shape):
        return [pltpu.SemaphoreType.DMA(shape)] * 2

    return pl.pallas_call(
        layer_kernel,
        out_shape=[jax.ShapeDtypeStruct((64, 2048), BF16)] * NT,
        in_specs=[pl.BlockSpec(memory_space=pl.ANY)] * 17,
        out_specs=[VMEM] * NT,
        scratch_shapes=[
            *(pltpu.VMEM(operand.shape, operand.dtype) for operand in operands),
            pltpu.SemaphoreType.DMA((17,)),
            pltpu.VMEM((64, 2048), BF16),
            pltpu.VMEM((NY, 128, 2048), BF16),
            pltpu.VMEM((2048, 256), BF16),
            pltpu.VMEM((2048, 128), BF16),
            pltpu.VMEM((2048, 128), BF16),
            pltpu.VMEM((NY, 16, 128), F32),
            pltpu.VMEM((NY, 16, 128), F32),
            pltpu.VMEM((NY, 128, 128), BF16),
            pltpu.VMEM((NY, 128, 128), BF16),
            pltpu.VMEM((NY, 128, 256), BF16),
            pltpu.VMEM((3, NY, 128, 256), BF16),
            pltpu.VMEM((3, NY, 128, 256), BF16),
            pltpu.VMEM((NY, 128, 256), BF16),
            pltpu.VMEM((8, 128), F32),
            pltpu.VMEM((NZ, 8, 128), F32),
            pltpu.VMEM((16, 128), F32),
            pltpu.VMEM((NZ, 16, 128), F32),
            pltpu.VMEM((NZ, 512, 128), F32),
            pltpu.VMEM((NZ, 512, 128), F32),
            pltpu.VMEM((256, 512), BF16),
            pltpu.VMEM((256, 2048), BF16),
            pltpu.VMEM((128, 2048), BF16),
            pltpu.VMEM((128, 1024), F32),
            pltpu.VMEM((128, 1024), F32),
            pltpu.VMEM((128, 1024), F32),
            pltpu.VMEM((128, 1024), F32),
            pltpu.VMEM((NY, 128, 1024), F32),
            pltpu.VMEM((NY, 8, 128), F32),
            pltpu.VMEM((NY, 128, 128), F32),
            pltpu.VMEM((NY, 128, 128), BF16),
            pltpu.VMEM((NY, 128, 128), BF16),
            pltpu.VMEM((NX, NY, 128, 128), BF16),
            pltpu.VMEM((NX, NY, 128, 128), BF16),
            pltpu.VMEM((NX, NT, 64, 512), BF16),
            pltpu.VMEM((NX, NT, 64, 512), BF16),
            *sems(NY), *sems(NY), *sems(4, NX), *sems(NY), *sems(4, NY), *sems(4, NY), *sems(NZ),
            *sems(NZ), *sems(NX, NY), *sems(NX, NY), *sems(NX, NT),
        ],
        compiler_params=pltpu.CompilerParams(
            collective_id=0, has_side_effects=True, vmem_limit_bytes=60 << 20
        ),
        name="layer",
    )(*operands)


def on_device(
    tokens, norm_gain, drive_weight, query_weight, key_weight, value_weight, key_offset, log_step,
    lambda_real, lambda_imag, input_map, output_map, skip_gain, forget, initial_state,
    scan_out_weight, attend_out_weight,
):
    parts = layer(
        tokens[0],
        norm_gain[None],
        drive_weight,
        query_weight,
        key_weight,
        value_weight,
        key_offset[:, 0, :],
        log_step[None],
        lambda_real,
        lambda_imag,
        input_map.transpose(0, 1, 3, 2),
        output_map,
        skip_gain.reshape(NY, 128),
        forget.reshape(NY, 8, 128),
        initial_state[:, 0],
        attend_out_weight,
        scan_out_weight,
    )
    return (parts[0].astype(F32) + parts[1].astype(F32)).astype(BF16)[None]


def solution(mesh):
    split = Mesh(
        mesh.devices.reshape(NZ, NY, mesh.shape["fs"], mesh.shape["tp"]),
        ("sp_0", "sp_1", "fs", "tp"),
    )
    in_specs = (
        P("fs", SP_TP, None),
        P(),
        P("fs", "tp"),
        P("fs", "tp"),
        P("fs", "tp"),
        P("fs", "tp"),
        P("tp", "fs", SP),
        P("tp"),
        P("tp", None),
        P("tp", None),
        P(None, "tp", None, None),
        P(None, "tp", None, None),
        P("tp"),
        P("tp", "fs", SP),
        P(None, "fs", "tp", None),
        P("tp", "fs"),
        P("tp", "fs"),
    )
    return jax.shard_map(
        on_device, mesh=split, in_specs=in_specs, out_specs=P("fs", SP_TP, None), check_vma=False
    )
```

```python
import math

import jax
import jax.numpy as jnp
from jax import lax
from jax.experimental import pallas as pl
from jax.experimental.pallas import tpu as pltpu
from jax.sharding import Mesh
from jax.sharding import PartitionSpec as P

SP_TP = ("sp_0", "sp_1", "tp")
SP = ("sp_0", "sp_1")
EPSILON = 1e-06
LOG2E = 1.4426950408889634
NZ, NY, NX, NT = 8, 4, 4, 2
BF16, F32 = jnp.bfloat16, jnp.float32
VMEM = pl.BlockSpec(memory_space=pltpu.VMEM)
MESH_ID = pl.DeviceIdType.MESH


def remote(src, dst, send_sem, recv_sem, where):
    return pltpu.make_async_remote_copy(
        src_ref=src, dst_ref=dst, send_sem=send_sem, recv_sem=recv_sem,
        device_id=where, device_id_type=MESH_ID,
    )


def greet(peers):
    barrier = pltpu.get_barrier_semaphore()
    for peer in peers:
        pl.semaphore_signal(barrier, inc=1, device_id=peer, device_id_type=MESH_ID)


def await_greetings(count):
    pl.semaphore_wait(pltpu.get_barrier_semaphore(), count)


def plane_peers(x, y, t):
    peers = [
        {"fs": (x + dx) % NX, "tp": (t + dt) % NT}
        for dx in range(NX) for dt in range(NT) if (dx, dt) != (0, 0)
    ]
    peers += [
        {"fs": (x + dx) % NX, "sp_1": (y + dy) % NY} for dx in range(NX) for dy in range(1, NY)
    ]
    return peers


def high_low(value):
    high = value.astype(BF16)
    return high, (value - high.astype(F32)).astype(BF16)


def attend_chunk(query, pairs, offset, ladder, visible=None):
    keys, values = pairs[:, :128], pairs[:, 128:]
    score = lax.dot_general(query, keys, (((1,), (1,)), ((), ())), preferred_element_type=F32)
    score = score + offset
    soft = jnp.maximum(score, LOG2E * jnp.log(1.0 + jnp.exp2(jnp.minimum(score, 126.0))))
    if visible is not None:
        soft = jnp.where(visible, soft, 0.0)
    soft = soft.astype(BF16)
    last = jnp.dot(soft[:, 256:], ladder[:, :256], preferred_element_type=F32)
    first = jnp.dot(soft[:, :256], ladder[:, :256], preferred_element_type=F32) + jnp.dot(
        soft[:, 256:], ladder[:, 256:], preferred_element_type=F32
    )
    weight = jnp.exp2(score + jnp.concatenate([first, last], axis=1))
    if visible is not None:
        weight = jnp.where(visible, weight, 0.0)
    return jnp.dot(weight.astype(BF16), values, preferred_element_type=F32), first[:, :128]


def turned(gain, state):
    return gain[0] * state + gain[1] * pltpu.roll(state, 64, 1)


def powers_times(left, right):
    return (
        left[0] * right[0] - left[1] * right[1],
        left[1] * right[0] + left[0] * right[1],
    )


def layer_kernel(
    *refs,
):
    operands, out, held_here, rest = refs[:17], refs[17], refs[18:35], refs[35:]
    run_layer(operands, out, held_here, *rest)


def run_layer(
    operands, out, held_here, s_operand,
    normed, rows_in, keyed_w, query_w, drive_w, packed, packed_in, driven_in, queries,
    own_in, right_in, left_in, far_in, offset_own, offset_in, state_own, state_in, acc, tot,
    ladder, into_map, out_map, fwd_p, fwd_q, inv_p, inv_q, held, ends, decay,
    attend_own, scan_own, attend_in, scan_in, part_out, part_in, product_own, half_out, half_in,
    s_rows, r_rows, s_half, r_half, s_weight, r_weight, s_packed, r_packed,
    s_right, r_right, s_left, r_left, s_offset, r_offset, s_state, r_state,
    s_scan, r_scan, s_part, r_part, s_slice, r_slice, s_relay, r_relay, s_attend, r_attend,
    s_last, r_last,
):
    (
        tok, gain_ref, w_drive, w_query, w_key, w_value, key_offset, log_step_ref, lambda_real,
        lambda_imag, input_map, output_map, skip_ref, forget_ref, initial_ref, w_attend, w_scan,
    ) = held_here
    z, y, x, t = (lax.axis_index(a) for a in ("sp_0", "sp_1", "fs", "tp"))
    fetches = [
        pltpu.make_async_copy(src, dst.at[x] if k == 15 else dst, s_operand.at[k])
        for k, (src, dst) in enumerate(zip(operands, held_here))
    ]
    for fetch in fetches:
        fetch.start()
    greet(plane_peers(x, y, t) + [{"sp_0": (z + dz) % NZ} for dz in range(1, NZ)])
    row = lax.broadcasted_iota(jnp.int32, (128, 128), 0)
    lane = lax.broadcasted_iota(jnp.int32, (128, 128), 1)
    up, down = {"sp_0": (z + 1) % NZ}, {"sp_0": (z + NZ - 1) % NZ}
    sent = []

    def send(copy):
        copy.start()
        sent.append(copy)
        return copy

    for k in (0, 1, 6, 13):
        fetches[k].wait()
    packed[:, :8, :] = forget_ref[...]
    packed[:, 8:, :] = jnp.zeros((NY, 8, 128), F32)
    offsets = key_offset[...].astype(F32) * LOG2E
    for k in range(NY):
        packed[k, 8:9, :] = offsets[k : k + 1]
    values = tok[...].astype(F32)
    scale = lax.rsqrt(jnp.mean(values * values, axis=1, keepdims=True) + EPSILON)
    normed[...] = (values * scale * gain_ref[...]).astype(BF16)
    for k in (2, 3, 4, 5, 15):
        fetches[k].wait()
    await_greetings(26)

    order = (0, 1, 3, 2)
    mine = pl.ds(pl.multiple_of(t * 64, 64), 64)
    sibling = {"tp": 1 - t}

    def row_copy(j):
        return remote(
            normed, rows_in.at[j, mine], s_rows.at[j], r_rows.at[j],
            {"sp_1": (y + order[j]) % NY},
        )

    def half_copy(j):
        return remote(
            rows_in.at[j, mine] if j else normed, rows_in.at[j, mine], s_half.at[j], r_half.at[j],
            sibling,
        )

    column = pl.ds(pl.multiple_of(y * 128, 128), 128)
    depth = pl.ds(pl.multiple_of(x * 512, 512), 512)
    sources = (w_key, w_value, w_query, w_drive)
    targets = (
        keyed_w.at[depth, :128], keyed_w.at[depth, 128:], query_w.at[depth], drive_w.at[depth]
    )

    def weight_copy(kind, dx):
        return remote(
            sources[kind].at[:, column], targets[kind], s_weight.at[kind, dx],
            r_weight.at[kind, dx], {"fs": (x + dx) % NX},
        )

    def slice_copy(dx):
        return remote(
            w_attend.at[x, column], w_attend.at[x, column], s_slice.at[dx], r_slice.at[dx],
            {"fs": (x + dx) % NX},
        )

    def relay_copy(dx, dy):
        part = w_attend.at[(x + NX - dx) % NX, column]
        return remote(
            part, part, s_relay.at[dx, dy], r_relay.at[dx, dy], {"sp_1": (y + dy) % NY}
        )

    packed_copies = [
        send(
            remote(
                packed.at[(y + dy) % NY], packed_in.at[y], s_packed.at[dy], r_packed.at[dy],
                {"sp_1": (y + dy) % NY},
            )
        )
        for dy in range(1, NY)
    ]
    send(half_copy(0))
    for j in (1, 2, 3):
        send(row_copy(j))
    for kind in (0, 1, None, 3, 2):
        for dx in (1, 3, 2):
            send(slice_copy(dx) if kind is None else weight_copy(kind, dx))
    packed_in[y] = packed[y]
    rows_in[0, mine] = normed[...]
    keyed_w[depth, :128] = w_key[:, column]
    keyed_w[depth, 128:] = w_value[:, column]
    query_w[depth] = w_query[:, column]
    drive_w[depth] = w_drive[:, column]

    for k in (7, 8, 9, 10, 11, 12, 14, 16):
        fetches[k].wait()
    sign = jnp.where(lane[:8] < 64, -1.0, 1.0)
    groups = pl.ds(pl.multiple_of(y * 8, 8), 8)

    def side_by_side(left, right):
        return jnp.concatenate([left, right], axis=1)

    lam_real = side_by_side(lambda_real[groups, :], lambda_real[groups, :])
    lam_imag = side_by_side(lambda_imag[groups, :], lambda_imag[groups, :])
    initial = side_by_side(initial_ref[0, groups, :], initial_ref[1, groups, :])
    spot = lax.broadcasted_iota(jnp.int32, (8, 32), 1) - lax.broadcasted_iota(
        jnp.int32, (8, 32), 0
    )
    step = jnp.exp(
        jnp.sum(jnp.where(spot == y * 8, log_step_ref[...], 0.0), axis=1, keepdims=True)
    )
    log_gain, rotate = lam_real * step, lam_imag * step
    cosine, sine, magnitude = jnp.cos(rotate), jnp.sin(rotate), jnp.exp(log_gain)
    bar_real, bar_imag = magnitude * cosine, magnitude * sine
    divisor = lam_real * lam_real + lam_imag * lam_imag
    shifted = bar_real - 1.0
    factor_real = (shifted * lam_real + bar_imag * lam_imag) / divisor
    factor_imag = (bar_imag * lam_real - shifted * lam_imag) / divisor * sign
    shrink = jnp.exp(-log_gain)
    gain = (bar_real, sign * bar_imag)
    inverse = (shrink * cosine, -sign * shrink * sine)
    gains, inverses = [gain], [inverse]
    for _ in range(9):
        gains.append(powers_times(gains[-1], gains[-1]))
    for _ in range(6):
        inverses.append(powers_times(inverses[-1], inverses[-1]))
    gain_block, gain_all = gains[7], gains[9]
    gain_last = powers_times(gain_block, inverse)
    into_map[...] = jnp.zeros_like(into_map)
    out_map[...] = jnp.zeros_like(out_map)
    for g in range(8):
        cols, swapped = pl.ds(g * 128, 128), pl.ds(1024 + g * 128, 128)
        raw = side_by_side(input_map[0, y * 8 + g], input_map[1, y * 8 + g])
        entry = factor_real[g : g + 1] * raw + factor_imag[g : g + 1] * pltpu.roll(raw, 64, 1)
        turned_entry = pltpu.roll(entry, 64, 1)
        for at in (g * 16, 128 + g * 16):
            into_map[at : at + 16, cols] = entry.astype(BF16)
            into_map[at : at + 16, swapped] = turned_entry.astype(BF16)
        raw = side_by_side(output_map[0, y * 8 + g], output_map[1, y * 8 + g])
        out_map[g * 16 : g * 16 + 16, cols] = (raw * -sign[:1]).astype(BF16)
        out_map[g * 16 : g * 16 + 16, swapped] = (pltpu.roll(raw, 64, 1) * -sign[:1]).astype(BF16)
        for table_p, table_q, steps in ((fwd_p, fwd_q, gains), (inv_p, inv_q, inverses)):
            real, imag = jnp.ones((8, 128), F32), jnp.zeros((8, 128), F32)
            for bit in range(3):
                by = tuple(part[g : g + 1] for part in steps[bit])
                new = powers_times((real, imag), by)
                chosen = (row[:8] & (1 << bit)) != 0
                real, imag = jnp.where(chosen, new[0], real), jnp.where(chosen, new[1], imag)
            table_p[:8, cols] = real
            table_q[:8, cols] = imag
            for bit in range(3, 7):
                n = 1 << bit
                by = tuple(part[g : g + 1] for part in steps[bit])
                new = powers_times((table_p[:n, cols], table_q[:n, cols]), by)
                table_p[n : 2 * n, cols] = new[0]
                table_q[n : 2 * n, cols] = new[1]
    ladder_row = lax.broadcasted_iota(jnp.int32, (256, 512), 0)
    ladder_lane = lax.broadcasted_iota(jnp.int32, (256, 512), 1)
    ladder[...] = jnp.where((ladder_lane >= 256) | (ladder_row >= ladder_lane), -1.0, 0.0).astype(
        BF16
    )

    def block_of(j):
        dy = j + j // 2 * (5 - 2 * j)
        return (y + NY - dy) % NY

    def right_copy(i, j):
        b = block_of(j)
        return remote(
            own_in.at[b] if i == 1 else right_in.at[i - 2, b],
            far_in.at[b] if i == 4 else right_in.at[i - 1, b],
            s_right.at[i - 1, j], r_right.at[i - 1, j], up,
        )

    def left_copy(i, j):
        b = block_of(j)
        return remote(
            own_in.at[b] if i == 1 else left_in.at[i - 2, b],
            far_in.at[b] if i == 4 else left_in.at[i - 1, b],
            s_left.at[i - 1, j], r_left.at[i - 1, j], down,
        )

    for copy in packed_copies:
        copy.wait_recv()
    for b in range(NY):
        offset_own[b : b + 1, :] = packed_in[b, 8:9, :]
        offset_in[0, b : b + 1, :] = packed_in[b, 8:9, :]
    offset_own[4:8, :] = jnp.zeros((4, 128), F32)
    offset_copies = [
        send(
            remote(
                offset_own, offset_in.at[dz], s_offset.at[dz], r_offset.at[dz],
                {"sp_0": (z + dz) % NZ},
            )
        )
        for dz in range(1, NZ)
    ]
    for j in (1, 2, 3):
        row_copy(j).wait_recv()
        send(half_copy(j))
    for kind in (0, 1):
        for dx in (1, 3, 2):
            weight_copy(kind, dx).wait_recv()
    for j in range(NY):
        half_copy(j).wait_recv()
    product = jnp.dot(
        rows_in[...].reshape(512, 2048), keyed_w[...], preferred_element_type=F32
    ).astype(BF16)
    for j in range(NY):
        own_in[block_of(j)] = product[j * 128 : (j + 1) * 128]
        right_copy(1, j).start()
        left_copy(1, j).start()
    until = jnp.where(lane <= row, 1.0, 0.0)
    until_half = until.astype(BF16)
    falls = []
    for b in range(NY):
        forget = packed_in[b, :8, :]
        spread = jnp.concatenate(
            [jnp.broadcast_to(forget[g : g + 1], (16, 128)) for g in range(8)], axis=0
        )
        decay[b] = lax.dot_general(
            until, spread, (((1,), (1,)), ((), ())), preferred_element_type=F32,
            precision=lax.Precision.HIGHEST,
        )
        falls.append(jnp.sum(forget, axis=1, keepdims=True))
    for dx in (1, 3, 2):
        slice_copy(dx).wait_recv()
        for dy in (1, 3, 2):
            send(relay_copy(dx, dy))

    def arrive(i, blocks=range(NY)):
        for j in blocks:
            if i < 4 or j < 2:
                right_copy(i, j).wait_recv()
                if i < 3 or i == 3 and j < 2:
                    right_copy(i + 1, j).start()
            if i < 4 or j >= 2:
                left_copy(i, j).wait_recv()
                if i < 3 or i == 3 and j >= 2:
                    left_copy(i + 1, j).start()

    def offset_row(dz):
        return jnp.concatenate([offset_in[dz, b : b + 1, :] for b in range(NY)], axis=1)

    def attend_far(dz, pairs):
        @pl.when(z >= dz)
        def _():
            acc[dz], tot[dz] = attend_chunk(
                queries[...].reshape(512, 128), pairs[...].reshape(512, 256), offset_row(dz),
                ladder[...],
            )

    def attend_step(i):
        attend_far(i, right_in.at[i - 1])
        attend_far(8 - i, left_in.at[i - 1])

    arrive(1)

    for dx in (1, 3, 2):
        weight_copy(3, dx).wait_recv()
    product = jnp.dot(
        rows_in[...].reshape(512, 2048), drive_w[...], preferred_element_type=F32
    ).astype(BF16)
    for j in range(NY):
        driven_in[block_of(j)] = product[j * 128 : (j + 1) * 128]
    local = jnp.zeros((8, 128), F32)
    fall_all = jnp.zeros((8, 1), F32)
    for b in range(NY):
        driven = driven_in[b].astype(F32) * jnp.exp(-decay[b])
        entered = jnp.dot(
            jnp.concatenate(high_low(driven), axis=1), into_map[...], preferred_element_type=F32
        )
        unturned = entered[:, :1024] * inv_p[...] + entered[:, 1024:] * inv_q[...]
        high, low = high_low(unturned)
        held[b] = jnp.dot(until_half, high, preferred_element_type=F32) + jnp.dot(
            until_half, low, preferred_element_type=F32
        )
        for g in range(8):
            ends[b, g : g + 1, :] = held[b, 127:128, g * 128 : (g + 1) * 128]
        fall_all = fall_all + falls[b]
        falls[b] = jnp.exp(falls[b])
        ends[b] = falls[b] * turned(gain_last, ends[b])
        local = falls[b] * turned(gain_block, local) + ends[b]
        arrive(2, (b,))
    state_own[:8, :] = local
    state_own[8:, :] = jnp.broadcast_to(fall_all, (8, 128))
    state_copies = [
        send(
            remote(
                state_own, state_in.at[dz], s_state.at[dz], r_state.at[dz],
                {"sp_0": (z + dz) % NZ},
            )
        )
        for dz in range(1, NZ)
    ]

    for dx in (1, 3, 2):
        weight_copy(2, dx).wait_recv()
    product = jnp.dot(
        rows_in[...].reshape(512, 2048), query_w[...], preferred_element_type=F32
    )
    product = (product * (LOG2E * 128**-0.5)).astype(BF16)
    for j in range(NY):
        queries[block_of(j)] = product[j * 128 : (j + 1) * 128]

    acc[0], tot[0] = attend_chunk(
        queries[...].reshape(512, 128), own_in[...].reshape(512, 256), offset_row(0), ladder[...],
        lax.broadcasted_iota(jnp.int32, (512, 512), 1)
        < lax.broadcasted_iota(jnp.int32, (512, 512), 0),
    )
    for copy in offset_copies:
        copy.wait_recv()
    arrive(3, (0, 1))

    for copy in state_copies:
        copy.wait_recv()
    carry = initial
    for source in range(NZ - 1):
        arrived = state_in[jnp.maximum(z - source, 1)]
        moved = jnp.exp(arrived[8:]) * turned(gain_all, carry) + arrived[:8]
        carry = jnp.where(source < z, moved, carry)
    for b in range(NY):
        entering = turned(gain, carry)
        whole = jnp.concatenate(
            [held[b, :, g * 128 : (g + 1) * 128] + entering[g : g + 1] for g in range(8)], axis=1
        )
        turned_states = jnp.concatenate(
            [(whole * fwd_p[...]).astype(BF16), (whole * fwd_q[...]).astype(BF16)], axis=1
        )
        read = lax.dot_general(
            turned_states, out_map[...], (((1,), (1,)), ((), ())), preferred_element_type=F32
        )
        read = read * jnp.exp(decay[b]) + skip_ref[pl.ds(y, 1), :] * driven_in[b].astype(F32)
        inner = math.sqrt(2.0 / math.pi) * (read + 0.044715 * (read * read * read))
        scan_own[b] = (0.5 * read * (1.0 + jnp.tanh(inner))).astype(BF16)
        carry = falls[b] * turned(gain_block, carry) + ends[b]

    def spread_copies(own, landing, s_sem, r_sem):
        return {
            (dx, dy): remote(
                own.at[(y + dy) % NY], landing.at[dx, dy], s_sem.at[dx, dy], r_sem.at[dx, dy],
                {"fs": (x + dx) % NX, "sp_1": (y + dy) % NY},
            )
            for dx in order for dy in (1, 3, 2, 0) if (dx, dy) != (0, 0)
        }

    scan_copies = spread_copies(scan_own, scan_in, s_scan, r_scan)
    for copy in scan_copies.values():
        send(copy)
    scan_in[0, 0] = scan_own[y]
    arrive(3, (2, 3))
    for i in (1, 2, 3):
        attend_step(i)

    def join(near, far):
        @pl.when(z >= far)
        def _():
            fallen = tot[near, :, :1]
            acc[near] += jnp.exp2(fallen) * acc[far]
            tot[near, :, :1] = fallen + tot[far, :, :1]

    for dz in (1, 2, 3):
        join(0, dz)
    for dz in (6, 7):
        join(5, dz)
    arrive(4)
    attend_far(4, far_in)
    for dz in (4, 5):
        join(0, dz)
    attend_own[...] = acc[0].astype(BF16).reshape(NY, 128, 128)
    attend_copies = [
        send(
            remote(
                attend_own.at[(y + dy) % NY], attend_in.at[:, column], s_attend.at[dy],
                r_attend.at[dy], {"sp_1": (y + dy) % NY},
            )
        )
        for dy in (1, 3, 2)
    ]
    attend_in[:, column] = attend_own[y]

    part_copies = {}
    for dx in order:
        total = None
        for dy in range(NY):
            if (dx, dy) != (0, 0):
                scan_copies[dx, dy].wait_recv()
            head = (y + NY - dy) % NY
            head_rows = pl.ds(pl.multiple_of(head * 128, 128), 128)
            product = jnp.dot(scan_in[dx, dy], w_scan[head_rows, :], preferred_element_type=F32)
            total = product if total is None else total + product
        rounded = total.astype(BF16)
        for k in range(NT):
            part_out[dx, k] = rounded[k * 64 : (k + 1) * 64]
        for dt in range(NT):
            if (dx, dt) != (0, 0):
                to = (t + dt) % NT
                part_copies[dx, dt] = send(
                    remote(
                        part_out.at[dx, to], part_in.at[dx, dt], s_part.at[dx, dt],
                        r_part.at[dx, dt], {"fs": (x + NX - dx) % NX, "tp": to},
                    )
                )
    part_in[0, 0] = part_out[0, t]
    for dx in (1, 3, 2):
        for dy in (1, 3, 2):
            relay_copy(dx, dy).wait_recv()
    for copy in attend_copies:
        copy.wait_recv()
    other = pl.ds(pl.multiple_of((1 - t) * 64, 64), 64)
    last_copies = []
    for k in range(NX):
        product_own[k] = jnp.dot(attend_in[...], w_attend[k], preferred_element_type=F32)
        half_out[k] = product_own[k, other, :].astype(BF16)
        last_copies.append(
            send(remote(half_out.at[k], half_in.at[k], s_last.at[k], r_last.at[k], sibling))
        )
    for copy in last_copies:
        copy.wait_recv()
    for dx in order:
        for dt in range(NT):
            if (dx, dt) != (0, 0):
                part_copies[dx, dt].wait_recv()
        k = (x + dx) % NX
        columns = pl.ds(pl.multiple_of(k * 512, 512), 512)
        scan_part = part_in[dx, 0].astype(F32) + part_in[dx, 1].astype(F32)
        out[:, columns] = (product_own[k, mine, :] + half_in[k].astype(F32) + scan_part).astype(BF16)
    for copy in sent:
        copy.wait_send()
    for i in range(1, 5):
        for j in range(NY):
            if i < 4 or j < 2:
                right_copy(i, j).wait_send()
            if i < 4 or j >= 2:
                left_copy(i, j).wait_send()


def layer(*operands):
    def sems(*shape):
        return [pltpu.SemaphoreType.DMA(shape)] * 2

    return pl.pallas_call(
        layer_kernel,
        out_shape=pltpu.VMEM((64, 2048), BF16),
        in_specs=[pl.BlockSpec(memory_space=pl.ANY)] * 17,
        out_specs=VMEM,
        scratch_shapes=[
            *(
                pltpu.VMEM((NX, 512, 512) if k == 15 else operand.shape, operand.dtype)
                for k, operand in enumerate(operands)
            ),
            pltpu.SemaphoreType.DMA((17,)),
            pltpu.VMEM((64, 2048), BF16),
            pltpu.VMEM((NY, 128, 2048), BF16),
            pltpu.VMEM((2048, 256), BF16),
            pltpu.VMEM((2048, 128), BF16),
            pltpu.VMEM((2048, 128), BF16),
            pltpu.VMEM((NY, 16, 128), F32),
            pltpu.VMEM((NY, 16, 128), F32),
            pltpu.VMEM((NY, 128, 128), BF16),
            pltpu.VMEM((NY, 128, 128), BF16),
            pltpu.VMEM((NY, 128, 256), BF16),
            pltpu.VMEM((3, NY, 128, 256), BF16),
            pltpu.VMEM((3, NY, 128, 256), BF16),
            pltpu.VMEM((NY, 128, 256), BF16),
            pltpu.VMEM((8, 128), F32),
            pltpu.VMEM((NZ, 8, 128), F32),
            pltpu.VMEM((16, 128), F32),
            pltpu.VMEM((NZ, 16, 128), F32),
            pltpu.VMEM((NZ, 512, 128), F32),
            pltpu.VMEM((NZ, 512, 128), F32),
            pltpu.VMEM((256, 512), BF16),
            pltpu.VMEM((256, 2048), BF16),
            pltpu.VMEM((128, 2048), BF16),
            pltpu.VMEM((128, 1024), F32),
            pltpu.VMEM((128, 1024), F32),
            pltpu.VMEM((128, 1024), F32),
            pltpu.VMEM((128, 1024), F32),
            pltpu.VMEM((NY, 128, 1024), F32),
            pltpu.VMEM((NY, 8, 128), F32),
            pltpu.VMEM((NY, 128, 128), F32),
            pltpu.VMEM((NY, 128, 128), BF16),
            pltpu.VMEM((NY, 128, 128), BF16),
            pltpu.VMEM((128, 512), BF16),
            pltpu.VMEM((NX, NY, 128, 128), BF16),
            pltpu.VMEM((NX, NT, 64, 512), BF16),
            pltpu.VMEM((NX, NT, 64, 512), BF16),
            pltpu.VMEM((NX, 128, 512), F32),
            pltpu.VMEM((NX, 64, 512), BF16),
            pltpu.VMEM((NX, 64, 512), BF16),
            *sems(NY), *sems(NY), *sems(4, NX), *sems(NY), *sems(4, NY), *sems(4, NY), *sems(NZ),
            *sems(NZ), *sems(NX, NY), *sems(NX, NT), *sems(NX), *sems(NX, NY), *sems(NY), *sems(NX),
        ],
        compiler_params=pltpu.CompilerParams(
            collective_id=0, has_side_effects=True, vmem_limit_bytes=60 << 20
        ),
        name="layer",
    )(*operands)


def on_device(
    tokens, norm_gain, drive_weight, query_weight, key_weight, value_weight, key_offset, log_step,
    lambda_real, lambda_imag, input_map, output_map, skip_gain, forget, initial_state,
    scan_out_weight, attend_out_weight,
):
    return layer(
        tokens[0],
        norm_gain[None],
        drive_weight,
        query_weight,
        key_weight,
        value_weight,
        key_offset[:, 0, :],
        log_step[None],
        lambda_real,
        lambda_imag,
        input_map.transpose(0, 1, 3, 2),
        output_map,
        skip_gain.reshape(NY, 128),
        forget.reshape(NY, 8, 128),
        initial_state[:, 0],
        attend_out_weight,
        scan_out_weight,
    )[None]


def solution(mesh):
    split = Mesh(
        mesh.devices.reshape(NZ, NY, mesh.shape["fs"], mesh.shape["tp"]),
        ("sp_0", "sp_1", "fs", "tp"),
    )
    in_specs = (
        P("fs", SP_TP, None),
        P(),
        P("fs", "tp"),
        P("fs", "tp"),
        P("fs", "tp"),
        P("fs", "tp"),
        P("tp", "fs", SP),
        P("tp"),
        P("tp", None),
        P("tp", None),
        P(None, "tp", None, None),
        P(None, "tp", None, None),
        P("tp"),
        P("tp", "fs", SP),
        P(None, "fs", "tp", None),
        P("tp", "fs"),
        P("tp", "fs"),
    )
    return jax.shard_map(
        on_device, mesh=split, in_specs=in_specs, out_specs=P("fs", SP_TP, None), check_vma=False
    )
```

```python
import math

import jax
import jax.numpy as jnp
from jax import lax
from jax.experimental import pallas as pl
from jax.experimental.pallas import tpu as pltpu
from jax.sharding import Mesh
from jax.sharding import PartitionSpec as P

SP_TP = ("sp_0", "sp_1", "tp")
SP = ("sp_0", "sp_1")
EPSILON = 1e-06
LOG2E = 1.4426950408889634
NZ, NY, NX, NT = 8, 4, 4, 2
BF16, F32 = jnp.bfloat16, jnp.float32
VMEM = pl.BlockSpec(memory_space=pltpu.VMEM)
MESH_ID = pl.DeviceIdType.MESH


def remote(src, dst, send_sem, recv_sem, where):
    return pltpu.make_async_remote_copy(
        src_ref=src, dst_ref=dst, send_sem=send_sem, recv_sem=recv_sem,
        device_id=where, device_id_type=MESH_ID,
    )


def greet(peers):
    barrier = pltpu.get_barrier_semaphore()
    for peer in peers:
        pl.semaphore_signal(barrier, inc=1, device_id=peer, device_id_type=MESH_ID)


def await_greetings(count):
    pl.semaphore_wait(pltpu.get_barrier_semaphore(), count)


def plane_peers(x, y, t):
    peers = [
        {"fs": (x + dx) % NX, "tp": (t + dt) % NT}
        for dx in range(NX) for dt in range(NT) if (dx, dt) != (0, 0)
    ]
    peers += [
        {"fs": (x + dx) % NX, "sp_1": (y + dy) % NY} for dx in range(NX) for dy in range(1, NY)
    ]
    return peers


def high_low(value):
    high = value.astype(BF16)
    return high, (value - high.astype(F32)).astype(BF16)


def attend_chunk(query, pairs, offset, ladder, visible=None):
    keys, values = pairs[:, :128], pairs[:, 128:]
    score = lax.dot_general(query, keys, (((1,), (1,)), ((), ())), preferred_element_type=F32)
    score = score + offset
    soft = jnp.maximum(score, LOG2E * jnp.log(1.0 + jnp.exp2(jnp.minimum(score, 126.0))))
    if visible is not None:
        soft = jnp.where(visible, soft, 0.0)
    soft = soft.astype(BF16)
    last = jnp.dot(soft[:, 256:], ladder[:, :256], preferred_element_type=F32)
    first = jnp.dot(soft[:, :256], ladder[:, :256], preferred_element_type=F32) + jnp.dot(
        soft[:, 256:], ladder[:, 256:], preferred_element_type=F32
    )
    weight = jnp.exp2(score + jnp.concatenate([first, last], axis=1))
    if visible is not None:
        weight = jnp.where(visible, weight, 0.0)
    return jnp.dot(weight.astype(BF16), values, preferred_element_type=F32), first[:, :128]


def turned(gain, state):
    return gain[0] * state + gain[1] * pltpu.roll(state, 64, 1)


def powers_times(left, right):
    return (
        left[0] * right[0] - left[1] * right[1],
        left[1] * right[0] + left[0] * right[1],
    )


def layer_kernel(
    *refs,
):
    operands, out, held_here, rest = refs[:17], refs[17], refs[18:35], refs[35:]
    run_layer(operands, out, held_here, *rest)


def run_layer(
    operands, out, held_here, s_operand,
    normed, rows_in, keyed_w, query_w, drive_w, packed, packed_in, driven_in, queries,
    own_in, right_in, left_in, far_in, offset_own, offset_in, state_own, state_in, acc, tot,
    ladder, into_map, out_map, fwd_p, fwd_q, inv_p, inv_q, held, ends, decay,
    attend_own, scan_own, attend_in, scan_in, part_out, part_in, product_own, half_out, half_in,
    s_rows, r_rows, s_half, r_half, s_weight, r_weight, s_packed, r_packed,
    s_right, r_right, s_left, r_left, s_offset, r_offset, s_state, r_state,
    s_scan, r_scan, s_part, r_part, s_slice, r_slice, s_relay, r_relay, s_attend, r_attend,
    s_last, r_last, s_drive, r_drive, s_share, r_share,
):
    (
        tok, gain_ref, w_drive, w_query, w_key, w_value, key_offset, log_step_ref, lambda_real,
        lambda_imag, input_map, output_map, skip_ref, forget_ref, initial_ref, w_attend, w_scan,
    ) = held_here
    z, y, x, t = (lax.axis_index(a) for a in ("sp_0", "sp_1", "fs", "tp"))
    fetches = [
        pltpu.make_async_copy(src, dst.at[x] if k == 15 else dst, s_operand.at[k])
        for k, (src, dst) in enumerate(zip(operands, held_here))
    ]
    for fetch in fetches:
        fetch.start()
    greet(plane_peers(x, y, t) + [{"sp_0": (z + dz) % NZ} for dz in range(1, NZ)])
    row = lax.broadcasted_iota(jnp.int32, (128, 128), 0)
    lane = lax.broadcasted_iota(jnp.int32, (128, 128), 1)
    up, down = {"sp_0": (z + 1) % NZ}, {"sp_0": (z + NZ - 1) % NZ}
    sent = []

    def send(copy):
        copy.start()
        sent.append(copy)
        return copy

    for k in (0, 1, 6, 13):
        fetches[k].wait()
    packed[:, :8, :] = forget_ref[...]
    packed[:, 8:, :] = jnp.zeros((NY, 8, 128), F32)
    offsets = key_offset[...].astype(F32) * LOG2E
    for k in range(NY):
        packed[k, 8:9, :] = offsets[k : k + 1]
    values = tok[...].astype(F32)
    scale = lax.rsqrt(jnp.mean(values * values, axis=1, keepdims=True) + EPSILON)
    normed[...] = (values * scale * gain_ref[...]).astype(BF16)
    for k in (2, 3, 4, 5, 15):
        fetches[k].wait()
    await_greetings(26)

    order = (0, 1, 3, 2)
    mine = pl.ds(pl.multiple_of(t * 64, 64), 64)
    sibling = {"tp": 1 - t}

    def row_copy(j):
        return remote(
            normed, rows_in.at[j, mine], s_rows.at[j], r_rows.at[j],
            {"sp_1": (y + order[j]) % NY},
        )

    def half_copy(j):
        return remote(
            rows_in.at[j, mine] if j else normed, rows_in.at[j, mine], s_half.at[j], r_half.at[j],
            sibling,
        )

    column = pl.ds(pl.multiple_of(y * 128, 128), 128)
    depth = pl.ds(pl.multiple_of(x * 512, 512), 512)
    sources = (w_key, w_value, w_query)
    targets = (keyed_w.at[depth, :128], keyed_w.at[depth, 128:], query_w.at[depth])

    def weight_copy(kind, dx):
        return remote(
            sources[kind].at[:, column], targets[kind], s_weight.at[kind, dx],
            r_weight.at[kind, dx], {"fs": (x + dx) % NX},
        )

    def eighth(k):
        return drive_w.at[pl.ds(pl.multiple_of(k * 512 + z * 64, 64), 64)]

    def drive_copy(dx):
        return remote(
            w_drive.at[pl.ds(pl.multiple_of(z * 64, 64), 64), column], eighth(x), s_drive.at[dx],
            r_drive.at[dx], {"fs": (x + dx) % NX},
        )

    def share_copy(dx, dz):
        part = eighth((x + NX - dx) % NX)
        return remote(
            part, part, s_share.at[dx, dz], r_share.at[dx, dz], {"sp_0": (z + dz) % NZ}
        )

    def slice_copy(dx):
        return remote(
            w_attend.at[x, column], w_attend.at[x, column], s_slice.at[dx], r_slice.at[dx],
            {"fs": (x + dx) % NX},
        )

    def relay_copy(dx, dy):
        part = w_attend.at[(x + NX - dx) % NX, column]
        return remote(
            part, part, s_relay.at[dx, dy], r_relay.at[dx, dy], {"sp_1": (y + dy) % NY}
        )

    packed_copies = [
        send(
            remote(
                packed.at[(y + dy) % NY], packed_in.at[y], s_packed.at[dy], r_packed.at[dy],
                {"sp_1": (y + dy) % NY},
            )
        )
        for dy in range(1, NY)
    ]
    send(half_copy(0))
    for j in (1, 2, 3):
        send(row_copy(j))
    for dx in (1, 3, 2):
        send(drive_copy(dx))
    for kind in (0, 1, None, 2):
        for dx in (1, 3, 2):
            send(slice_copy(dx) if kind is None else weight_copy(kind, dx))
    packed_in[y] = packed[y]
    rows_in[0, mine] = normed[...]
    keyed_w[depth, :128] = w_key[:, column]
    keyed_w[depth, 128:] = w_value[:, column]
    query_w[depth] = w_query[:, column]
    drive_w[depth] = w_drive[:, column]

    for k in (7, 8, 9, 10, 11, 12, 14, 16):
        fetches[k].wait()
    sign = jnp.where(lane[:8] < 64, -1.0, 1.0)
    groups = pl.ds(pl.multiple_of(y * 8, 8), 8)

    def side_by_side(left, right):
        return jnp.concatenate([left, right], axis=1)

    lam_real = side_by_side(lambda_real[groups, :], lambda_real[groups, :])
    lam_imag = side_by_side(lambda_imag[groups, :], lambda_imag[groups, :])
    initial = side_by_side(initial_ref[0, groups, :], initial_ref[1, groups, :])
    spot = lax.broadcasted_iota(jnp.int32, (8, 32), 1) - lax.broadcasted_iota(
        jnp.int32, (8, 32), 0
    )
    step = jnp.exp(
        jnp.sum(jnp.where(spot == y * 8, log_step_ref[...], 0.0), axis=1, keepdims=True)
    )
    log_gain, rotate = lam_real * step, lam_imag * step
    cosine, sine, magnitude = jnp.cos(rotate), jnp.sin(rotate), jnp.exp(log_gain)
    bar_real, bar_imag = magnitude * cosine, magnitude * sine
    divisor = lam_real * lam_real + lam_imag * lam_imag
    shifted = bar_real - 1.0
    factor_real = (shifted * lam_real + bar_imag * lam_imag) / divisor
    factor_imag = (bar_imag * lam_real - shifted * lam_imag) / divisor * sign
    shrink = jnp.exp(-log_gain)
    gain = (bar_real, sign * bar_imag)
    inverse = (shrink * cosine, -sign * shrink * sine)
    gains, inverses = [gain], [inverse]
    for _ in range(9):
        gains.append(powers_times(gains[-1], gains[-1]))
    for _ in range(6):
        inverses.append(powers_times(inverses[-1], inverses[-1]))
    gain_block, gain_all = gains[7], gains[9]
    gain_last = powers_times(gain_block, inverse)
    into_map[...] = jnp.zeros_like(into_map)
    out_map[...] = jnp.zeros_like(out_map)
    for g in range(8):
        cols, swapped = pl.ds(g * 128, 128), pl.ds(1024 + g * 128, 128)
        raw = side_by_side(input_map[0, y * 8 + g], input_map[1, y * 8 + g])
        entry = factor_real[g : g + 1] * raw + factor_imag[g : g + 1] * pltpu.roll(raw, 64, 1)
        turned_entry = pltpu.roll(entry, 64, 1)
        for at in (g * 16, 128 + g * 16):
            into_map[at : at + 16, cols] = entry.astype(BF16)
            into_map[at : at + 16, swapped] = turned_entry.astype(BF16)
        raw = side_by_side(output_map[0, y * 8 + g], output_map[1, y * 8 + g])
        out_map[g * 16 : g * 16 + 16, cols] = (raw * -sign[:1]).astype(BF16)
        out_map[g * 16 : g * 16 + 16, swapped] = (pltpu.roll(raw, 64, 1) * -sign[:1]).astype(BF16)
        for table_p, table_q, steps in ((fwd_p, fwd_q, gains), (inv_p, inv_q, inverses)):
            real, imag = jnp.ones((8, 128), F32), jnp.zeros((8, 128), F32)
            for bit in range(3):
                by = tuple(part[g : g + 1] for part in steps[bit])
                new = powers_times((real, imag), by)
                chosen = (row[:8] & (1 << bit)) != 0
                real, imag = jnp.where(chosen, new[0], real), jnp.where(chosen, new[1], imag)
            table_p[:8, cols] = real
            table_q[:8, cols] = imag
            for bit in range(3, 7):
                n = 1 << bit
                by = tuple(part[g : g + 1] for part in steps[bit])
                new = powers_times((table_p[:n, cols], table_q[:n, cols]), by)
                table_p[n : 2 * n, cols] = new[0]
                table_q[n : 2 * n, cols] = new[1]
    ladder_row = lax.broadcasted_iota(jnp.int32, (256, 512), 0)
    ladder_lane = lax.broadcasted_iota(jnp.int32, (256, 512), 1)
    ladder[...] = jnp.where((ladder_lane >= 256) | (ladder_row >= ladder_lane), -1.0, 0.0).astype(
        BF16
    )

    def block_of(j):
        dy = j + j // 2 * (5 - 2 * j)
        return (y + NY - dy) % NY

    def right_copy(i, j):
        b = block_of(j)
        return remote(
            own_in.at[b] if i == 1 else right_in.at[i - 2, b],
            far_in.at[b] if i == 4 else right_in.at[i - 1, b],
            s_right.at[i - 1, j], r_right.at[i - 1, j], up,
        )

    def left_copy(i, j):
        b = block_of(j)
        return remote(
            own_in.at[b] if i == 1 else left_in.at[i - 2, b],
            far_in.at[b] if i == 4 else left_in.at[i - 1, b],
            s_left.at[i - 1, j], r_left.at[i - 1, j], down,
        )

    for copy in packed_copies:
        copy.wait_recv()
    for b in range(NY):
        offset_own[b : b + 1, :] = packed_in[b, 8:9, :]
        offset_in[0, b : b + 1, :] = packed_in[b, 8:9, :]
    offset_own[4:8, :] = jnp.zeros((4, 128), F32)
    offset_copies = [
        send(
            remote(
                offset_own, offset_in.at[dz], s_offset.at[dz], r_offset.at[dz],
                {"sp_0": (z + dz) % NZ},
            )
        )
        for dz in range(1, NZ)
    ]
    for dx in (1, 3, 2):
        drive_copy(dx).wait_recv()
        for dz in (1, 7, 2, 6, 3, 5, 4):
            send(share_copy(dx, dz))
    until = jnp.where(lane <= row, 1.0, 0.0)
    until_half = until.astype(BF16)
    falls = []
    for b in range(NY):
        forget = packed_in[b, :8, :]
        spread = jnp.concatenate(
            [jnp.broadcast_to(forget[g : g + 1], (16, 128)) for g in range(8)], axis=0
        )
        decay[b] = lax.dot_general(
            until, spread, (((1,), (1,)), ((), ())), preferred_element_type=F32,
            precision=lax.Precision.HIGHEST,
        )
        falls.append(jnp.sum(forget, axis=1, keepdims=True))
    for j in (1, 2, 3):
        row_copy(j).wait_recv()
        send(half_copy(j))
    for kind in (0, 1):
        for dx in (1, 3, 2):
            weight_copy(kind, dx).wait_recv()
    for j in range(NY):
        half_copy(j).wait_recv()
    product = jnp.dot(
        rows_in[...].reshape(512, 2048), keyed_w[...], preferred_element_type=F32
    ).astype(BF16)
    for j in range(NY):
        own_in[block_of(j)] = product[j * 128 : (j + 1) * 128]
        right_copy(1, j).start()
        left_copy(1, j).start()
    def arrive(i, blocks=range(NY)):
        for j in blocks:
            if i < 4 or j < 2:
                right_copy(i, j).wait_recv()
                if i < 3 or i == 3 and j < 2:
                    right_copy(i + 1, j).start()
            if i < 4 or j >= 2:
                left_copy(i, j).wait_recv()
                if i < 3 or i == 3 and j >= 2:
                    left_copy(i + 1, j).start()

    def offset_row(dz):
        return jnp.concatenate([offset_in[dz, b : b + 1, :] for b in range(NY)], axis=1)

    def attend_far(dz, pairs):
        @pl.when(z >= dz)
        def _():
            acc[dz], tot[dz] = attend_chunk(
                queries[...].reshape(512, 128), pairs[...].reshape(512, 256), offset_row(dz),
                ladder[...],
            )

    def attend_step(i):
        attend_far(i, right_in.at[i - 1])
        attend_far(8 - i, left_in.at[i - 1])

    def pass_slice(dx):
        slice_copy(dx).wait_recv()
        for dy in (1, 3, 2):
            send(relay_copy(dx, dy))

    for dx in (1, 3, 2):
        for dz in range(1, NZ):
            share_copy(dx, dz).wait_recv()
    product = jnp.dot(
        rows_in[...].reshape(512, 2048), drive_w[...], preferred_element_type=F32
    ).astype(BF16)
    for j in range(NY):
        driven_in[block_of(j)] = product[j * 128 : (j + 1) * 128]
    local = jnp.zeros((8, 128), F32)
    fall_all = jnp.zeros((8, 1), F32)
    for b in range(NY):
        driven = driven_in[b].astype(F32) * jnp.exp(-decay[b])
        entered = jnp.dot(
            jnp.concatenate(high_low(driven), axis=1), into_map[...], preferred_element_type=F32
        )
        unturned = entered[:, :1024] * inv_p[...] + entered[:, 1024:] * inv_q[...]
        high, low = high_low(unturned)
        held[b] = jnp.dot(until_half, high, preferred_element_type=F32) + jnp.dot(
            until_half, low, preferred_element_type=F32
        )
        for g in range(8):
            ends[b, g : g + 1, :] = held[b, 127:128, g * 128 : (g + 1) * 128]
        fall_all = fall_all + falls[b]
        falls[b] = jnp.exp(falls[b])
        ends[b] = falls[b] * turned(gain_last, ends[b])
        local = falls[b] * turned(gain_block, local) + ends[b]
        if b == 1:
            pass_slice(1)
        elif b > 1:
            arrive(1, (b - 2,))
    state_own[:8, :] = local
    state_own[8:, :] = jnp.broadcast_to(fall_all, (8, 128))
    state_copies = [
        send(
            remote(
                state_own, state_in.at[dz], s_state.at[dz], r_state.at[dz],
                {"sp_0": (z + dz) % NZ},
            )
        )
        for dz in range(1, NZ)
    ]

    arrive(1, (2, 3))
    pass_slice(3)
    for dx in (1, 3, 2):
        weight_copy(2, dx).wait_recv()
    product = jnp.dot(
        rows_in[...].reshape(512, 2048), query_w[...], preferred_element_type=F32
    )
    product = (product * (LOG2E * 128**-0.5)).astype(BF16)
    for j in range(NY):
        queries[block_of(j)] = product[j * 128 : (j + 1) * 128]

    arrive(2, (0, 1))
    acc[0], tot[0] = attend_chunk(
        queries[...].reshape(512, 128), own_in[...].reshape(512, 256), offset_row(0), ladder[...],
        lax.broadcasted_iota(jnp.int32, (512, 512), 1)
        < lax.broadcasted_iota(jnp.int32, (512, 512), 0),
    )
    for copy in offset_copies:
        copy.wait_recv()
    arrive(2, (2,))
    attend_step(1)
    arrive(2, (3,))

    for copy in state_copies:
        copy.wait_recv()
    carry = initial
    for source in range(NZ - 1):
        arrived = state_in[jnp.maximum(z - source, 1)]
        moved = jnp.exp(arrived[8:]) * turned(gain_all, carry) + arrived[:8]
        carry = jnp.where(source < z, moved, carry)
    for b in range(NY):
        entering = turned(gain, carry)
        whole = jnp.concatenate(
            [held[b, :, g * 128 : (g + 1) * 128] + entering[g : g + 1] for g in range(8)], axis=1
        )
        turned_states = jnp.concatenate(
            [(whole * fwd_p[...]).astype(BF16), (whole * fwd_q[...]).astype(BF16)], axis=1
        )
        read = lax.dot_general(
            turned_states, out_map[...], (((1,), (1,)), ((), ())), preferred_element_type=F32
        )
        read = read * jnp.exp(decay[b]) + skip_ref[pl.ds(y, 1), :] * driven_in[b].astype(F32)
        inner = math.sqrt(2.0 / math.pi) * (read + 0.044715 * (read * read * read))
        scan_own[b] = (0.5 * read * (1.0 + jnp.tanh(inner))).astype(BF16)
        carry = falls[b] * turned(gain_block, carry) + ends[b]

    def spread_copies(own, landing, s_sem, r_sem):
        return {
            (dx, dy): remote(
                own.at[(y + dy) % NY], landing.at[dx, dy], s_sem.at[dx, dy], r_sem.at[dx, dy],
                {"fs": (x + dx) % NX, "sp_1": (y + dy) % NY},
            )
            for dx in order for dy in (1, 3, 2, 0) if (dx, dy) != (0, 0)
        }

    scan_copies = spread_copies(scan_own, scan_in, s_scan, r_scan)
    for copy in scan_copies.values():
        send(copy)
    scan_in[0, 0] = scan_own[y]
    pass_slice(2)
    arrive(3, (0, 1))
    attend_step(2)
    arrive(3, (2, 3))
    attend_step(3)

    def join(near, far):
        @pl.when(z >= far)
        def _():
            fallen = tot[near, :, :1]
            acc[near] += jnp.exp2(fallen) * acc[far]
            tot[near, :, :1] = fallen + tot[far, :, :1]

    for dz in (1, 2, 3):
        join(0, dz)
    for dz in (6, 7):
        join(5, dz)
    arrive(4)
    attend_far(4, far_in)
    for dz in (4, 5):
        join(0, dz)
    attend_own[...] = acc[0].astype(BF16).reshape(NY, 128, 128)
    attend_copies = [
        send(
            remote(
                attend_own.at[(y + dy) % NY], attend_in.at[:, column], s_attend.at[dy],
                r_attend.at[dy], {"sp_1": (y + dy) % NY},
            )
        )
        for dy in (1, 3, 2)
    ]
    attend_in[:, column] = attend_own[y]

    part_copies = {}
    for dx in order:
        total = None
        for dy in range(NY):
            if (dx, dy) != (0, 0):
                scan_copies[dx, dy].wait_recv()
            head = (y + NY - dy) % NY
            head_rows = pl.ds(pl.multiple_of(head * 128, 128), 128)
            product = jnp.dot(scan_in[dx, dy], w_scan[head_rows, :], preferred_element_type=F32)
            total = product if total is None else total + product
        rounded = total.astype(BF16)
        for k in range(NT):
            part_out[dx, k] = rounded[k * 64 : (k + 1) * 64]
        for dt in range(NT):
            if (dx, dt) != (0, 0):
                to = (t + dt) % NT
                part_copies[dx, dt] = send(
                    remote(
                        part_out.at[dx, to], part_in.at[dx, dt], s_part.at[dx, dt],
                        r_part.at[dx, dt], {"fs": (x + NX - dx) % NX, "tp": to},
                    )
                )
    part_in[0, 0] = part_out[0, t]
    for dx in (1, 3, 2):
        for dy in (1, 3, 2):
            relay_copy(dx, dy).wait_recv()
    for copy in attend_copies:
        copy.wait_recv()
    other = pl.ds(pl.multiple_of((1 - t) * 64, 64), 64)
    last_copies = []
    for k in range(NX):
        product_own[k] = jnp.dot(attend_in[...], w_attend[k], preferred_element_type=F32)
        half_out[k] = product_own[k, other, :].astype(BF16)
        last_copies.append(
            send(remote(half_out.at[k], half_in.at[k], s_last.at[k], r_last.at[k], sibling))
        )
    for copy in last_copies:
        copy.wait_recv()
    for dx in order:
        for dt in range(NT):
            if (dx, dt) != (0, 0):
                part_copies[dx, dt].wait_recv()
        k = (x + dx) % NX
        columns = pl.ds(pl.multiple_of(k * 512, 512), 512)
        scan_part = part_in[dx, 0].astype(F32) + part_in[dx, 1].astype(F32)
        out[:, columns] = (product_own[k, mine, :] + half_in[k].astype(F32) + scan_part).astype(BF16)
    for copy in sent:
        copy.wait_send()
    for i in range(1, 5):
        for j in range(NY):
            if i < 4 or j < 2:
                right_copy(i, j).wait_send()
            if i < 4 or j >= 2:
                left_copy(i, j).wait_send()


def layer(*operands):
    def sems(*shape):
        return [pltpu.SemaphoreType.DMA(shape)] * 2

    return pl.pallas_call(
        layer_kernel,
        out_shape=pltpu.VMEM((64, 2048), BF16),
        in_specs=[pl.BlockSpec(memory_space=pl.ANY)] * 17,
        out_specs=VMEM,
        scratch_shapes=[
            *(
                pltpu.VMEM((NX, 512, 512) if k == 15 else operand.shape, operand.dtype)
                for k, operand in enumerate(operands)
            ),
            pltpu.SemaphoreType.DMA((17,)),
            pltpu.VMEM((64, 2048), BF16),
            pltpu.VMEM((NY, 128, 2048), BF16),
            pltpu.VMEM((2048, 256), BF16),
            pltpu.VMEM((2048, 128), BF16),
            pltpu.VMEM((2048, 128), BF16),
            pltpu.VMEM((NY, 16, 128), F32),
            pltpu.VMEM((NY, 16, 128), F32),
            pltpu.VMEM((NY, 128, 128), BF16),
            pltpu.VMEM((NY, 128, 128), BF16),
            pltpu.VMEM((NY, 128, 256), BF16),
            pltpu.VMEM((3, NY, 128, 256), BF16),
            pltpu.VMEM((3, NY, 128, 256), BF16),
            pltpu.VMEM((NY, 128, 256), BF16),
            pltpu.VMEM((8, 128), F32),
            pltpu.VMEM((NZ, 8, 128), F32),
            pltpu.VMEM((16, 128), F32),
            pltpu.VMEM((NZ, 16, 128), F32),
            pltpu.VMEM((NZ, 512, 128), F32),
            pltpu.VMEM((NZ, 512, 128), F32),
            pltpu.VMEM((256, 512), BF16),
            pltpu.VMEM((256, 2048), BF16),
            pltpu.VMEM((128, 2048), BF16),
            pltpu.VMEM((128, 1024), F32),
            pltpu.VMEM((128, 1024), F32),
            pltpu.VMEM((128, 1024), F32),
            pltpu.VMEM((128, 1024), F32),
            pltpu.VMEM((NY, 128, 1024), F32),
            pltpu.VMEM((NY, 8, 128), F32),
            pltpu.VMEM((NY, 128, 128), F32),
            pltpu.VMEM((NY, 128, 128), BF16),
            pltpu.VMEM((NY, 128, 128), BF16),
            pltpu.VMEM((128, 512), BF16),
            pltpu.VMEM((NX, NY, 128, 128), BF16),
            pltpu.VMEM((NX, NT, 64, 512), BF16),
            pltpu.VMEM((NX, NT, 64, 512), BF16),
            pltpu.VMEM((NX, 128, 512), F32),
            pltpu.VMEM((NX, 64, 512), BF16),
            pltpu.VMEM((NX, 64, 512), BF16),
            *sems(NY), *sems(NY), *sems(3, NX), *sems(NY), *sems(4, NY), *sems(4, NY), *sems(NZ),
            *sems(NZ), *sems(NX, NY), *sems(NX, NT), *sems(NX), *sems(NX, NY), *sems(NY), *sems(NX),
            *sems(NX), *sems(NX, NZ),
        ],
        compiler_params=pltpu.CompilerParams(
            collective_id=0, has_side_effects=True, vmem_limit_bytes=60 << 20
        ),
        name="layer",
    )(*operands)


def on_device(
    tokens, norm_gain, drive_weight, query_weight, key_weight, value_weight, key_offset, log_step,
    lambda_real, lambda_imag, input_map, output_map, skip_gain, forget, initial_state,
    scan_out_weight, attend_out_weight,
):
    return layer(
        tokens[0],
        norm_gain[None],
        drive_weight,
        query_weight,
        key_weight,
        value_weight,
        key_offset[:, 0, :],
        log_step[None],
        lambda_real,
        lambda_imag,
        input_map.transpose(0, 1, 3, 2),
        output_map,
        skip_gain.reshape(NY, 128),
        forget.reshape(NY, 8, 128),
        initial_state[:, 0],
        attend_out_weight,
        scan_out_weight,
    )[None]


def solution(mesh):
    split = Mesh(
        mesh.devices.reshape(NZ, NY, mesh.shape["fs"], mesh.shape["tp"]),
        ("sp_0", "sp_1", "fs", "tp"),
    )
    in_specs = (
        P("fs", SP_TP, None),
        P(),
        P("fs", "tp"),
        P("fs", "tp"),
        P("fs", "tp"),
        P("fs", "tp"),
        P("tp", "fs", SP),
        P("tp"),
        P("tp", None),
        P("tp", None),
        P(None, "tp", None, None),
        P(None, "tp", None, None),
        P("tp"),
        P("tp", "fs", SP),
        P(None, "fs", "tp", None),
        P("tp", "fs"),
        P("tp", "fs"),
    )
    return jax.shard_map(
        on_device, mesh=split, in_specs=in_specs, out_specs=P("fs", SP_TP, None), check_vma=False
    )
```

```python
import math

import jax
import jax.numpy as jnp
from jax import lax
from jax.experimental import pallas as pl
from jax.experimental.pallas import tpu as pltpu
from jax.sharding import Mesh
from jax.sharding import PartitionSpec as P

SP_TP = ("sp_0", "sp_1", "tp")
SP = ("sp_0", "sp_1")
EPSILON = 1e-06
LOG2E = 1.4426950408889634
NZ, NY, NX, NT = 8, 4, 4, 2
BF16, F32 = jnp.bfloat16, jnp.float32
TOGETHER = (
    "half", "keyed", "query", "packed", "offset", "state", "scan", "pre", "part", "hop", "attend",
    "last", "share",
)
SENT = TOGETHER + ("rows", "right", "left", "slice", "relay", "drive")
VMEM = pl.BlockSpec(memory_space=pltpu.VMEM)
MESH_ID = pl.DeviceIdType.MESH


def remote(src, dst, send_sem, recv_sem, where):
    return pltpu.make_async_remote_copy(
        src_ref=src, dst_ref=dst, send_sem=send_sem, recv_sem=recv_sem,
        device_id=where, device_id_type=MESH_ID,
    )


def greet(peers):
    barrier = pltpu.get_barrier_semaphore()
    for peer in peers:
        pl.semaphore_signal(barrier, inc=1, device_id=peer, device_id_type=MESH_ID)


def await_greetings(count):
    pl.semaphore_wait(pltpu.get_barrier_semaphore(), count)


def plane_peers(x, y, t):
    peers = [
        {"fs": (x + dx) % NX, "tp": (t + dt) % NT}
        for dx in range(NX) for dt in range(NT) if (dx, dt) != (0, 0)
    ]
    peers += [
        {"fs": (x + dx) % NX, "sp_1": (y + dy) % NY} for dx in range(NX) for dy in range(1, NY)
    ]
    return peers


def high_low(value):
    high = value.astype(BF16)
    return high, (value - high.astype(F32)).astype(BF16)


def attend_chunk(query, pairs, offset, ladder, visible=None):
    keys, values = pairs[:, :128], pairs[:, 128:]
    score = lax.dot_general(query, keys, (((1,), (1,)), ((), ())), preferred_element_type=F32)
    score = score + offset
    soft = jnp.maximum(score, LOG2E * jnp.log(1.0 + jnp.exp2(jnp.minimum(score, 126.0))))
    if visible is not None:
        soft = jnp.where(visible, soft, 0.0)
    soft = soft.astype(BF16)
    last = jnp.dot(soft[:, 256:], ladder[:, :256], preferred_element_type=F32)
    first = jnp.dot(soft[:, :256], ladder[:, :256], preferred_element_type=F32) + jnp.dot(
        soft[:, 256:], ladder[:, 256:], preferred_element_type=F32
    )
    weight = jnp.exp2(score + jnp.concatenate([first, last], axis=1))
    if visible is not None:
        weight = jnp.where(visible, weight, 0.0)
    return jnp.dot(weight.astype(BF16), values, preferred_element_type=F32), first[:, :128]


def turned(gain, state):
    return gain[0] * state + gain[1] * pltpu.roll(state, 64, 1)


def powers_times(left, right):
    return (
        left[0] * right[0] - left[1] * right[1],
        left[1] * right[0] + left[0] * right[1],
    )


def layer_kernel(
    *refs,
):
    operands, out, held_here, rest = refs[:17], refs[17], refs[18:35], refs[35:]
    run_layer(operands, out, held_here, *rest)


def run_layer(
    operands, out, held_here, s_operand,
    normed, rows_in, keyed_w, query_w, drive_w, packed, packed_in, driven_in, queries,
    own_in, right_in, left_in, far_in, offset_own, offset_in, state_own, state_in, acc, tot,
    ladder, into_map, out_map, fwd_p, fwd_q, inv_p, inv_q, held, ends, decay,
    attend_own, scan_own, attend_in, scan_in, part_out, part_in, product_own, half_out, half_in,
    scan_product, pre_out, pre_in,
    s_all, r_all, r_rows, r_right, r_left, r_slice, r_relay, r_drive,
):
    (
        tok, gain_ref, w_drive, w_query, w_key, w_value, key_offset, log_step_ref, lambda_real,
        lambda_imag, input_map, output_map, skip_ref, forget_ref, initial_ref, w_attend, w_scan,
    ) = held_here
    z, y, x, t = (lax.axis_index(a) for a in ("sp_0", "sp_1", "fs", "tp"))
    fetches = [
        pltpu.make_async_copy(src, dst.at[x] if k == 15 else dst, s_operand.at[k])
        for k, (src, dst) in enumerate(zip(operands, held_here))
    ]
    for fetch in fetches:
        fetch.start()
    greet(plane_peers(x, y, t) + [{"sp_0": (z + dz) % NZ} for dz in range(1, NZ)])
    row = lax.broadcasted_iota(jnp.int32, (128, 128), 0)
    lane = lax.broadcasted_iota(jnp.int32, (128, 128), 1)
    up, down = {"sp_0": (z + 1) % NZ}, {"sp_0": (z + NZ - 1) % NZ}
    s_of = {name: s_all.at[k] for k, name in enumerate(SENT)}
    r_of = {name: r_all.at[k] for k, name in enumerate(TOGETHER)}

    def send(copy):
        copy.start()
        return copy

    def await_all(name, data):
        remote(data, data, s_of[name], r_of[name], sibling).wait_recv()

    for k in (0, 1, 6, 13):
        fetches[k].wait()
    packed[:, :8, :] = forget_ref[...]
    packed[:, 8:, :] = jnp.zeros((NY, 8, 128), F32)
    offsets = key_offset[...].astype(F32) * LOG2E
    for k in range(NY):
        packed[k, 8:9, :] = offsets[k : k + 1]
    values = tok[...].astype(F32)
    scale = lax.rsqrt(jnp.mean(values * values, axis=1, keepdims=True) + EPSILON)
    normed[...] = (values * scale * gain_ref[...]).astype(BF16)
    for k in (2, 3, 4, 5, 15):
        fetches[k].wait()
    await_greetings(26)

    order = (0, 1, 3, 2)
    mine = pl.ds(pl.multiple_of(t * 64, 64), 64)
    sibling = {"tp": 1 - t}

    def row_copy(j):
        return remote(
            normed, rows_in.at[j, mine], s_of["rows"], r_rows.at[j - 1],
            {"sp_1": (y + order[j]) % NY},
        )

    def half_copy(j):
        return remote(
            rows_in.at[j, mine] if j else normed, rows_in.at[j, mine], s_of["half"], r_of["half"],
            sibling,
        )

    column = pl.ds(pl.multiple_of(y * 128, 128), 128)
    depth = pl.ds(pl.multiple_of(x * 512, 512), 512)
    sources = (w_key, w_value, w_query)
    targets = (keyed_w.at[depth, :128], keyed_w.at[depth, 128:], query_w.at[depth])

    def weight_copy(kind, dx):
        group = "query" if kind == 2 else "keyed"
        return remote(
            sources[kind].at[:, column], targets[kind], s_of[group], r_of[group],
            {"fs": (x + dx) % NX},
        )

    def eighth(k):
        return drive_w.at[pl.ds(pl.multiple_of(k * 512 + z * 64, 64), 64)]

    def drive_copy(dx):
        return remote(
            w_drive.at[pl.ds(pl.multiple_of(z * 64, 64), 64), column], eighth(x), s_of["drive"],
            r_drive.at[dx - 1], {"fs": (x + dx) % NX},
        )

    def share_copy(dx, dz):
        part = eighth((x + NX - dx) % NX)
        return remote(
            part, part, s_of["share"], r_of["share"], {"sp_0": (z + dz) % NZ}
        )

    def slice_copy(dx):
        return remote(
            w_attend.at[x, column], w_attend.at[x, column], s_of["slice"], r_slice.at[dx - 1],
            {"fs": (x + dx) % NX},
        )

    def relay_copy(dx, dy):
        part = w_attend.at[(x + NX - dx) % NX, column]
        return remote(
            part, part, s_of["relay"], r_relay.at[dx - 1, dy // 2], {"sp_1": (y + dy) % NY}
        )

    def hop_copy(dx, dy):
        start = (y + NY - dy) % NY * 128 + dy // 2 * 64
        part = w_attend.at[
            (x + NX - dx) % NX, pl.ds(pl.multiple_of(start, 64), 64)
        ]
        return remote(part, part, s_of["hop"], r_of["hop"], {"sp_1": (y + dy) % NY})

    for dy in range(1, NY):
        send(
            remote(
                packed.at[(y + dy) % NY], packed_in.at[y], s_of["packed"], r_of["packed"],
                {"sp_1": (y + dy) % NY},
            )
        )
    send(half_copy(0))
    for j in (1, 2, 3):
        send(row_copy(j))
    for dx in (1, 3, 2):
        send(drive_copy(dx))
    for kind in (0, 1, None, 2):
        for dx in (1, 3, 2):
            send(slice_copy(dx) if kind is None else weight_copy(kind, dx))
    packed_in[y] = packed[y]
    rows_in[0, mine] = normed[...]
    keyed_w[depth, :128] = w_key[:, column]
    keyed_w[depth, 128:] = w_value[:, column]
    query_w[depth] = w_query[:, column]
    drive_w[depth] = w_drive[:, column]

    for k in (7, 8, 9, 10, 11, 12, 14, 16):
        fetches[k].wait()
    sign = jnp.where(lane[:8] < 64, -1.0, 1.0)
    groups = pl.ds(pl.multiple_of(y * 8, 8), 8)

    def side_by_side(left, right):
        return jnp.concatenate([left, right], axis=1)

    lam_real = side_by_side(lambda_real[groups, :], lambda_real[groups, :])
    lam_imag = side_by_side(lambda_imag[groups, :], lambda_imag[groups, :])
    initial = side_by_side(initial_ref[0, groups, :], initial_ref[1, groups, :])
    spot = lax.broadcasted_iota(jnp.int32, (8, 32), 1) - lax.broadcasted_iota(
        jnp.int32, (8, 32), 0
    )
    step = jnp.exp(
        jnp.sum(jnp.where(spot == y * 8, log_step_ref[...], 0.0), axis=1, keepdims=True)
    )
    log_gain, rotate = lam_real * step, lam_imag * step
    cosine, sine, magnitude = jnp.cos(rotate), jnp.sin(rotate), jnp.exp(log_gain)
    bar_real, bar_imag = magnitude * cosine, magnitude * sine
    divisor = lam_real * lam_real + lam_imag * lam_imag
    shifted = bar_real - 1.0
    factor_real = (shifted * lam_real + bar_imag * lam_imag) / divisor
    factor_imag = (bar_imag * lam_real - shifted * lam_imag) / divisor * sign
    shrink = jnp.exp(-log_gain)
    gain = (bar_real, sign * bar_imag)
    inverse = (shrink * cosine, -sign * shrink * sine)
    gains, inverses = [gain], [inverse]
    for _ in range(9):
        gains.append(powers_times(gains[-1], gains[-1]))
    for _ in range(6):
        inverses.append(powers_times(inverses[-1], inverses[-1]))
    gain_block, gain_all = gains[7], gains[9]
    gain_last = powers_times(gain_block, inverse)
    into_map[...] = jnp.zeros_like(into_map)
    out_map[...] = jnp.zeros_like(out_map)
    for g in range(8):
        cols, swapped = pl.ds(g * 128, 128), pl.ds(1024 + g * 128, 128)
        raw = side_by_side(input_map[0, y * 8 + g], input_map[1, y * 8 + g])
        entry = factor_real[g : g + 1] * raw + factor_imag[g : g + 1] * pltpu.roll(raw, 64, 1)
        turned_entry = pltpu.roll(entry, 64, 1)
        for at in (g * 16, 128 + g * 16):
            into_map[at : at + 16, cols] = entry.astype(BF16)
            into_map[at : at + 16, swapped] = turned_entry.astype(BF16)
        raw = side_by_side(output_map[0, y * 8 + g], output_map[1, y * 8 + g])
        out_map[g * 16 : g * 16 + 16, cols] = (raw * -sign[:1]).astype(BF16)
        out_map[g * 16 : g * 16 + 16, swapped] = (pltpu.roll(raw, 64, 1) * -sign[:1]).astype(BF16)
        for table_p, table_q, steps in ((fwd_p, fwd_q, gains), (inv_p, inv_q, inverses)):
            real, imag = jnp.ones((8, 128), F32), jnp.zeros((8, 128), F32)
            for bit in range(3):
                by = tuple(part[g : g + 1] for part in steps[bit])
                new = powers_times((real, imag), by)
                chosen = (row[:8] & (1 << bit)) != 0
                real, imag = jnp.where(chosen, new[0], real), jnp.where(chosen, new[1], imag)
            table_p[:8, cols] = real
            table_q[:8, cols] = imag
            for bit in range(3, 7):
                n = 1 << bit
                by = tuple(part[g : g + 1] for part in steps[bit])
                new = powers_times((table_p[:n, cols], table_q[:n, cols]), by)
                table_p[n : 2 * n, cols] = new[0]
                table_q[n : 2 * n, cols] = new[1]
    ladder_row = lax.broadcasted_iota(jnp.int32, (256, 512), 0)
    ladder_lane = lax.broadcasted_iota(jnp.int32, (256, 512), 1)
    ladder[...] = jnp.where((ladder_lane >= 256) | (ladder_row >= ladder_lane), -1.0, 0.0).astype(
        BF16
    )

    def block_of(j):
        dy = j + j // 2 * (5 - 2 * j)
        return (y + NY - dy) % NY

    def right_copy(i, j):
        b = block_of(j)
        return remote(
            own_in.at[b] if i == 1 else right_in.at[i - 2, b],
            far_in.at[b] if i == 4 else right_in.at[i - 1, b],
            s_of["right"], r_right.at[4 * i - 4 + j], up,
        )

    def left_copy(i, j):
        b = block_of(j)
        return remote(
            own_in.at[b] if i == 1 else left_in.at[i - 2, b],
            far_in.at[b] if i == 4 else left_in.at[i - 1, b],
            s_of["left"], r_left.at[4 * i - 4 + j - (2 if i == 4 else 0)], down,
        )

    await_all("packed", packed_in.at[:3])
    for b in range(NY):
        offset_own[b : b + 1, :] = packed_in[b, 8:9, :]
        offset_in[0, b : b + 1, :] = packed_in[b, 8:9, :]
    offset_own[4:8, :] = jnp.zeros((4, 128), F32)
    for dz in range(1, NZ):
        send(
            remote(
                offset_own, offset_in.at[dz], s_of["offset"], r_of["offset"],
                {"sp_0": (z + dz) % NZ},
            )
        )
    for dx in (1, 3, 2):
        drive_copy(dx).wait_recv()
        for dz in (1, 7, 2, 6, 3, 5, 4):
            send(share_copy(dx, dz))
    until = jnp.where(lane <= row, 1.0, 0.0)
    until_half = until.astype(BF16)
    falls = []
    for b in range(NY):
        forget = packed_in[b, :8, :]
        spread = jnp.concatenate(
            [jnp.broadcast_to(forget[g : g + 1], (16, 128)) for g in range(8)], axis=0
        )
        decay[b] = lax.dot_general(
            until, spread, (((1,), (1,)), ((), ())), preferred_element_type=F32,
            precision=lax.Precision.HIGHEST,
        )
        falls.append(jnp.sum(forget, axis=1, keepdims=True))
    for j in (1, 2, 3):
        row_copy(j).wait_recv()
        send(half_copy(j))
    await_all("keyed", keyed_w.at[:1536])
    await_all("half", rows_in.at[:2])
    product = jnp.dot(
        rows_in[...].reshape(512, 2048), keyed_w[...], preferred_element_type=F32
    ).astype(BF16)
    for j in range(NY):
        own_in[block_of(j)] = product[j * 128 : (j + 1) * 128]
        right_copy(1, j).start()
        left_copy(1, j).start()
    def arrive(i, blocks=range(NY)):
        for j in blocks:
            if i < 4 or j < 2:
                right_copy(i, j).wait_recv()
                if i < 3 or i == 3 and j < 2:
                    right_copy(i + 1, j).start()
            if i < 4 or j >= 2:
                left_copy(i, j).wait_recv()
                if i < 3 or i == 3 and j >= 2:
                    left_copy(i + 1, j).start()

    def offset_row(dz):
        return jnp.concatenate([offset_in[dz, b : b + 1, :] for b in range(NY)], axis=1)

    def attend_far(dz, pairs):
        @pl.when(z >= dz)
        def _():
            acc[dz], tot[dz] = attend_chunk(
                queries[...].reshape(512, 128), pairs[...].reshape(512, 256), offset_row(dz),
                ladder[...],
            )

    def attend_step(i):
        attend_far(i, right_in.at[i - 1])
        attend_far(8 - i, left_in.at[i - 1])

    def pass_slice(dx):
        slice_copy(dx).wait_recv()
        for dy in (1, 3):
            send(relay_copy(dx, dy))

    def pass_on(dx):
        for dy in (1, 3):
            relay_copy(dx, dy).wait_recv()
            send(hop_copy(dx, dy))

    await_all("share", drive_w.at[:1344])
    product = jnp.dot(
        rows_in[...].reshape(512, 2048), drive_w[...], preferred_element_type=F32
    ).astype(BF16)
    for j in range(NY):
        driven_in[block_of(j)] = product[j * 128 : (j + 1) * 128]
    local = jnp.zeros((8, 128), F32)
    fall_all = jnp.zeros((8, 1), F32)
    for b in range(NY):
        driven = driven_in[b].astype(F32) * jnp.exp(-decay[b])
        entered = jnp.dot(
            jnp.concatenate(high_low(driven), axis=1), into_map[...], preferred_element_type=F32
        )
        unturned = entered[:, :1024] * inv_p[...] + entered[:, 1024:] * inv_q[...]
        high, low = high_low(unturned)
        held[b] = jnp.dot(until_half, high, preferred_element_type=F32) + jnp.dot(
            until_half, low, preferred_element_type=F32
        )
        for g in range(8):
            ends[b, g : g + 1, :] = held[b, 127:128, g * 128 : (g + 1) * 128]
        fall_all = fall_all + falls[b]
        falls[b] = jnp.exp(falls[b])
        ends[b] = falls[b] * turned(gain_last, ends[b])
        local = falls[b] * turned(gain_block, local) + ends[b]
        if b == 1:
            pass_slice(1)
        elif b > 1:
            arrive(1, (b - 2,))
    pass_slice(3)
    state_own[:8, :] = local
    state_own[8:, :] = jnp.broadcast_to(fall_all, (8, 128))
    for dz in range(1, NZ):
        send(
            remote(
                state_own, state_in.at[dz], s_of["state"], r_of["state"],
                {"sp_0": (z + dz) % NZ},
            )
        )

    arrive(1, (2, 3))
    pass_slice(2)
    pass_on(1)
    await_all("query", query_w.at[:1536])
    product = jnp.dot(
        rows_in[...].reshape(512, 2048), query_w[...], preferred_element_type=F32
    )
    product = (product * (LOG2E * 128**-0.5)).astype(BF16)
    for j in range(NY):
        queries[block_of(j)] = product[j * 128 : (j + 1) * 128]

    arrive(2, (0, 1))
    pass_on(3)
    acc[0], tot[0] = attend_chunk(
        queries[...].reshape(512, 128), own_in[...].reshape(512, 256), offset_row(0), ladder[...],
        lax.broadcasted_iota(jnp.int32, (512, 512), 1)
        < lax.broadcasted_iota(jnp.int32, (512, 512), 0),
    )
    await_all("offset", offset_in.at[:7])
    pass_on(2)

    await_all("state", state_in.at[:7])
    carry = initial
    for source in range(NZ - 1):
        arrived = state_in[jnp.maximum(z - source, 1)]
        moved = jnp.exp(arrived[8:]) * turned(gain_all, carry) + arrived[:8]
        carry = jnp.where(source < z, moved, carry)
    for b in range(NY):
        entering = turned(gain, carry)
        whole = jnp.concatenate(
            [held[b, :, g * 128 : (g + 1) * 128] + entering[g : g + 1] for g in range(8)], axis=1
        )
        turned_states = jnp.concatenate(
            [(whole * fwd_p[...]).astype(BF16), (whole * fwd_q[...]).astype(BF16)], axis=1
        )
        read = lax.dot_general(
            turned_states, out_map[...], (((1,), (1,)), ((), ())), preferred_element_type=F32
        )
        read = read * jnp.exp(decay[b]) + skip_ref[pl.ds(y, 1), :] * driven_in[b].astype(F32)
        inner = math.sqrt(2.0 / math.pi) * (read + 0.044715 * (read * read * read))
        scan_own[b] = (0.5 * read * (1.0 + jnp.tanh(inner))).astype(BF16)
        carry = falls[b] * turned(gain_block, carry) + ends[b]

    for dx in order:
        for dy in (1, 3, 2, 0):
            if (dx, dy) != (0, 0):
                send(
                    remote(
                        scan_own.at[(y + dy) % NY], scan_in.at[dx, dy], s_of["scan"],
                        r_of["scan"], {"fs": (x + dx) % NX, "sp_1": (y + dy) % NY},
                    )
                )
    scan_in[0, 0] = scan_own[y]
    arrive(2, (2, 3))
    attend_step(1)
    arrive(3, (0, 1))
    attend_step(2)
    arrive(3, (2, 3))
    attend_step(3)

    def join(near, far):
        @pl.when(z >= far)
        def _():
            fallen = tot[near, :, :1]
            acc[near] += jnp.exp2(fallen) * acc[far]
            tot[near, :, :1] = fallen + tot[far, :, :1]

    for dz in (1, 2, 3):
        join(0, dz)
    for dz in (6, 7):
        join(5, dz)
    other = pl.ds(pl.multiple_of((1 - t) * 64, 64), 64)
    await_all("scan", drive_w.at[:1920])
    for dx in order:
        total = None
        for dy in range(NY):
            head = (y + NY - dy) % NY
            head_rows = pl.ds(pl.multiple_of(head * 128, 128), 128)
            product = jnp.dot(scan_in[dx, dy], w_scan[head_rows, :], preferred_element_type=F32)
            total = product if total is None else total + product
        scan_product[dx] = total
        pre_out[dx] = scan_product[dx, other, :].astype(BF16)
        send(remote(pre_out.at[dx], pre_in.at[dx], s_of["pre"], r_of["pre"], sibling))
    arrive(4)
    attend_far(4, far_in)
    await_all("pre", pre_in)
    for dx in (1, 3, 2):
        part_out[dx] = (scan_product[dx, mine, :] + pre_in[dx].astype(F32)).astype(BF16)
        send(
            remote(
                part_out.at[dx], part_in.at[dx], s_of["part"], r_of["part"],
                {"fs": (x + NX - dx) % NX},
            )
        )
    for dz in (4, 5):
        join(0, dz)
    attend_own[...] = acc[0].astype(BF16).reshape(NY, 128, 128)
    for dy in (1, 3, 2):
        send(
            remote(
                attend_own.at[(y + dy) % NY], attend_in.at[:, column], s_of["attend"],
                r_of["attend"], {"sp_1": (y + dy) % NY},
            )
        )
    attend_in[:, column] = attend_own[y]

    await_all("hop", w_attend.at[0, :384])
    await_all("attend", drive_w.at[:384])
    for k in range(NX):
        product_own[k] = jnp.dot(attend_in[...], w_attend[k], preferred_element_type=F32)
        half_out[k] = product_own[k, other, :].astype(BF16)
        send(remote(half_out.at[k], half_in.at[k], s_of["last"], r_of["last"], sibling))
    await_all("last", half_in)
    await_all("part", w_attend.at[0, :192])
    for dx in order:
        k = (x + dx) % NX
        columns = pl.ds(pl.multiple_of(k * 512, 512), 512)
        scan_part = scan_product[0, mine, :] + pre_in[0].astype(F32)
        if dx:
            scan_part = part_in[dx].astype(F32)
        out[:, columns] = (product_own[k, mine, :] + half_in[k].astype(F32) + scan_part).astype(BF16)
    for name, data in {
        "rows": rows_in.at[:3, :64],
        "half": rows_in.at[:2],
        "keyed": keyed_w.at[:1536],
        "query": query_w.at[:1536],
        "packed": packed_in.at[:3],
        "right": w_attend.at[:2, :448],
        "left": w_attend.at[:2, :448],
        "offset": offset_in.at[:7],
        "state": state_in.at[:7],
        "scan": drive_w.at[:1920],
        "pre": pre_in,
        "part": w_attend.at[0, :192],
        "slice": w_attend.at[0, :384],
        "relay": w_attend.at[:3, :256],
        "hop": w_attend.at[0, :384],
        "attend": drive_w.at[:384],
        "last": half_in,
        "drive": drive_w.at[:192],
        "share": drive_w.at[:1344],
    }.items():
        remote(data, data, s_of[name], r_rows.at[0], sibling).wait_send()


def layer(*operands):
    return pl.pallas_call(
        layer_kernel,
        out_shape=pltpu.VMEM((64, 2048), BF16),
        in_specs=[pl.BlockSpec(memory_space=pl.ANY)] * 17,
        out_specs=VMEM,
        scratch_shapes=[
            *(
                pltpu.VMEM((NX, 512, 512) if k == 15 else operand.shape, operand.dtype)
                for k, operand in enumerate(operands)
            ),
            pltpu.SemaphoreType.DMA((17,)),
            pltpu.VMEM((64, 2048), BF16),
            pltpu.VMEM((NY, 128, 2048), BF16),
            pltpu.VMEM((2048, 256), BF16),
            pltpu.VMEM((2048, 128), BF16),
            pltpu.VMEM((2048, 128), BF16),
            pltpu.VMEM((NY, 16, 128), F32),
            pltpu.VMEM((NY, 16, 128), F32),
            pltpu.VMEM((NY, 128, 128), BF16),
            pltpu.VMEM((NY, 128, 128), BF16),
            pltpu.VMEM((NY, 128, 256), BF16),
            pltpu.VMEM((3, NY, 128, 256), BF16),
            pltpu.VMEM((3, NY, 128, 256), BF16),
            pltpu.VMEM((NY, 128, 256), BF16),
            pltpu.VMEM((8, 128), F32),
            pltpu.VMEM((NZ, 8, 128), F32),
            pltpu.VMEM((16, 128), F32),
            pltpu.VMEM((NZ, 16, 128), F32),
            pltpu.VMEM((NZ, 512, 128), F32),
            pltpu.VMEM((NZ, 512, 128), F32),
            pltpu.VMEM((256, 512), BF16),
            pltpu.VMEM((256, 2048), BF16),
            pltpu.VMEM((128, 2048), BF16),
            pltpu.VMEM((128, 1024), F32),
            pltpu.VMEM((128, 1024), F32),
            pltpu.VMEM((128, 1024), F32),
            pltpu.VMEM((128, 1024), F32),
            pltpu.VMEM((NY, 128, 1024), F32),
            pltpu.VMEM((NY, 8, 128), F32),
            pltpu.VMEM((NY, 128, 128), F32),
            pltpu.VMEM((NY, 128, 128), BF16),
            pltpu.VMEM((NY, 128, 128), BF16),
            pltpu.VMEM((128, 512), BF16),
            pltpu.VMEM((NX, NY, 128, 128), BF16),
            pltpu.VMEM((NX, 64, 512), BF16),
            pltpu.VMEM((NX, 64, 512), BF16),
            pltpu.VMEM((NX, 128, 512), F32),
            pltpu.VMEM((NX, 64, 512), BF16),
            pltpu.VMEM((NX, 64, 512), BF16),
            pltpu.VMEM((NX, 128, 512), F32),
            pltpu.VMEM((NX, 64, 512), BF16),
            pltpu.VMEM((NX, 64, 512), BF16),
            *(
                pltpu.SemaphoreType.DMA(shape)
                for shape in (
                    (len(SENT),), (len(TOGETHER),), (3,), (14,), (14,), (3,), (3, 2), (3,)
                )
            ),
        ],
        compiler_params=pltpu.CompilerParams(
            collective_id=0, has_side_effects=True, vmem_limit_bytes=60 << 20
        ),
        name="layer",
    )(*operands)


def on_device(
    tokens, norm_gain, drive_weight, query_weight, key_weight, value_weight, key_offset, log_step,
    lambda_real, lambda_imag, input_map, output_map, skip_gain, forget, initial_state,
    scan_out_weight, attend_out_weight,
):
    return layer(
        tokens[0],
        norm_gain[None],
        drive_weight,
        query_weight,
        key_weight,
        value_weight,
        key_offset[:, 0, :],
        log_step[None],
        lambda_real,
        lambda_imag,
        input_map.transpose(0, 1, 3, 2),
        output_map,
        skip_gain.reshape(NY, 128),
        forget.reshape(NY, 8, 128),
        initial_state[:, 0],
        attend_out_weight,
        scan_out_weight,
    )[None]


def solution(mesh):
    split = Mesh(
        mesh.devices.reshape(NZ, NY, mesh.shape["fs"], mesh.shape["tp"]),
        ("sp_0", "sp_1", "fs", "tp"),
    )
    in_specs = (
        P("fs", SP_TP, None),
        P(),
        P("fs", "tp"),
        P("fs", "tp"),
        P("fs", "tp"),
        P("fs", "tp"),
        P("tp", "fs", SP),
        P("tp"),
        P("tp", None),
        P("tp", None),
        P(None, "tp", None, None),
        P(None, "tp", None, None),
        P("tp"),
        P("tp", "fs", SP),
        P(None, "fs", "tp", None),
        P("tp", "fs"),
        P("tp", "fs"),
    )
    return jax.shard_map(
        on_device, mesh=split, in_specs=in_specs, out_specs=P("fs", SP_TP, None), check_vma=False
    )
```

```python
import math

import jax
import jax.numpy as jnp
from jax import lax
from jax.experimental import pallas as pl
from jax.experimental.pallas import tpu as pltpu
from jax.sharding import Mesh
from jax.sharding import PartitionSpec as P

SP_TP = ("sp_0", "sp_1", "tp")
SP = ("sp_0", "sp_1")
EPSILON = 1e-06
LOG2E = 1.4426950408889634
NZ, NY, NX, NT = 8, 4, 4, 2
BF16, F32 = jnp.bfloat16, jnp.float32
TOGETHER = (
    "half", "keyed", "query", "packed", "offset", "state", "scan", "pre", "part", "hop", "attend",
    "last", "share", "far_rows", "values",
)
SENT = TOGETHER + ("rows", "right", "left", "slice", "relay", "drive")
VMEM = pl.BlockSpec(memory_space=pltpu.VMEM)
MESH_ID = pl.DeviceIdType.MESH


def remote(src, dst, send_sem, recv_sem, where):
    return pltpu.make_async_remote_copy(
        src_ref=src, dst_ref=dst, send_sem=send_sem, recv_sem=recv_sem,
        device_id=where, device_id_type=MESH_ID,
    )


def greet(peers):
    barrier = pltpu.get_barrier_semaphore()
    for peer in peers:
        pl.semaphore_signal(barrier, inc=1, device_id=peer, device_id_type=MESH_ID)


def await_greetings(count):
    pl.semaphore_wait(pltpu.get_barrier_semaphore(), count)


def plane_peers(x, y, t):
    peers = [
        {"fs": (x + dx) % NX, "tp": (t + dt) % NT}
        for dx in range(NX) for dt in range(NT) if (dx, dt) != (0, 0)
    ]
    peers += [
        {"fs": (x + dx) % NX, "sp_1": (y + dy) % NY} for dx in range(NX) for dy in range(1, NY)
    ]
    return peers


def high_low(value):
    high = value.astype(BF16)
    return high, (value - high.astype(F32)).astype(BF16)


def attend_chunk(query, pairs, offset, ladder, visible=None):
    keys, values = pairs[:, :128], pairs[:, 128:]
    score = lax.dot_general(query, keys, (((1,), (1,)), ((), ())), preferred_element_type=F32)
    score = score + offset
    soft = jnp.maximum(score, LOG2E * jnp.log(1.0 + jnp.exp2(jnp.minimum(score, 126.0))))
    if visible is not None:
        soft = jnp.where(visible, soft, 0.0)
    soft = soft.astype(BF16)
    last = jnp.dot(soft[:, 256:], ladder[:, :256], preferred_element_type=F32)
    first = jnp.dot(soft[:, :256], ladder[:, :256], preferred_element_type=F32) + jnp.dot(
        soft[:, 256:], ladder[:, 256:], preferred_element_type=F32
    )
    weight = jnp.exp2(score + jnp.concatenate([first, last], axis=1))
    if visible is not None:
        weight = jnp.where(visible, weight, 0.0)
    return jnp.dot(weight.astype(BF16), values, preferred_element_type=F32), first[:, :128]


def turned(gain, state):
    return gain[0] * state + gain[1] * pltpu.roll(state, 64, 1)


def powers_times(left, right):
    return (
        left[0] * right[0] - left[1] * right[1],
        left[1] * right[0] + left[0] * right[1],
    )


def layer_kernel(
    *refs,
):
    operands, out, held_here, rest = refs[:17], refs[17], refs[18:35], refs[35:]
    run_layer(operands, out, held_here, *rest)


def run_layer(
    operands, out, held_here, s_operand,
    normed, rows_in, keyed_w, query_w, drive_w, packed, packed_in, driven_in, queries,
    own_in, right_in, left_in, far_in, offset_own, offset_in, state_own, state_in, acc, tot,
    ladder, into_map, out_map, fwd_p, fwd_q, inv_p, inv_q, held, ends, decay,
    attend_own, scan_own, attend_in, scan_in, part_out, part_in, product_own, half_out, half_in,
    scan_product, pre_out, pre_in,
    s_all, r_all, r_rows, r_right, r_left, r_slice, r_relay, r_drive,
):
    (
        tok, gain_ref, w_drive, w_query, w_key, w_value, key_offset, log_step_ref, lambda_real,
        lambda_imag, input_map, output_map, skip_ref, forget_ref, initial_ref, w_attend, w_scan,
    ) = held_here
    z, y, x, t = (lax.axis_index(a) for a in ("sp_0", "sp_1", "fs", "tp"))
    fetches = [
        pltpu.make_async_copy(src, dst.at[x] if k == 15 else dst, s_operand.at[k])
        for k, (src, dst) in enumerate(zip(operands, held_here))
    ]
    for fetch in fetches:
        fetch.start()
    greet(plane_peers(x, y, t) + [{"sp_0": (z + dz) % NZ} for dz in range(1, NZ)])
    row = lax.broadcasted_iota(jnp.int32, (128, 128), 0)
    lane = lax.broadcasted_iota(jnp.int32, (128, 128), 1)
    up, down = {"sp_0": (z + 1) % NZ}, {"sp_0": (z + NZ - 1) % NZ}
    s_of = {name: s_all.at[k] for k, name in enumerate(SENT)}
    r_of = {name: r_all.at[k] for k, name in enumerate(TOGETHER)}

    def send(copy):
        copy.start()
        return copy

    def await_all(name, data):
        remote(data, data, s_of[name], r_of[name], sibling).wait_recv()

    for k in (0, 1, 6, 13):
        fetches[k].wait()
    packed[:, :8, :] = forget_ref[...]
    packed[:, 8:, :] = jnp.zeros((NY, 8, 128), F32)
    offsets = key_offset[...].astype(F32) * LOG2E
    for k in range(NY):
        packed[k, 8:9, :] = offsets[k : k + 1]
    values = tok[...].astype(F32)
    scale = lax.rsqrt(jnp.mean(values * values, axis=1, keepdims=True) + EPSILON)
    normed[...] = (values * scale * gain_ref[...]).astype(BF16)
    for k in (2, 3, 4, 5, 15):
        fetches[k].wait()
    await_greetings(26)

    order = (0, 1, 3, 2)
    mine = pl.ds(pl.multiple_of(t * 64, 64), 64)
    sibling = {"tp": 1 - t}

    def quarter(half):
        return pl.ds(pl.multiple_of(t * 64 + half * 32, 32), 32)

    def row_copy(j, half):
        return remote(
            normed.at[pl.ds(half * 32, 32)], rows_in.at[j, quarter(half)], s_of["rows"],
            r_rows.at[2 * j - 2 + half], {"sp_1": (y + order[j]) % NY},
        )

    def far_row_copy(j):
        part = quarter(j - 1)
        return remote(
            rows_in.at[j, part], rows_in.at[3, part], s_of["far_rows"], r_of["far_rows"],
            {"sp_1": (y + order[j]) % NY},
        )

    def half_copy(j):
        return remote(
            rows_in.at[j, mine] if j else normed, rows_in.at[j, mine], s_of["half"], r_of["half"],
            sibling,
        )

    column = pl.ds(pl.multiple_of(y * 128, 128), 128)
    depth = pl.ds(pl.multiple_of(x * 512, 512), 512)
    sources = (w_key, w_value, w_query)
    targets = (keyed_w.at[depth, :128], keyed_w.at[depth, 128:], query_w.at[depth])

    def weight_copy(kind, dx):
        group = "query" if kind == 2 else "keyed"
        return remote(
            sources[kind].at[:, column], targets[kind], s_of[group], r_of[group],
            {"fs": (x + dx) % NX},
        )

    def eighth(k):
        return drive_w.at[pl.ds(pl.multiple_of(k * 512 + z * 64, 64), 64)]

    def drive_copy(dx):
        return remote(
            w_drive.at[pl.ds(pl.multiple_of(z * 64, 64), 64), column], eighth(x), s_of["drive"],
            r_drive.at[dx - 1], {"fs": (x + dx) % NX},
        )

    def value_eighth(k):
        return keyed_w.at[pl.ds(pl.multiple_of(k * 512 + z * 64, 64), 64), 128:]

    def value_copy():
        return remote(
            w_value.at[pl.ds(pl.multiple_of(z * 64, 64), 64), column], value_eighth(x),
            s_of["drive"], r_drive.at[3], {"fs": (x + 2) % NX},
        )

    def value_share_copy(dz):
        part = value_eighth((x + 2) % NX)
        return remote(part, part, s_of["values"], r_of["values"], {"sp_0": (z + dz) % NZ})

    def share_copy(dx, dz):
        part = eighth((x + NX - dx) % NX)
        return remote(
            part, part, s_of["share"], r_of["share"], {"sp_0": (z + dz) % NZ}
        )

    def slice_copy(dx):
        return remote(
            w_attend.at[x, column], w_attend.at[x, column], s_of["slice"], r_slice.at[dx - 1],
            {"fs": (x + dx) % NX},
        )

    def relay_copy(dx, dy):
        part = w_attend.at[(x + NX - dx) % NX, column]
        return remote(
            part, part, s_of["relay"], r_relay.at[dx - 1, dy // 2], {"sp_1": (y + dy) % NY}
        )

    def hop_copy(dx, dy):
        start = (y + NY - dy) % NY * 128 + dy // 2 * 64
        part = w_attend.at[
            (x + NX - dx) % NX, pl.ds(pl.multiple_of(start, 64), 64)
        ]
        return remote(part, part, s_of["hop"], r_of["hop"], {"sp_1": (y + dy) % NY})

    for dy in range(1, NY):
        send(
            remote(
                packed.at[(y + dy) % NY], packed_in.at[y], s_of["packed"], r_of["packed"],
                {"sp_1": (y + dy) % NY},
            )
        )
    send(half_copy(0))
    for half in (0, 1):
        send(row_copy(1, half))
        send(row_copy(2, 1 - half))
    send(value_copy())
    for dx in (2, 1, 3):
        send(drive_copy(dx))
    for dx in (2, 1, 3):
        send(weight_copy(0, dx))
    for dx in (1, 3):
        send(weight_copy(1, dx))
    for dx in (1, 3, 2):
        send(slice_copy(dx))
    for dx in (2, 1, 3):
        send(weight_copy(2, dx))
    packed_in[y] = packed[y]
    rows_in[0, mine] = normed[...]
    keyed_w[depth, :128] = w_key[:, column]
    keyed_w[depth, 128:] = w_value[:, column]
    query_w[depth] = w_query[:, column]
    drive_w[depth] = w_drive[:, column]

    for k in (7, 8, 9, 10, 11, 12, 14, 16):
        fetches[k].wait()
    sign = jnp.where(lane[:8] < 64, -1.0, 1.0)
    groups = pl.ds(pl.multiple_of(y * 8, 8), 8)

    def side_by_side(left, right):
        return jnp.concatenate([left, right], axis=1)

    lam_real = side_by_side(lambda_real[groups, :], lambda_real[groups, :])
    lam_imag = side_by_side(lambda_imag[groups, :], lambda_imag[groups, :])
    initial = side_by_side(initial_ref[0, groups, :], initial_ref[1, groups, :])
    spot = lax.broadcasted_iota(jnp.int32, (8, 32), 1) - lax.broadcasted_iota(
        jnp.int32, (8, 32), 0
    )
    step = jnp.exp(
        jnp.sum(jnp.where(spot == y * 8, log_step_ref[...], 0.0), axis=1, keepdims=True)
    )
    log_gain, rotate = lam_real * step, lam_imag * step
    cosine, sine, magnitude = jnp.cos(rotate), jnp.sin(rotate), jnp.exp(log_gain)
    bar_real, bar_imag = magnitude * cosine, magnitude * sine
    divisor = lam_real * lam_real + lam_imag * lam_imag
    shifted = bar_real - 1.0
    factor_real = (shifted * lam_real + bar_imag * lam_imag) / divisor
    factor_imag = (bar_imag * lam_real - shifted * lam_imag) / divisor * sign
    shrink = jnp.exp(-log_gain)
    gain = (bar_real, sign * bar_imag)
    inverse = (shrink * cosine, -sign * shrink * sine)
    gains, inverses = [gain], [inverse]
    for _ in range(9):
        gains.append(powers_times(gains[-1], gains[-1]))
    for _ in range(6):
        inverses.append(powers_times(inverses[-1], inverses[-1]))
    gain_block, gain_all = gains[7], gains[9]
    gain_last = powers_times(gain_block, inverse)
    into_map[...] = jnp.zeros_like(into_map)
    out_map[...] = jnp.zeros_like(out_map)
    for g in range(8):
        cols, swapped = pl.ds(g * 128, 128), pl.ds(1024 + g * 128, 128)
        raw = side_by_side(input_map[0, y * 8 + g], input_map[1, y * 8 + g])
        entry = factor_real[g : g + 1] * raw + factor_imag[g : g + 1] * pltpu.roll(raw, 64, 1)
        turned_entry = pltpu.roll(entry, 64, 1)
        for at in (g * 16, 128 + g * 16):
            into_map[at : at + 16, cols] = entry.astype(BF16)
            into_map[at : at + 16, swapped] = turned_entry.astype(BF16)
        raw = side_by_side(output_map[0, y * 8 + g], output_map[1, y * 8 + g])
        out_map[g * 16 : g * 16 + 16, cols] = (raw * -sign[:1]).astype(BF16)
        out_map[g * 16 : g * 16 + 16, swapped] = (pltpu.roll(raw, 64, 1) * -sign[:1]).astype(BF16)
        for table_p, table_q, steps in ((fwd_p, fwd_q, gains), (inv_p, inv_q, inverses)):
            real, imag = jnp.ones((8, 128), F32), jnp.zeros((8, 128), F32)
            for bit in range(3):
                by = tuple(part[g : g + 1] for part in steps[bit])
                new = powers_times((real, imag), by)
                chosen = (row[:8] & (1 << bit)) != 0
                real, imag = jnp.where(chosen, new[0], real), jnp.where(chosen, new[1], imag)
            table_p[:8, cols] = real
            table_q[:8, cols] = imag
            for bit in range(3, 7):
                n = 1 << bit
                by = tuple(part[g : g + 1] for part in steps[bit])
                new = powers_times((table_p[:n, cols], table_q[:n, cols]), by)
                table_p[n : 2 * n, cols] = new[0]
                table_q[n : 2 * n, cols] = new[1]
    ladder_row = lax.broadcasted_iota(jnp.int32, (256, 512), 0)
    ladder_lane = lax.broadcasted_iota(jnp.int32, (256, 512), 1)
    ladder[...] = jnp.where((ladder_lane >= 256) | (ladder_row >= ladder_lane), -1.0, 0.0).astype(
        BF16
    )

    def block_of(j):
        dy = j + j // 2 * (5 - 2 * j)
        return (y + NY - dy) % NY

    def right_copy(i, j):
        b = block_of(j)
        return remote(
            own_in.at[b] if i == 1 else right_in.at[i - 2, b],
            far_in.at[b] if i == 4 else right_in.at[i - 1, b],
            s_of["right"], r_right.at[4 * i - 4 + j], up,
        )

    def left_copy(i, j):
        b = block_of(j)
        return remote(
            own_in.at[b] if i == 1 else left_in.at[i - 2, b],
            far_in.at[b] if i == 4 else left_in.at[i - 1, b],
            s_of["left"], r_left.at[4 * i - 4 + j - (2 if i == 4 else 0)], down,
        )

    await_all("packed", packed_in.at[:3])
    for b in range(NY):
        offset_own[b : b + 1, :] = packed_in[b, 8:9, :]
        offset_in[0, b : b + 1, :] = packed_in[b, 8:9, :]
    offset_own[4:8, :] = jnp.zeros((4, 128), F32)
    for dz in range(1, NZ):
        send(
            remote(
                offset_own, offset_in.at[dz], s_of["offset"], r_of["offset"],
                {"sp_0": (z + dz) % NZ},
            )
        )
    value_copy().wait_recv()
    for dz in (4, 3, 5, 2, 6, 1, 7):
        send(value_share_copy(dz))
    for dx in (2, 1, 3):
        drive_copy(dx).wait_recv()
        for dz in (4, 3, 5, 2, 6, 1, 7):
            send(share_copy(dx, dz))
    until = jnp.where(lane <= row, 1.0, 0.0)
    until_half = until.astype(BF16)
    falls = []
    for b in range(NY):
        forget = packed_in[b, :8, :]
        spread = jnp.concatenate(
            [jnp.broadcast_to(forget[g : g + 1], (16, 128)) for g in range(8)], axis=0
        )
        decay[b] = lax.dot_general(
            until, spread, (((1,), (1,)), ((), ())), preferred_element_type=F32,
            precision=lax.Precision.HIGHEST,
        )
        falls.append(jnp.sum(forget, axis=1, keepdims=True))
    for half in (0, 1):
        row_copy(1, half).wait_recv()
        row_copy(2, 1 - half).wait_recv()
        for j in (1, 2):
            send(half_copy(j) if half else far_row_copy(j))
    await_all("far_rows", rows_in.at[3, :64])
    send(half_copy(3))
    await_all("keyed", keyed_w.at[:1280])
    await_all("values", drive_w.at[:448])
    await_all("half", rows_in.at[:2])
    product = jnp.dot(
        rows_in[...].reshape(512, 2048), keyed_w[...], preferred_element_type=F32
    ).astype(BF16)
    for j in range(NY):
        own_in[block_of(j)] = product[j * 128 : (j + 1) * 128]
        right_copy(1, j).start()
        left_copy(1, j).start()
    def arrive(i, blocks=range(NY)):
        for j in blocks:
            if i < 4 or j < 2:
                right_copy(i, j).wait_recv()
                if i < 3 or i == 3 and j < 2:
                    right_copy(i + 1, j).start()
            if i < 4 or j >= 2:
                left_copy(i, j).wait_recv()
                if i < 3 or i == 3 and j >= 2:
                    left_copy(i + 1, j).start()

    def offset_row(dz):
        return jnp.concatenate([offset_in[dz, b : b + 1, :] for b in range(NY)], axis=1)

    def attend_far(dz, pairs):
        @pl.when(z >= dz)
        def _():
            acc[dz], tot[dz] = attend_chunk(
                queries[...].reshape(512, 128), pairs[...].reshape(512, 256), offset_row(dz),
                ladder[...],
            )

    def attend_step(i):
        attend_far(i, right_in.at[i - 1])
        attend_far(8 - i, left_in.at[i - 1])

    def pass_slice(dx):
        slice_copy(dx).wait_recv()
        for dy in (1, 3):
            send(relay_copy(dx, dy))

    def pass_on(dx):
        for dy in (1, 3):
            relay_copy(dx, dy).wait_recv()
            send(hop_copy(dx, dy))

    pass_slice(1)
    arrive(1, (0,))
    await_all("share", drive_w.at[:1344])
    product = jnp.dot(
        rows_in[...].reshape(512, 2048), drive_w[...], preferred_element_type=F32
    ).astype(BF16)
    for j in range(NY):
        driven_in[block_of(j)] = product[j * 128 : (j + 1) * 128]
    local = jnp.zeros((8, 128), F32)
    fall_all = jnp.zeros((8, 1), F32)
    for b in range(NY):
        driven = driven_in[b].astype(F32) * jnp.exp(-decay[b])
        entered = jnp.dot(
            jnp.concatenate(high_low(driven), axis=1), into_map[...], preferred_element_type=F32
        )
        unturned = entered[:, :1024] * inv_p[...] + entered[:, 1024:] * inv_q[...]
        high, low = high_low(unturned)
        held[b] = jnp.dot(until_half, high, preferred_element_type=F32) + jnp.dot(
            until_half, low, preferred_element_type=F32
        )
        for g in range(8):
            ends[b, g : g + 1, :] = held[b, 127:128, g * 128 : (g + 1) * 128]
        fall_all = fall_all + falls[b]
        falls[b] = jnp.exp(falls[b])
        ends[b] = falls[b] * turned(gain_last, ends[b])
        local = falls[b] * turned(gain_block, local) + ends[b]
        if b == 1:
            pass_slice(3)
        if b < 3:
            arrive(1, (b + 1,))
    state_own[:8, :] = local
    state_own[8:, :] = jnp.broadcast_to(fall_all, (8, 128))
    for dz in range(1, NZ):
        send(
            remote(
                state_own, state_in.at[dz], s_of["state"], r_of["state"],
                {"sp_0": (z + dz) % NZ},
            )
        )

    pass_slice(2)
    pass_on(1)
    await_all("query", query_w.at[:1536])
    product = jnp.dot(
        rows_in[...].reshape(512, 2048), query_w[...], preferred_element_type=F32
    )
    product = (product * (LOG2E * 128**-0.5)).astype(BF16)
    for j in range(NY):
        queries[block_of(j)] = product[j * 128 : (j + 1) * 128]

    arrive(2, (0, 1))
    pass_on(3)
    acc[0], tot[0] = attend_chunk(
        queries[...].reshape(512, 128), own_in[...].reshape(512, 256), offset_row(0), ladder[...],
        lax.broadcasted_iota(jnp.int32, (512, 512), 1)
        < lax.broadcasted_iota(jnp.int32, (512, 512), 0),
    )
    await_all("offset", offset_in.at[:7])
    pass_on(2)

    await_all("state", state_in.at[:7])
    carry = initial
    for source in range(NZ - 1):
        arrived = state_in[jnp.maximum(z - source, 1)]
        moved = jnp.exp(arrived[8:]) * turned(gain_all, carry) + arrived[:8]
        carry = jnp.where(source < z, moved, carry)
    for b in range(NY):
        entering = turned(gain, carry)
        whole = jnp.concatenate(
            [held[b, :, g * 128 : (g + 1) * 128] + entering[g : g + 1] for g in range(8)], axis=1
        )
        turned_states = jnp.concatenate(
            [(whole * fwd_p[...]).astype(BF16), (whole * fwd_q[...]).astype(BF16)], axis=1
        )
        read = lax.dot_general(
            turned_states, out_map[...], (((1,), (1,)), ((), ())), preferred_element_type=F32
        )
        read = read * jnp.exp(decay[b]) + skip_ref[pl.ds(y, 1), :] * driven_in[b].astype(F32)
        inner = math.sqrt(2.0 / math.pi) * (read + 0.044715 * (read * read * read))
        scan_own[b] = (0.5 * read * (1.0 + jnp.tanh(inner))).astype(BF16)
        carry = falls[b] * turned(gain_block, carry) + ends[b]

    for dx in (2, 1, 3, 0):
        for dy in (2, 1, 3, 0):
            if (dx, dy) != (0, 0):
                send(
                    remote(
                        scan_own.at[(y + dy) % NY], scan_in.at[dx, dy], s_of["scan"],
                        r_of["scan"], {"fs": (x + dx) % NX, "sp_1": (y + dy) % NY},
                    )
                )
    scan_in[0, 0] = scan_own[y]
    arrive(2, (2, 3))
    attend_step(1)
    arrive(3, (0, 1))
    attend_step(2)
    arrive(3, (2, 3))
    attend_step(3)

    def join(near, far):
        @pl.when(z >= far)
        def _():
            fallen = tot[near, :, :1]
            acc[near] += jnp.exp2(fallen) * acc[far]
            tot[near, :, :1] = fallen + tot[far, :, :1]

    for dz in (1, 2, 3):
        join(0, dz)
    for dz in (6, 7):
        join(5, dz)
    other = pl.ds(pl.multiple_of((1 - t) * 64, 64), 64)
    await_all("scan", drive_w.at[:1920])
    for dx in order:
        total = None
        for dy in range(NY):
            head = (y + NY - dy) % NY
            head_rows = pl.ds(pl.multiple_of(head * 128, 128), 128)
            product = jnp.dot(scan_in[dx, dy], w_scan[head_rows, :], preferred_element_type=F32)
            total = product if total is None else total + product
        scan_product[dx] = total
        pre_out[dx] = scan_product[dx, other, :].astype(BF16)
        send(remote(pre_out.at[dx], pre_in.at[dx], s_of["pre"], r_of["pre"], sibling))
    arrive(4)
    attend_far(4, far_in)
    for dz in (4, 5):
        join(0, dz)
    attend_own[...] = acc[0].astype(BF16).reshape(NY, 128, 128)
    for dy in (2, 1, 3):
        send(
            remote(
                attend_own.at[(y + dy) % NY], attend_in.at[:, column], s_of["attend"],
                r_of["attend"], {"sp_1": (y + dy) % NY},
            )
        )
    attend_in[:, column] = attend_own[y]
    await_all("pre", pre_in)
    for dx in (2, 1, 3):
        part_out[dx] = (scan_product[dx, mine, :] + pre_in[dx].astype(F32)).astype(BF16)
        send(
            remote(
                part_out.at[dx], part_in.at[dx], s_of["part"], r_of["part"],
                {"fs": (x + NX - dx) % NX},
            )
        )

    await_all("hop", w_attend.at[0, :384])
    await_all("attend", drive_w.at[:384])
    for k in range(NX):
        product_own[k] = jnp.dot(attend_in[...], w_attend[k], preferred_element_type=F32)
        half_out[k] = product_own[k, other, :].astype(BF16)
        send(remote(half_out.at[k], half_in.at[k], s_of["last"], r_of["last"], sibling))
    await_all("last", half_in)
    await_all("part", w_attend.at[0, :192])
    for dx in order:
        k = (x + dx) % NX
        columns = pl.ds(pl.multiple_of(k * 512, 512), 512)
        scan_part = scan_product[0, mine, :] + pre_in[0].astype(F32)
        if dx:
            scan_part = part_in[dx].astype(F32)
        out[:, columns] = (product_own[k, mine, :] + half_in[k].astype(F32) + scan_part).astype(BF16)
    for name, data in {
        "rows": rows_in.at[:2, :64],
        "half": rows_in.at[:2],
        "keyed": keyed_w.at[:1280],
        "values": drive_w.at[:448],
        "far_rows": rows_in.at[3, :64],
        "query": query_w.at[:1536],
        "packed": packed_in.at[:3],
        "right": w_attend.at[:2, :448],
        "left": w_attend.at[:2, :448],
        "offset": offset_in.at[:7],
        "state": state_in.at[:7],
        "scan": drive_w.at[:1920],
        "pre": pre_in,
        "part": w_attend.at[0, :192],
        "slice": w_attend.at[0, :384],
        "relay": w_attend.at[:3, :256],
        "hop": w_attend.at[0, :384],
        "attend": drive_w.at[:384],
        "last": half_in,
        "drive": drive_w.at[:256],
        "share": drive_w.at[:1344],
    }.items():
        remote(data, data, s_of[name], r_rows.at[0], sibling).wait_send()


def layer(*operands):
    return pl.pallas_call(
        layer_kernel,
        out_shape=pltpu.VMEM((64, 2048), BF16),
        in_specs=[pl.BlockSpec(memory_space=pl.ANY)] * 17,
        out_specs=VMEM,
        scratch_shapes=[
            *(
                pltpu.VMEM((NX, 512, 512) if k == 15 else operand.shape, operand.dtype)
                for k, operand in enumerate(operands)
            ),
            pltpu.SemaphoreType.DMA((17,)),
            pltpu.VMEM((64, 2048), BF16),
            pltpu.VMEM((NY, 128, 2048), BF16),
            pltpu.VMEM((2048, 256), BF16),
            pltpu.VMEM((2048, 128), BF16),
            pltpu.VMEM((2048, 128), BF16),
            pltpu.VMEM((NY, 16, 128), F32),
            pltpu.VMEM((NY, 16, 128), F32),
            pltpu.VMEM((NY, 128, 128), BF16),
            pltpu.VMEM((NY, 128, 128), BF16),
            pltpu.VMEM((NY, 128, 256), BF16),
            pltpu.VMEM((3, NY, 128, 256), BF16),
            pltpu.VMEM((3, NY, 128, 256), BF16),
            pltpu.VMEM((NY, 128, 256), BF16),
            pltpu.VMEM((8, 128), F32),
            pltpu.VMEM((NZ, 8, 128), F32),
            pltpu.VMEM((16, 128), F32),
            pltpu.VMEM((NZ, 16, 128), F32),
            pltpu.VMEM((NZ, 512, 128), F32),
            pltpu.VMEM((NZ, 512, 128), F32),
            pltpu.VMEM((256, 512), BF16),
            pltpu.VMEM((256, 2048), BF16),
            pltpu.VMEM((128, 2048), BF16),
            pltpu.VMEM((128, 1024), F32),
            pltpu.VMEM((128, 1024), F32),
            pltpu.VMEM((128, 1024), F32),
            pltpu.VMEM((128, 1024), F32),
            pltpu.VMEM((NY, 128, 1024), F32),
            pltpu.VMEM((NY, 8, 128), F32),
            pltpu.VMEM((NY, 128, 128), F32),
            pltpu.VMEM((NY, 128, 128), BF16),
            pltpu.VMEM((NY, 128, 128), BF16),
            pltpu.VMEM((128, 512), BF16),
            pltpu.VMEM((NX, NY, 128, 128), BF16),
            pltpu.VMEM((NX, 64, 512), BF16),
            pltpu.VMEM((NX, 64, 512), BF16),
            pltpu.VMEM((NX, 128, 512), F32),
            pltpu.VMEM((NX, 64, 512), BF16),
            pltpu.VMEM((NX, 64, 512), BF16),
            pltpu.VMEM((NX, 128, 512), F32),
            pltpu.VMEM((NX, 64, 512), BF16),
            pltpu.VMEM((NX, 64, 512), BF16),
            *(
                pltpu.SemaphoreType.DMA(shape)
                for shape in (
                    (len(SENT),), (len(TOGETHER),), (4,), (14,), (14,), (3,), (3, 2), (4,)
                )
            ),
        ],
        compiler_params=pltpu.CompilerParams(
            collective_id=0, has_side_effects=True, vmem_limit_bytes=60 << 20
        ),
        name="layer",
    )(*operands)


def on_device(
    tokens, norm_gain, drive_weight, query_weight, key_weight, value_weight, key_offset, log_step,
    lambda_real, lambda_imag, input_map, output_map, skip_gain, forget, initial_state,
    scan_out_weight, attend_out_weight,
):
    return layer(
        tokens[0],
        norm_gain[None],
        drive_weight,
        query_weight,
        key_weight,
        value_weight,
        key_offset[:, 0, :],
        log_step[None],
        lambda_real,
        lambda_imag,
        input_map.transpose(0, 1, 3, 2),
        output_map,
        skip_gain.reshape(NY, 128),
        forget.reshape(NY, 8, 128),
        initial_state[:, 0],
        attend_out_weight,
        scan_out_weight,
    )[None]


def solution(mesh):
    split = Mesh(
        mesh.devices.reshape(NZ, NY, mesh.shape["fs"], mesh.shape["tp"]),
        ("sp_0", "sp_1", "fs", "tp"),
    )
    in_specs = (
        P("fs", SP_TP, None),
        P(),
        P("fs", "tp"),
        P("fs", "tp"),
        P("fs", "tp"),
        P("fs", "tp"),
        P("tp", "fs", SP),
        P("tp"),
        P("tp", None),
        P("tp", None),
        P(None, "tp", None, None),
        P(None, "tp", None, None),
        P("tp"),
        P("tp", "fs", SP),
        P(None, "fs", "tp", None),
        P("tp", "fs"),
        P("tp", "fs"),
    )
    return jax.shard_map(
        on_device, mesh=split, in_specs=in_specs, out_specs=P("fs", SP_TP, None), check_vma=False
    )
```

```python
import math

import jax
import jax.numpy as jnp
from jax import lax
from jax.experimental import pallas as pl
from jax.experimental.pallas import tpu as pltpu
from jax.sharding import Mesh
from jax.sharding import PartitionSpec as P

SP_TP = ("sp_0", "sp_1", "tp")
SP = ("sp_0", "sp_1")
EPSILON = 1e-06
LOG2E = 1.4426950408889634
NZ, NY, NX, NT = 8, 4, 4, 2
BF16, F32 = jnp.bfloat16, jnp.float32
TOGETHER = (
    "half", "keyed", "query", "packed", "offset", "state", "scan", "pre", "part", "hop", "attend",
    "last", "share", "far_rows", "values",
)
SENT = TOGETHER + ("rows", "right", "left", "slice", "relay", "drive")
VMEM = pl.BlockSpec(memory_space=pltpu.VMEM)
MESH_ID = pl.DeviceIdType.MESH


def remote(src, dst, send_sem, recv_sem, where):
    return pltpu.make_async_remote_copy(
        src_ref=src, dst_ref=dst, send_sem=send_sem, recv_sem=recv_sem,
        device_id=where, device_id_type=MESH_ID,
    )


def greet(peers):
    barrier = pltpu.get_barrier_semaphore()
    for peer in peers:
        pl.semaphore_signal(barrier, inc=1, device_id=peer, device_id_type=MESH_ID)


def await_greetings(count):
    pl.semaphore_wait(pltpu.get_barrier_semaphore(), count)


def plane_peers(x, y, t):
    peers = [
        {"fs": (x + dx) % NX, "tp": (t + dt) % NT}
        for dx in range(NX) for dt in range(NT) if (dx, dt) != (0, 0)
    ]
    peers += [
        {"fs": (x + dx) % NX, "sp_1": (y + dy) % NY} for dx in range(NX) for dy in range(1, NY)
    ]
    return peers


def high_low(value):
    high = value.astype(BF16)
    return high, (value - high.astype(F32)).astype(BF16)


def attend_chunk(query, pairs, offset, ladder, visible=None):
    keys, values = pairs[:, :128], pairs[:, 128:]
    score = lax.dot_general(query, keys, (((1,), (1,)), ((), ())), preferred_element_type=F32)
    score = score + offset
    soft = jnp.maximum(score, LOG2E * jnp.log(1.0 + jnp.exp2(jnp.minimum(score, 126.0))))
    if visible is not None:
        soft = jnp.where(visible, soft, 0.0)
    soft = soft.astype(BF16)
    last = jnp.dot(soft[:, 256:], ladder[:, :256], preferred_element_type=F32)
    first = jnp.dot(soft[:, :256], ladder[:, :256], preferred_element_type=F32) + jnp.dot(
        soft[:, 256:], ladder[:, 256:], preferred_element_type=F32
    )
    weight = jnp.exp2(score + jnp.concatenate([first, last], axis=1))
    if visible is not None:
        weight = jnp.where(visible, weight, 0.0)
    return jnp.dot(weight.astype(BF16), values, preferred_element_type=F32), first[:, :128]


def turned(gain, state):
    return gain[0] * state + gain[1] * pltpu.roll(state, 64, 1)


def powers_times(left, right):
    return (
        left[0] * right[0] - left[1] * right[1],
        left[1] * right[0] + left[0] * right[1],
    )


def layer_kernel(
    *refs,
):
    operands, out, held_here, rest = refs[:17], refs[17], refs[18:35], refs[35:]
    run_layer(operands, out, held_here, *rest)


def run_layer(
    operands, out, held_here, s_operand,
    normed, rows_in, keyed_w, query_w, drive_w, packed, packed_in, driven_in, queries,
    own_in, right_in, left_in, far_in, offset_own, offset_in, state_own, state_in, acc, tot,
    ladder, into_map, out_map, fwd_p, fwd_q, inv_p, inv_q, held, ends, decay,
    attend_own, scan_own, attend_in, scan_in, part_out, part_in, product_own, half_out, half_in,
    scan_product, pre_out, pre_in,
    s_all, r_all, r_rows, r_right, r_left, r_slice, r_relay, r_drive,
):
    (
        tok, gain_ref, w_drive, w_query, w_key, w_value, key_offset, log_step_ref, lambda_real,
        lambda_imag, input_map, output_map, skip_ref, forget_ref, initial_ref, w_attend, w_scan,
    ) = held_here
    z, y, x, t = (lax.axis_index(a) for a in ("sp_0", "sp_1", "fs", "tp"))
    fetches = [
        pltpu.make_async_copy(src, dst.at[x] if k == 15 else dst, s_operand.at[k])
        for k, (src, dst) in enumerate(zip(operands, held_here))
    ]
    for fetch in fetches:
        fetch.start()
    greet(plane_peers(x, y, t) + [{"sp_0": (z + dz) % NZ} for dz in range(1, NZ)])
    row = lax.broadcasted_iota(jnp.int32, (128, 128), 0)
    lane = lax.broadcasted_iota(jnp.int32, (128, 128), 1)
    up, down = {"sp_0": (z + 1) % NZ}, {"sp_0": (z + NZ - 1) % NZ}
    s_of = {name: s_all.at[k] for k, name in enumerate(SENT)}
    r_of = {name: r_all.at[k] for k, name in enumerate(TOGETHER)}

    def send(copy):
        copy.start()
        return copy

    def await_all(name, data):
        remote(data, data, s_of[name], r_of[name], sibling).wait_recv()

    for k in (0, 1, 6, 13):
        fetches[k].wait()
    packed[:, :8, :] = forget_ref[...]
    packed[:, 8:, :] = jnp.zeros((NY, 8, 128), F32)
    offsets = key_offset[...].astype(F32) * LOG2E
    for k in range(NY):
        packed[k, 8:9, :] = offsets[k : k + 1]
    values = tok[...].astype(F32)
    scale = lax.rsqrt(jnp.mean(values * values, axis=1, keepdims=True) + EPSILON)
    normed[...] = (values * scale * gain_ref[...]).astype(BF16)
    for k in (2, 3, 4, 5, 15):
        fetches[k].wait()
    await_greetings(26)

    order = (0, 1, 3, 2)
    mine = pl.ds(pl.multiple_of(t * 64, 64), 64)
    sibling = {"tp": 1 - t}

    def quarter(half):
        return pl.ds(pl.multiple_of(t * 64 + half * 32, 32), 32)

    def row_copy(j, half):
        return remote(
            normed.at[pl.ds(half * 32, 32)], rows_in.at[j, quarter(half)], s_of["rows"],
            r_rows.at[2 * j - 2 + half], {"sp_1": (y + order[j]) % NY},
        )

    def far_row_copy(j):
        part = quarter(j - 1)
        return remote(
            rows_in.at[j, part], rows_in.at[3, part], s_of["far_rows"], r_of["far_rows"],
            {"sp_1": (y + order[j]) % NY},
        )

    def half_copy(j):
        return remote(
            rows_in.at[j, mine] if j else normed, rows_in.at[j, mine], s_of["half"], r_of["half"],
            sibling,
        )

    column = pl.ds(pl.multiple_of(y * 128, 128), 128)
    depth = pl.ds(pl.multiple_of(x * 512, 512), 512)
    sources = (w_key, w_value, w_query)
    targets = (keyed_w.at[depth, :128], keyed_w.at[depth, 128:], query_w.at[depth])

    def weight_copy(kind, dx):
        group = "query" if kind == 2 else "keyed"
        return remote(
            sources[kind].at[:, column], targets[kind], s_of[group], r_of[group],
            {"fs": (x + dx) % NX},
        )

    def eighth(k):
        return drive_w.at[pl.ds(pl.multiple_of(k * 512 + z * 64, 64), 64)]

    def drive_copy(dx):
        return remote(
            w_drive.at[pl.ds(pl.multiple_of(z * 64, 64), 64), column], eighth(x), s_of["drive"],
            r_drive.at[dx - 1], {"fs": (x + dx) % NX},
        )

    def value_eighth(k):
        return keyed_w.at[pl.ds(pl.multiple_of(k * 512 + z * 64, 64), 64), 128:]

    def value_copy():
        return remote(
            w_value.at[pl.ds(pl.multiple_of(z * 64, 64), 64), column], value_eighth(x),
            s_of["drive"], r_drive.at[3], {"fs": (x + 2) % NX},
        )

    def value_share_copy(dz):
        part = value_eighth((x + 2) % NX)
        return remote(part, part, s_of["values"], r_of["values"], {"sp_0": (z + dz) % NZ})

    def share_copy(dx, dz):
        part = eighth((x + NX - dx) % NX)
        return remote(
            part, part, s_of["share"], r_of["share"], {"sp_0": (z + dz) % NZ}
        )

    def slice_copy(dx):
        return remote(
            w_attend.at[x, column], w_attend.at[x, column], s_of["slice"], r_slice.at[dx - 1],
            {"fs": (x + dx) % NX},
        )

    def relay_copy(dx, dy):
        part = w_attend.at[(x + NX - dx) % NX, column]
        return remote(
            part, part, s_of["relay"], r_relay.at[dx - 1, dy // 2], {"sp_1": (y + dy) % NY}
        )

    def hop_copy(dx, dy):
        start = (y + NY - dy) % NY * 128 + dy // 2 * 64
        part = w_attend.at[
            (x + NX - dx) % NX, pl.ds(pl.multiple_of(start, 64), 64)
        ]
        return remote(part, part, s_of["hop"], r_of["hop"], {"sp_1": (y + dy) % NY})

    for dy in range(1, NY):
        send(
            remote(
                packed.at[(y + dy) % NY], packed_in.at[y], s_of["packed"], r_of["packed"],
                {"sp_1": (y + dy) % NY},
            )
        )
    send(half_copy(0))
    for half in (0, 1):
        send(row_copy(1, half))
        send(row_copy(2, 1 - half))
    send(value_copy())
    for dx in (2, 1, 3):
        send(drive_copy(dx))
    for dx in (2, 1, 3):
        send(weight_copy(0, dx))
    for dx in (1, 3):
        send(weight_copy(1, dx))
    for dx in (1, 3, 2):
        send(slice_copy(dx))
    for dx in (2, 1, 3):
        send(weight_copy(2, dx))
    packed_in[y] = packed[y]
    rows_in[0, mine] = normed[...]
    keyed_w[depth, :128] = w_key[:, column]
    keyed_w[depth, 128:] = w_value[:, column]
    query_w[depth] = w_query[:, column]
    drive_w[depth] = w_drive[:, column]

    for k in (7, 8, 9, 10, 11, 12, 14, 16):
        fetches[k].wait()
    sign = jnp.where(lane[:8] < 64, -1.0, 1.0)
    groups = pl.ds(pl.multiple_of(y * 8, 8), 8)

    def side_by_side(left, right):
        return jnp.concatenate([left, right], axis=1)

    lam_real = side_by_side(lambda_real[groups, :], lambda_real[groups, :])
    lam_imag = side_by_side(lambda_imag[groups, :], lambda_imag[groups, :])
    initial = side_by_side(initial_ref[0, groups, :], initial_ref[1, groups, :])
    spot = lax.broadcasted_iota(jnp.int32, (8, 32), 1) - lax.broadcasted_iota(
        jnp.int32, (8, 32), 0
    )
    step = jnp.exp(
        jnp.sum(jnp.where(spot == y * 8, log_step_ref[...], 0.0), axis=1, keepdims=True)
    )
    log_gain, rotate = lam_real * step, lam_imag * step
    cosine, sine, magnitude = jnp.cos(rotate), jnp.sin(rotate), jnp.exp(log_gain)
    bar_real, bar_imag = magnitude * cosine, magnitude * sine
    divisor = lam_real * lam_real + lam_imag * lam_imag
    shifted = bar_real - 1.0
    factor_real = (shifted * lam_real + bar_imag * lam_imag) / divisor
    factor_imag = (bar_imag * lam_real - shifted * lam_imag) / divisor * sign
    shrink = jnp.exp(-log_gain)
    gain = (bar_real, sign * bar_imag)
    inverse = (shrink * cosine, -sign * shrink * sine)
    gains, inverses = [gain], [inverse]
    for _ in range(9):
        gains.append(powers_times(gains[-1], gains[-1]))
    for _ in range(6):
        inverses.append(powers_times(inverses[-1], inverses[-1]))
    gain_block, gain_all = gains[7], gains[9]
    gain_last = powers_times(gain_block, inverse)
    into_map[...] = jnp.zeros_like(into_map)
    out_map[...] = jnp.zeros_like(out_map)
    for g in range(8):
        cols, swapped = pl.ds(g * 128, 128), pl.ds(1024 + g * 128, 128)
        raw = side_by_side(input_map[0, y * 8 + g], input_map[1, y * 8 + g])
        entry = factor_real[g : g + 1] * raw + factor_imag[g : g + 1] * pltpu.roll(raw, 64, 1)
        turned_entry = pltpu.roll(entry, 64, 1)
        for at in (g * 16, 128 + g * 16):
            into_map[at : at + 16, cols] = entry.astype(BF16)
            into_map[at : at + 16, swapped] = turned_entry.astype(BF16)
        raw = side_by_side(output_map[0, y * 8 + g], output_map[1, y * 8 + g])
        out_map[g * 16 : g * 16 + 16, cols] = (raw * -sign[:1]).astype(BF16)
        out_map[g * 16 : g * 16 + 16, swapped] = (pltpu.roll(raw, 64, 1) * -sign[:1]).astype(BF16)
        for table_p, table_q, steps in ((fwd_p, fwd_q, gains), (inv_p, inv_q, inverses)):
            real, imag = jnp.ones((8, 128), F32), jnp.zeros((8, 128), F32)
            for bit in range(3):
                by = tuple(part[g : g + 1] for part in steps[bit])
                new = powers_times((real, imag), by)
                chosen = (row[:8] & (1 << bit)) != 0
                real, imag = jnp.where(chosen, new[0], real), jnp.where(chosen, new[1], imag)
            table_p[:8, cols] = real
            table_q[:8, cols] = imag
            for bit in range(3, 7):
                n = 1 << bit
                by = tuple(part[g : g + 1] for part in steps[bit])
                new = powers_times((table_p[:n, cols], table_q[:n, cols]), by)
                table_p[n : 2 * n, cols] = new[0]
                table_q[n : 2 * n, cols] = new[1]
    ladder_row = lax.broadcasted_iota(jnp.int32, (256, 512), 0)
    ladder_lane = lax.broadcasted_iota(jnp.int32, (256, 512), 1)
    ladder[...] = jnp.where((ladder_lane >= 256) | (ladder_row >= ladder_lane), -1.0, 0.0).astype(
        BF16
    )

    def block_of(j):
        dy = j + j // 2 * (5 - 2 * j)
        return (y + NY - dy) % NY

    def right_copy(i, j):
        b = block_of(j)
        return remote(
            own_in.at[b] if i == 1 else right_in.at[i - 2, b],
            far_in.at[b] if i == 4 else right_in.at[i - 1, b],
            s_of["right"], r_right.at[4 * i - 4 + j], up,
        )

    def left_copy(i, j):
        b = block_of(j)
        return remote(
            own_in.at[b] if i == 1 else left_in.at[i - 2, b],
            far_in.at[b] if i == 4 else left_in.at[i - 1, b],
            s_of["left"], r_left.at[4 * i - 4 + j - (2 if i == 4 else 0)], down,
        )

    await_all("packed", packed_in.at[:3])
    for b in range(NY):
        offset_own[b : b + 1, :] = packed_in[b, 8:9, :]
        offset_in[0, b : b + 1, :] = packed_in[b, 8:9, :]
    offset_own[4:8, :] = jnp.zeros((4, 128), F32)
    for dz in range(1, NZ):
        send(
            remote(
                offset_own, offset_in.at[dz], s_of["offset"], r_of["offset"],
                {"sp_0": (z + dz) % NZ},
            )
        )
    value_copy().wait_recv()
    for dz in (4, 3, 5, 2, 6, 1, 7):
        send(value_share_copy(dz))
    for dx in (2, 1, 3):
        drive_copy(dx).wait_recv()
        for dz in (4, 3, 5, 2, 6, 1, 7):
            send(share_copy(dx, dz))
    until = jnp.where(lane <= row, 1.0, 0.0)
    until_half = until.astype(BF16)
    falls = []
    for b in range(NY):
        forget = packed_in[b, :8, :]
        spread = jnp.concatenate(
            [jnp.broadcast_to(forget[g : g + 1], (16, 128)) for g in range(8)], axis=0
        )
        decay[b] = lax.dot_general(
            until, spread, (((1,), (1,)), ((), ())), preferred_element_type=F32,
            precision=lax.Precision.HIGHEST,
        )
        falls.append(jnp.sum(forget, axis=1, keepdims=True))
    for half in (0, 1):
        row_copy(1, half).wait_recv()
        row_copy(2, 1 - half).wait_recv()
        for j in (1, 2):
            send(half_copy(j) if half else far_row_copy(j))
    await_all("far_rows", rows_in.at[3, :64])
    send(half_copy(3))
    await_all("keyed", keyed_w.at[:1280])
    await_all("values", drive_w.at[:448])
    await_all("half", rows_in.at[:2])
    product = jnp.dot(
        rows_in[...].reshape(512, 2048), keyed_w[...], preferred_element_type=F32
    ).astype(BF16)
    for j in range(NY):
        own_in[block_of(j)] = product[j * 128 : (j + 1) * 128]
        right_copy(1, j).start()
        left_copy(1, j).start()
    def arrive(i, blocks=range(NY)):
        for j in blocks:
            if i < 4 or j < 2:
                right_copy(i, j).wait_recv()
                if i < 3 or i == 3 and j < 2:
                    right_copy(i + 1, j).start()
            if i < 4 or j >= 2:
                left_copy(i, j).wait_recv()
                if i < 3 or i == 3 and j >= 2:
                    left_copy(i + 1, j).start()

    def offset_row(dz):
        return jnp.concatenate([offset_in[dz, b : b + 1, :] for b in range(NY)], axis=1)

    def attend_far(dz, pairs):
        @pl.when(z >= dz)
        def _():
            acc[dz], tot[dz] = attend_chunk(
                queries[...].reshape(512, 128), pairs[...].reshape(512, 256), offset_row(dz),
                ladder[...],
            )

    def attend_step(i):
        attend_far(i, right_in.at[i - 1])
        attend_far(8 - i, left_in.at[i - 1])

    def pass_slice(dx):
        slice_copy(dx).wait_recv()
        for dy in (1, 3):
            send(relay_copy(dx, dy))

    def pass_on(dx):
        for dy in (1, 3):
            relay_copy(dx, dy).wait_recv()
            send(hop_copy(dx, dy))

    pass_slice(1)
    await_all("share", drive_w.at[:1344])
    product = jnp.dot(
        rows_in[...].reshape(512, 2048), drive_w[...], preferred_element_type=F32
    ).astype(BF16)
    for j in range(NY):
        driven_in[block_of(j)] = product[j * 128 : (j + 1) * 128]
    local = jnp.zeros((8, 128), F32)
    fall_all = jnp.zeros((8, 1), F32)
    for b in range(NY):
        driven = driven_in[b].astype(F32) * jnp.exp(-decay[b])
        entered = jnp.dot(
            jnp.concatenate(high_low(driven), axis=1), into_map[...], preferred_element_type=F32
        )
        unturned = entered[:, :1024] * inv_p[...] + entered[:, 1024:] * inv_q[...]
        high, low = high_low(unturned)
        held[b] = jnp.dot(until_half, high, preferred_element_type=F32) + jnp.dot(
            until_half, low, preferred_element_type=F32
        )
        for g in range(8):
            ends[b, g : g + 1, :] = held[b, 127:128, g * 128 : (g + 1) * 128]
        fall_all = fall_all + falls[b]
        falls[b] = jnp.exp(falls[b])
        ends[b] = falls[b] * turned(gain_last, ends[b])
        local = falls[b] * turned(gain_block, local) + ends[b]
        if b == 1:
            pass_slice(3)
            pass_slice(2)
        if b < 3:
            arrive(1, (b,))
    state_own[:8, :] = local
    state_own[8:, :] = jnp.broadcast_to(fall_all, (8, 128))
    for dz in range(1, NZ):
        send(
            remote(
                state_own, state_in.at[dz], s_of["state"], r_of["state"],
                {"sp_0": (z + dz) % NZ},
            )
        )

    arrive(1, (3,))
    arrive(2, (0,))
    pass_on(1)
    arrive(2, (1,))
    await_all("query", query_w.at[:1536])
    product = jnp.dot(
        rows_in[...].reshape(512, 2048), query_w[...], preferred_element_type=F32
    )
    product = (product * (LOG2E * 128**-0.5)).astype(BF16)
    for j in range(NY):
        queries[block_of(j)] = product[j * 128 : (j + 1) * 128]

    arrive(2, (2,))
    acc[0], tot[0] = attend_chunk(
        queries[...].reshape(512, 128), own_in[...].reshape(512, 256), offset_row(0), ladder[...],
        lax.broadcasted_iota(jnp.int32, (512, 512), 1)
        < lax.broadcasted_iota(jnp.int32, (512, 512), 0),
    )
    await_all("offset", offset_in.at[:7])
    pass_on(3)
    arrive(2, (3,))
    arrive(3, (0,))
    attend_far(1, right_in.at[0])
    arrive(3, (1,))
    pass_on(2)

    await_all("state", state_in.at[:7])
    carry = initial
    for source in range(NZ - 1):
        arrived = state_in[jnp.maximum(z - source, 1)]
        moved = jnp.exp(arrived[8:]) * turned(gain_all, carry) + arrived[:8]
        carry = jnp.where(source < z, moved, carry)
    for b in range(NY):
        entering = turned(gain, carry)
        whole = jnp.concatenate(
            [held[b, :, g * 128 : (g + 1) * 128] + entering[g : g + 1] for g in range(8)], axis=1
        )
        turned_states = jnp.concatenate(
            [(whole * fwd_p[...]).astype(BF16), (whole * fwd_q[...]).astype(BF16)], axis=1
        )
        read = lax.dot_general(
            turned_states, out_map[...], (((1,), (1,)), ((), ())), preferred_element_type=F32
        )
        read = read * jnp.exp(decay[b]) + skip_ref[pl.ds(y, 1), :] * driven_in[b].astype(F32)
        inner = math.sqrt(2.0 / math.pi) * (read + 0.044715 * (read * read * read))
        scan_own[b] = (0.5 * read * (1.0 + jnp.tanh(inner))).astype(BF16)
        carry = falls[b] * turned(gain_block, carry) + ends[b]

    for dx in (2, 1, 3, 0):
        for dy in (2, 1, 3, 0):
            if (dx, dy) != (0, 0):
                send(
                    remote(
                        scan_own.at[(y + dy) % NY], scan_in.at[dx, dy], s_of["scan"],
                        r_of["scan"], {"fs": (x + dx) % NX, "sp_1": (y + dy) % NY},
                    )
                )
    scan_in[0, 0] = scan_own[y]
    arrive(3, (2,))
    attend_far(7, left_in.at[0])
    arrive(3, (3,))
    attend_step(2)
    attend_step(3)

    def join(near, far):
        @pl.when(z >= far)
        def _():
            fallen = tot[near, :, :1]
            acc[near] += jnp.exp2(fallen) * acc[far]
            tot[near, :, :1] = fallen + tot[far, :, :1]

    for dz in (1, 2, 3):
        join(0, dz)
    for dz in (6, 7):
        join(5, dz)
    arrive(4)
    attend_far(4, far_in)
    for dz in (4, 5):
        join(0, dz)
    attend_own[...] = acc[0].astype(BF16).reshape(NY, 128, 128)
    for dy in (2, 1, 3):
        send(
            remote(
                attend_own.at[(y + dy) % NY], attend_in.at[:, column], s_of["attend"],
                r_of["attend"], {"sp_1": (y + dy) % NY},
            )
        )
    attend_in[:, column] = attend_own[y]
    other = pl.ds(pl.multiple_of((1 - t) * 64, 64), 64)
    await_all("scan", drive_w.at[:1920])
    for dx in order:
        total = None
        for dy in range(NY):
            head = (y + NY - dy) % NY
            head_rows = pl.ds(pl.multiple_of(head * 128, 128), 128)
            product = jnp.dot(scan_in[dx, dy], w_scan[head_rows, :], preferred_element_type=F32)
            total = product if total is None else total + product
        scan_product[dx] = total
        pre_out[dx] = scan_product[dx, other, :].astype(BF16)
        send(remote(pre_out.at[dx], pre_in.at[dx], s_of["pre"], r_of["pre"], sibling))
    await_all("hop", w_attend.at[0, :384])
    await_all("attend", drive_w.at[:384])
    for k in range(NX):
        product_own[k] = jnp.dot(attend_in[...], w_attend[k], preferred_element_type=F32)
        half_out[k] = product_own[k, other, :].astype(BF16)
        send(remote(half_out.at[k], half_in.at[k], s_of["last"], r_of["last"], sibling))
    await_all("pre", pre_in)
    for dx in (2, 1, 3):
        part_out[dx] = (scan_product[dx, mine, :] + pre_in[dx].astype(F32)).astype(BF16)
        send(
            remote(
                part_out.at[dx], part_in.at[dx], s_of["part"], r_of["part"],
                {"fs": (x + NX - dx) % NX},
            )
        )
    await_all("last", half_in)
    await_all("part", w_attend.at[0, :192])
    for dx in order:
        k = (x + dx) % NX
        columns = pl.ds(pl.multiple_of(k * 512, 512), 512)
        scan_part = scan_product[0, mine, :] + pre_in[0].astype(F32)
        if dx:
            scan_part = part_in[dx].astype(F32)
        out[:, columns] = (product_own[k, mine, :] + half_in[k].astype(F32) + scan_part).astype(BF16)
    for name, data in {
        "rows": rows_in.at[:2, :64],
        "half": rows_in.at[:2],
        "keyed": keyed_w.at[:1280],
        "values": drive_w.at[:448],
        "far_rows": rows_in.at[3, :64],
        "query": query_w.at[:1536],
        "packed": packed_in.at[:3],
        "right": w_attend.at[:2, :448],
        "left": w_attend.at[:2, :448],
        "offset": offset_in.at[:7],
        "state": state_in.at[:7],
        "scan": drive_w.at[:1920],
        "pre": pre_in,
        "part": w_attend.at[0, :192],
        "slice": w_attend.at[0, :384],
        "relay": w_attend.at[:3, :256],
        "hop": w_attend.at[0, :384],
        "attend": drive_w.at[:384],
        "last": half_in,
        "drive": drive_w.at[:256],
        "share": drive_w.at[:1344],
    }.items():
        remote(data, data, s_of[name], r_rows.at[0], sibling).wait_send()


def layer(*operands):
    return pl.pallas_call(
        layer_kernel,
        out_shape=pltpu.VMEM((64, 2048), BF16),
        in_specs=[pl.BlockSpec(memory_space=pl.ANY)] * 17,
        out_specs=VMEM,
        scratch_shapes=[
            *(
                pltpu.VMEM((NX, 512, 512) if k == 15 else operand.shape, operand.dtype)
                for k, operand in enumerate(operands)
            ),
            pltpu.SemaphoreType.DMA((17,)),
            pltpu.VMEM((64, 2048), BF16),
            pltpu.VMEM((NY, 128, 2048), BF16),
            pltpu.VMEM((2048, 256), BF16),
            pltpu.VMEM((2048, 128), BF16),
            pltpu.VMEM((2048, 128), BF16),
            pltpu.VMEM((NY, 16, 128), F32),
            pltpu.VMEM((NY, 16, 128), F32),
            pltpu.VMEM((NY, 128, 128), BF16),
            pltpu.VMEM((NY, 128, 128), BF16),
            pltpu.VMEM((NY, 128, 256), BF16),
            pltpu.VMEM((3, NY, 128, 256), BF16),
            pltpu.VMEM((3, NY, 128, 256), BF16),
            pltpu.VMEM((NY, 128, 256), BF16),
            pltpu.VMEM((8, 128), F32),
            pltpu.VMEM((NZ, 8, 128), F32),
            pltpu.VMEM((16, 128), F32),
            pltpu.VMEM((NZ, 16, 128), F32),
            pltpu.VMEM((NZ, 512, 128), F32),
            pltpu.VMEM((NZ, 512, 128), F32),
            pltpu.VMEM((256, 512), BF16),
            pltpu.VMEM((256, 2048), BF16),
            pltpu.VMEM((128, 2048), BF16),
            pltpu.VMEM((128, 1024), F32),
            pltpu.VMEM((128, 1024), F32),
            pltpu.VMEM((128, 1024), F32),
            pltpu.VMEM((128, 1024), F32),
            pltpu.VMEM((NY, 128, 1024), F32),
            pltpu.VMEM((NY, 8, 128), F32),
            pltpu.VMEM((NY, 128, 128), F32),
            pltpu.VMEM((NY, 128, 128), BF16),
            pltpu.VMEM((NY, 128, 128), BF16),
            pltpu.VMEM((128, 512), BF16),
            pltpu.VMEM((NX, NY, 128, 128), BF16),
            pltpu.VMEM((NX, 64, 512), BF16),
            pltpu.VMEM((NX, 64, 512), BF16),
            pltpu.VMEM((NX, 128, 512), F32),
            pltpu.VMEM((NX, 64, 512), BF16),
            pltpu.VMEM((NX, 64, 512), BF16),
            pltpu.VMEM((NX, 128, 512), F32),
            pltpu.VMEM((NX, 64, 512), BF16),
            pltpu.VMEM((NX, 64, 512), BF16),
            *(
                pltpu.SemaphoreType.DMA(shape)
                for shape in (
                    (len(SENT),), (len(TOGETHER),), (4,), (14,), (14,), (3,), (3, 2), (4,)
                )
            ),
        ],
        compiler_params=pltpu.CompilerParams(
            collective_id=0, has_side_effects=True, vmem_limit_bytes=60 << 20
        ),
        name="layer",
    )(*operands)


def on_device(
    tokens, norm_gain, drive_weight, query_weight, key_weight, value_weight, key_offset, log_step,
    lambda_real, lambda_imag, input_map, output_map, skip_gain, forget, initial_state,
    scan_out_weight, attend_out_weight,
):
    return layer(
        tokens[0],
        norm_gain[None],
        drive_weight,
        query_weight,
        key_weight,
        value_weight,
        key_offset[:, 0, :],
        log_step[None],
        lambda_real,
        lambda_imag,
        input_map.transpose(0, 1, 3, 2),
        output_map,
        skip_gain.reshape(NY, 128),
        forget.reshape(NY, 8, 128),
        initial_state[:, 0],
        attend_out_weight,
        scan_out_weight,
    )[None]


def solution(mesh):
    split = Mesh(
        mesh.devices.reshape(NZ, NY, mesh.shape["fs"], mesh.shape["tp"]),
        ("sp_0", "sp_1", "fs", "tp"),
    )
    in_specs = (
        P("fs", SP_TP, None),
        P(),
        P("fs", "tp"),
        P("fs", "tp"),
        P("fs", "tp"),
        P("fs", "tp"),
        P("tp", "fs", SP),
        P("tp"),
        P("tp", None),
        P("tp", None),
        P(None, "tp", None, None),
        P(None, "tp", None, None),
        P("tp"),
        P("tp", "fs", SP),
        P(None, "fs", "tp", None),
        P("tp", "fs"),
        P("tp", "fs"),
    )
    return jax.shard_map(
        on_device, mesh=split, in_specs=in_specs, out_specs=P("fs", SP_TP, None), check_vma=False
    )
```

```python
import math

import jax
import jax.numpy as jnp
from jax import lax
from jax.experimental import pallas as pl
from jax.experimental.pallas import tpu as pltpu
from jax.sharding import Mesh
from jax.sharding import PartitionSpec as P

SP_TP = ("sp_0", "sp_1", "tp")
SP = ("sp_0", "sp_1")
EPSILON = 1e-06
LOG2E = 1.4426950408889634
NZ, NY, NX, NT = 8, 4, 4, 2
BF16, F32 = jnp.bfloat16, jnp.float32
TOGETHER = (
    "half", "keyed", "query", "packed", "offset", "state", "scan", "pre", "part", "hop", "attend",
    "last", "share", "far_rows", "values",
)
SENT = TOGETHER + ("rows", "right", "left", "slice", "relay", "drive")
VMEM = pl.BlockSpec(memory_space=pltpu.VMEM)
MESH_ID = pl.DeviceIdType.MESH


def remote(src, dst, send_sem, recv_sem, where):
    return pltpu.make_async_remote_copy(
        src_ref=src, dst_ref=dst, send_sem=send_sem, recv_sem=recv_sem,
        device_id=where, device_id_type=MESH_ID,
    )


def greet(peers):
    barrier = pltpu.get_barrier_semaphore()
    for peer in peers:
        pl.semaphore_signal(barrier, inc=1, device_id=peer, device_id_type=MESH_ID)


def await_greetings(count):
    pl.semaphore_wait(pltpu.get_barrier_semaphore(), count)


def plane_peers(x, y, t):
    peers = [
        {"fs": (x + dx) % NX, "tp": (t + dt) % NT}
        for dx in range(NX) for dt in range(NT) if (dx, dt) != (0, 0)
    ]
    peers += [
        {"fs": (x + dx) % NX, "sp_1": (y + dy) % NY} for dx in range(NX) for dy in range(1, NY)
    ]
    return peers


def high_low(value):
    high = value.astype(BF16)
    return high, (value - high.astype(F32)).astype(BF16)


def attend_chunk(query, pairs, offset, ladder, visible=None):
    keys, values = pairs[:, :128], pairs[:, 128:]
    score = lax.dot_general(query, keys, (((1,), (1,)), ((), ())), preferred_element_type=F32)
    score = score + offset
    soft = jnp.maximum(score, LOG2E * jnp.log(1.0 + jnp.exp2(jnp.minimum(score, 126.0))))
    if visible is not None:
        soft = jnp.where(visible, soft, 0.0)
    soft = soft.astype(BF16)
    last = jnp.dot(soft[:, 256:], ladder[:, :256], preferred_element_type=F32)
    first = jnp.dot(soft[:, :256], ladder[:, :256], preferred_element_type=F32) + jnp.dot(
        soft[:, 256:], ladder[:, 256:], preferred_element_type=F32
    )
    weight = jnp.exp2(score + jnp.concatenate([first, last], axis=1))
    if visible is not None:
        weight = jnp.where(visible, weight, 0.0)
    return jnp.dot(weight.astype(BF16), values, preferred_element_type=F32), first[:, :128]


def turned(gain, state):
    return gain[0] * state + gain[1] * pltpu.roll(state, 64, 1)


def powers_times(left, right):
    return (
        left[0] * right[0] - left[1] * right[1],
        left[1] * right[0] + left[0] * right[1],
    )


def layer_kernel(
    *refs,
):
    operands, out, held_here, rest = refs[:17], refs[17], refs[18:35], refs[35:]
    run_layer(operands, out, held_here, *rest)


def run_layer(
    operands, out, held_here, s_operand,
    normed, rows_in, keyed_w, query_w, drive_w, packed, packed_in, driven_in, queries,
    own_in, right_in, left_in, far_in, offset_own, offset_in, state_own, state_in, acc, tot,
    ladder, into_map, out_map, fwd_p, fwd_q, inv_p, inv_q, held, ends, decay,
    attend_own, scan_own, attend_in, scan_in, part_out, part_in, product_own, half_out, half_in,
    scan_product, pre_out, pre_in,
    s_all, r_all, r_rows, r_right, r_left, r_slice, r_relay, r_drive,
):
    (
        tok, gain_ref, w_drive, w_query, w_key, w_value, key_offset, log_step_ref, lambda_real,
        lambda_imag, input_map, output_map, skip_ref, forget_ref, initial_ref, w_attend, w_scan,
    ) = held_here
    z, y, x, t = (lax.axis_index(a) for a in ("sp_0", "sp_1", "fs", "tp"))
    fetches = [
        pltpu.make_async_copy(src, dst.at[x] if k == 15 else dst, s_operand.at[k])
        for k, (src, dst) in enumerate(zip(operands, held_here))
    ]
    for fetch in fetches:
        fetch.start()
    greet(plane_peers(x, y, t) + [{"sp_0": (z + dz) % NZ} for dz in range(1, NZ)])
    row = lax.broadcasted_iota(jnp.int32, (128, 128), 0)
    lane = lax.broadcasted_iota(jnp.int32, (128, 128), 1)
    up, down = {"sp_0": (z + 1) % NZ}, {"sp_0": (z + NZ - 1) % NZ}
    s_of = {name: s_all.at[k] for k, name in enumerate(SENT)}
    r_of = {name: r_all.at[k] for k, name in enumerate(TOGETHER)}

    def send(copy):
        copy.start()
        return copy

    def await_all(name, data):
        remote(data, data, s_of[name], r_of[name], sibling).wait_recv()

    for k in (0, 1, 6, 13):
        fetches[k].wait()
    packed[:, :8, :] = forget_ref[...]
    packed[:, 8:, :] = jnp.zeros((NY, 8, 128), F32)
    offsets = key_offset[...].astype(F32) * LOG2E
    for k in range(NY):
        packed[k, 8:9, :] = offsets[k : k + 1]
    values = tok[...].astype(F32)
    scale = lax.rsqrt(jnp.mean(values * values, axis=1, keepdims=True) + EPSILON)
    normed[...] = (values * scale * gain_ref[...]).astype(BF16)
    for k in (2, 3, 4, 5, 15):
        fetches[k].wait()
    await_greetings(26)

    order = (0, 1, 3, 2)
    mine = pl.ds(pl.multiple_of(t * 64, 64), 64)
    sibling = {"tp": 1 - t}

    def quarter(half):
        return pl.ds(pl.multiple_of(t * 64 + half * 32, 32), 32)

    def row_copy(j, half):
        return remote(
            normed.at[pl.ds(half * 32, 32)], rows_in.at[j, quarter(half)], s_of["rows"],
            r_rows.at[2 * j - 2 + half], {"sp_1": (y + order[j]) % NY},
        )

    def far_row_copy(j):
        part = quarter(j - 1)
        return remote(
            rows_in.at[j, part], rows_in.at[3, part], s_of["far_rows"], r_of["far_rows"],
            {"sp_1": (y + order[j]) % NY},
        )

    def half_copy(j):
        return remote(
            rows_in.at[j, mine] if j else normed, rows_in.at[j, mine], s_of["half"], r_of["half"],
            sibling,
        )

    column = pl.ds(pl.multiple_of(y * 128, 128), 128)
    depth = pl.ds(pl.multiple_of(x * 512, 512), 512)
    sources = (w_key, w_value, w_query)
    targets = (keyed_w.at[depth, :128], keyed_w.at[depth, 128:], query_w.at[depth])

    def weight_copy(kind, dx):
        group = "query" if kind == 2 else "keyed"
        return remote(
            sources[kind].at[:, column], targets[kind], s_of[group], r_of[group],
            {"fs": (x + dx) % NX},
        )

    def eighth(k):
        return drive_w.at[pl.ds(pl.multiple_of(k * 512 + z * 64, 64), 64)]

    def drive_copy(dx):
        return remote(
            w_drive.at[pl.ds(pl.multiple_of(z * 64, 64), 64), column], eighth(x), s_of["drive"],
            r_drive.at[dx - 1], {"fs": (x + dx) % NX},
        )

    def value_eighth(k):
        return keyed_w.at[pl.ds(pl.multiple_of(k * 512 + z * 64, 64), 64), 128:]

    def value_copy():
        return remote(
            w_value.at[pl.ds(pl.multiple_of(z * 64, 64), 64), column], value_eighth(x),
            s_of["drive"], r_drive.at[3], {"fs": (x + 2) % NX},
        )

    def value_share_copy(dz):
        part = value_eighth((x + 2) % NX)
        return remote(part, part, s_of["values"], r_of["values"], {"sp_0": (z + dz) % NZ})

    def share_copy(dx, dz):
        part = eighth((x + NX - dx) % NX)
        return remote(
            part, part, s_of["share"], r_of["share"], {"sp_0": (z + dz) % NZ}
        )

    def slice_copy(dx):
        return remote(
            w_attend.at[x, column], w_attend.at[x, column], s_of["slice"], r_slice.at[dx - 1],
            {"fs": (x + dx) % NX},
        )

    def relay_copy(dx, dy):
        part = w_attend.at[(x + NX - dx) % NX, column]
        return remote(
            part, part, s_of["relay"], r_relay.at[dx - 1, dy // 2], {"sp_1": (y + dy) % NY}
        )

    def hop_copy(dx, dy):
        start = (y + NY - dy) % NY * 128 + dy // 2 * 64
        part = w_attend.at[
            (x + NX - dx) % NX, pl.ds(pl.multiple_of(start, 64), 64)
        ]
        return remote(part, part, s_of["hop"], r_of["hop"], {"sp_1": (y + dy) % NY})

    for dy in range(1, NY):
        send(
            remote(
                packed.at[(y + dy) % NY], packed_in.at[y], s_of["packed"], r_of["packed"],
                {"sp_1": (y + dy) % NY},
            )
        )
    send(half_copy(0))
    for half in (0, 1):
        send(row_copy(1, half))
        send(row_copy(2, 1 - half))
    send(value_copy())
    for dx in (2, 1, 3):
        send(drive_copy(dx))
    for dx in (2, 1, 3):
        send(weight_copy(0, dx))
    for dx in (1, 3):
        send(weight_copy(1, dx))
    for dx in (1, 3, 2):
        send(slice_copy(dx))
    for dx in (2, 1, 3):
        send(weight_copy(2, dx))
    packed_in[y] = packed[y]
    rows_in[0, mine] = normed[...]
    keyed_w[depth, :128] = w_key[:, column]
    keyed_w[depth, 128:] = w_value[:, column]
    query_w[depth] = w_query[:, column]
    drive_w[depth] = w_drive[:, column]

    for k in (7, 8, 9, 10, 11, 12, 14, 16):
        fetches[k].wait()
    sign = jnp.where(lane[:8] < 64, -1.0, 1.0)
    groups = pl.ds(pl.multiple_of(y * 8, 8), 8)

    def side_by_side(left, right):
        return jnp.concatenate([left, right], axis=1)

    lam_real = side_by_side(lambda_real[groups, :], lambda_real[groups, :])
    lam_imag = side_by_side(lambda_imag[groups, :], lambda_imag[groups, :])
    initial = side_by_side(initial_ref[0, groups, :], initial_ref[1, groups, :])
    spot = lax.broadcasted_iota(jnp.int32, (8, 32), 1) - lax.broadcasted_iota(
        jnp.int32, (8, 32), 0
    )
    step = jnp.exp(
        jnp.sum(jnp.where(spot == y * 8, log_step_ref[...], 0.0), axis=1, keepdims=True)
    )
    log_gain, rotate = lam_real * step, lam_imag * step
    cosine, sine, magnitude = jnp.cos(rotate), jnp.sin(rotate), jnp.exp(log_gain)
    bar_real, bar_imag = magnitude * cosine, magnitude * sine
    divisor = lam_real * lam_real + lam_imag * lam_imag
    shifted = bar_real - 1.0
    factor_real = (shifted * lam_real + bar_imag * lam_imag) / divisor
    factor_imag = (bar_imag * lam_real - shifted * lam_imag) / divisor * sign
    shrink = jnp.exp(-log_gain)
    gain = (bar_real, sign * bar_imag)
    inverse = (shrink * cosine, -sign * shrink * sine)
    gains, inverses = [gain], [inverse]
    for _ in range(9):
        gains.append(powers_times(gains[-1], gains[-1]))
    for _ in range(6):
        inverses.append(powers_times(inverses[-1], inverses[-1]))
    gain_block, gain_all = gains[7], gains[9]
    gain_last = powers_times(gain_block, inverse)
    into_map[...] = jnp.zeros_like(into_map)
    out_map[...] = jnp.zeros_like(out_map)
    for g in range(8):
        cols, swapped = pl.ds(g * 128, 128), pl.ds(1024 + g * 128, 128)
        raw = side_by_side(input_map[0, y * 8 + g], input_map[1, y * 8 + g])
        entry = factor_real[g : g + 1] * raw + factor_imag[g : g + 1] * pltpu.roll(raw, 64, 1)
        turned_entry = pltpu.roll(entry, 64, 1)
        for at in (g * 16, 128 + g * 16):
            into_map[at : at + 16, cols] = entry.astype(BF16)
            into_map[at : at + 16, swapped] = turned_entry.astype(BF16)
        raw = side_by_side(output_map[0, y * 8 + g], output_map[1, y * 8 + g])
        out_map[g * 16 : g * 16 + 16, cols] = (raw * -sign[:1]).astype(BF16)
        out_map[g * 16 : g * 16 + 16, swapped] = (pltpu.roll(raw, 64, 1) * -sign[:1]).astype(BF16)
        for table_p, table_q, steps in ((fwd_p, fwd_q, gains), (inv_p, inv_q, inverses)):
            real, imag = jnp.ones((8, 128), F32), jnp.zeros((8, 128), F32)
            for bit in range(3):
                by = tuple(part[g : g + 1] for part in steps[bit])
                new = powers_times((real, imag), by)
                chosen = (row[:8] & (1 << bit)) != 0
                real, imag = jnp.where(chosen, new[0], real), jnp.where(chosen, new[1], imag)
            table_p[:8, cols] = real
            table_q[:8, cols] = imag
            for bit in range(3, 7):
                n = 1 << bit
                by = tuple(part[g : g + 1] for part in steps[bit])
                new = powers_times((table_p[:n, cols], table_q[:n, cols]), by)
                table_p[n : 2 * n, cols] = new[0]
                table_q[n : 2 * n, cols] = new[1]
    ladder_row = lax.broadcasted_iota(jnp.int32, (256, 512), 0)
    ladder_lane = lax.broadcasted_iota(jnp.int32, (256, 512), 1)
    ladder[...] = jnp.where((ladder_lane >= 256) | (ladder_row >= ladder_lane), -1.0, 0.0).astype(
        BF16
    )

    def block_of(j):
        dy = j + j // 2 * (5 - 2 * j)
        return (y + NY - dy) % NY

    def right_copy(i, j):
        b = block_of(j)
        return remote(
            own_in.at[b] if i == 1 else right_in.at[i - 2, b],
            far_in.at[b] if i == 4 else right_in.at[i - 1, b],
            s_of["right"], r_right.at[4 * i - 4 + j], up,
        )

    def left_copy(i, j):
        b = block_of(j)
        return remote(
            own_in.at[b] if i == 1 else left_in.at[i - 2, b],
            far_in.at[b] if i == 4 else left_in.at[i - 1, b],
            s_of["left"], r_left.at[4 * i - 4 + j - (2 if i == 4 else 0)], down,
        )

    await_all("packed", packed_in.at[:3])
    for b in range(NY):
        offset_own[b : b + 1, :] = packed_in[b, 8:9, :]
        offset_in[0, b : b + 1, :] = packed_in[b, 8:9, :]
    offset_own[4:8, :] = jnp.zeros((4, 128), F32)
    for dz in range(1, NZ):
        send(
            remote(
                offset_own, offset_in.at[dz], s_of["offset"], r_of["offset"],
                {"sp_0": (z + dz) % NZ},
            )
        )
    value_copy().wait_recv()
    for dz in (4, 3, 5, 2, 6, 1, 7):
        send(value_share_copy(dz))
    for dx in (2, 1, 3):
        drive_copy(dx).wait_recv()
        for dz in (4, 3, 5, 2, 6, 1, 7):
            send(share_copy(dx, dz))
    until = jnp.where(lane <= row, 1.0, 0.0)
    until_half = until.astype(BF16)
    falls = []
    for b in range(NY):
        forget = packed_in[b, :8, :]
        spread = jnp.concatenate(
            [jnp.broadcast_to(forget[g : g + 1], (16, 128)) for g in range(8)], axis=0
        )
        decay[b] = lax.dot_general(
            until, spread, (((1,), (1,)), ((), ())), preferred_element_type=F32,
            precision=lax.Precision.HIGHEST,
        )
        falls.append(jnp.sum(forget, axis=1, keepdims=True))
    for half in (0, 1):
        row_copy(1, half).wait_recv()
        row_copy(2, 1 - half).wait_recv()
        for j in (1, 2):
            send(half_copy(j) if half else far_row_copy(j))
    await_all("far_rows", rows_in.at[3, :64])
    send(half_copy(3))
    await_all("keyed", keyed_w.at[:1280])
    await_all("values", drive_w.at[:448])
    await_all("half", rows_in.at[:2])
    product = jnp.dot(
        rows_in[...].reshape(512, 2048), keyed_w[...], preferred_element_type=F32
    ).astype(BF16)
    for j in range(NY):
        own_in[block_of(j)] = product[j * 128 : (j + 1) * 128]
        right_copy(1, j).start()
        left_copy(1, j).start()
    def arrive(i, blocks=range(NY)):
        for j in blocks:
            if i < 4 or j < 2:
                right_copy(i, j).wait_recv()
                if i < 3 or i == 3 and j < 2:
                    right_copy(i + 1, j).start()
            if i < 4 or j >= 2:
                left_copy(i, j).wait_recv()
                if i < 3 or i == 3 and j >= 2:
                    left_copy(i + 1, j).start()

    def offset_row(dz):
        return jnp.concatenate([offset_in[dz, b : b + 1, :] for b in range(NY)], axis=1)

    def attend_far(dz, pairs):
        @pl.when(z >= dz)
        def _():
            acc[dz], tot[dz] = attend_chunk(
                queries[...].reshape(512, 128), pairs[...].reshape(512, 256), offset_row(dz),
                ladder[...],
            )

    def attend_step(i):
        attend_far(i, right_in.at[i - 1])
        attend_far(8 - i, left_in.at[i - 1])

    def pass_slice(dx):
        slice_copy(dx).wait_recv()
        for dy in (1, 3):
            send(relay_copy(dx, dy))

    def pass_on(dx):
        for dy in (1, 3):
            relay_copy(dx, dy).wait_recv()
            send(hop_copy(dx, dy))

    pass_slice(1)
    await_all("share", drive_w.at[:1344])
    product = jnp.dot(
        rows_in[...].reshape(512, 2048), drive_w[...], preferred_element_type=F32
    ).astype(BF16)
    for j in range(NY):
        driven_in[block_of(j)] = product[j * 128 : (j + 1) * 128]
    local = jnp.zeros((8, 128), F32)
    fall_all = jnp.zeros((8, 1), F32)
    for b in range(NY):
        driven = driven_in[b].astype(F32) * jnp.exp(-decay[b])
        entered = jnp.dot(
            jnp.concatenate(high_low(driven), axis=1), into_map[...], preferred_element_type=F32
        )
        unturned = entered[:, :1024] * inv_p[...] + entered[:, 1024:] * inv_q[...]
        high, low = high_low(unturned)
        held[b] = jnp.dot(until_half, high, preferred_element_type=F32) + jnp.dot(
            until_half, low, preferred_element_type=F32
        )
        for g in range(8):
            ends[b, g : g + 1, :] = held[b, 127:128, g * 128 : (g + 1) * 128]
        fall_all = fall_all + falls[b]
        falls[b] = jnp.exp(falls[b])
        ends[b] = falls[b] * turned(gain_last, ends[b])
        local = falls[b] * turned(gain_block, local) + ends[b]
        if b == 1:
            pass_slice(3)
            pass_slice(2)
        if b < 3:
            arrive(1, (b,))
    state_own[:8, :] = local
    state_own[8:, :] = jnp.broadcast_to(fall_all, (8, 128))
    for dz in range(1, NZ):
        send(
            remote(
                state_own, state_in.at[dz], s_of["state"], r_of["state"],
                {"sp_0": (z + dz) % NZ},
            )
        )

    arrive(1, (3,))
    arrive(2, (0,))
    pass_on(1)
    arrive(2, (1,))
    await_all("query", query_w.at[:1536])
    product = jnp.dot(
        rows_in[...].reshape(512, 2048), query_w[...], preferred_element_type=F32
    )
    product = (product * (LOG2E * 128**-0.5)).astype(BF16)
    for j in range(NY):
        queries[block_of(j)] = product[j * 128 : (j + 1) * 128]

    arrive(2, (2,))
    acc[0], tot[0] = attend_chunk(
        queries[...].reshape(512, 128), own_in[...].reshape(512, 256), offset_row(0), ladder[...],
        lax.broadcasted_iota(jnp.int32, (512, 512), 1)
        < lax.broadcasted_iota(jnp.int32, (512, 512), 0),
    )
    await_all("offset", offset_in.at[:7])
    pass_on(3)
    pass_on(2)
    arrive(2, (3,))

    await_all("state", state_in.at[:7])
    carry = initial
    for source in range(NZ - 1):
        arrived = state_in[jnp.maximum(z - source, 1)]
        moved = jnp.exp(arrived[8:]) * turned(gain_all, carry) + arrived[:8]
        carry = jnp.where(source < z, moved, carry)
    for b in range(NY):
        entering = turned(gain, carry)
        whole = jnp.concatenate(
            [held[b, :, g * 128 : (g + 1) * 128] + entering[g : g + 1] for g in range(8)], axis=1
        )
        turned_states = jnp.concatenate(
            [(whole * fwd_p[...]).astype(BF16), (whole * fwd_q[...]).astype(BF16)], axis=1
        )
        read = lax.dot_general(
            turned_states, out_map[...], (((1,), (1,)), ((), ())), preferred_element_type=F32
        )
        read = read * jnp.exp(decay[b]) + skip_ref[pl.ds(y, 1), :] * driven_in[b].astype(F32)
        inner = math.sqrt(2.0 / math.pi) * (read + 0.044715 * (read * read * read))
        scan_own[b] = (0.5 * read * (1.0 + jnp.tanh(inner))).astype(BF16)
        carry = falls[b] * turned(gain_block, carry) + ends[b]

    for dx in (2, 1, 3, 0):
        for dy in (2, 1, 3, 0):
            if (dx, dy) != (0, 0):
                send(
                    remote(
                        scan_own.at[(y + dy) % NY], scan_in.at[dx, dy], s_of["scan"],
                        r_of["scan"], {"fs": (x + dx) % NX, "sp_1": (y + dy) % NY},
                    )
                )
    scan_in[0, 0] = scan_own[y]
    arrive(3, (0,))
    attend_far(1, right_in.at[0])
    arrive(3, (1,))
    attend_far(7, left_in.at[0])
    arrive(3, (2,))
    attend_far(2, right_in.at[1])
    arrive(3, (3,))
    attend_far(6, left_in.at[1])
    attend_step(3)

    def join(near, far):
        @pl.when(z >= far)
        def _():
            fallen = tot[near, :, :1]
            acc[near] += jnp.exp2(fallen) * acc[far]
            tot[near, :, :1] = fallen + tot[far, :, :1]

    for dz in (1, 2, 3):
        join(0, dz)
    for dz in (6, 7):
        join(5, dz)
    other = pl.ds(pl.multiple_of((1 - t) * 64, 64), 64)
    await_all("scan", drive_w.at[:1920])
    for dx in order:
        total = None
        for dy in range(NY):
            head = (y + NY - dy) % NY
            head_rows = pl.ds(pl.multiple_of(head * 128, 128), 128)
            product = jnp.dot(scan_in[dx, dy], w_scan[head_rows, :], preferred_element_type=F32)
            total = product if total is None else total + product
        scan_product[dx] = total
        pre_out[dx] = scan_product[dx, other, :].astype(BF16)
        send(remote(pre_out.at[dx], pre_in.at[dx], s_of["pre"], r_of["pre"], sibling))
    arrive(4)
    attend_far(4, far_in)
    for dz in (4, 5):
        join(0, dz)
    attend_own[...] = acc[0].astype(BF16).reshape(NY, 128, 128)
    for dy in (2, 1, 3):
        send(
            remote(
                attend_own.at[(y + dy) % NY], attend_in.at[:, column], s_of["attend"],
                r_of["attend"], {"sp_1": (y + dy) % NY},
            )
        )
    attend_in[:, column] = attend_own[y]
    await_all("pre", pre_in)
    for dx in (2, 1, 3):
        part_out[dx] = (scan_product[dx, mine, :] + pre_in[dx].astype(F32)).astype(BF16)
        send(
            remote(
                part_out.at[dx], part_in.at[dx], s_of["part"], r_of["part"],
                {"fs": (x + NX - dx) % NX},
            )
        )
    await_all("hop", w_attend.at[0, :384])
    await_all("attend", drive_w.at[:384])
    for k in range(NX):
        product_own[k] = jnp.dot(attend_in[...], w_attend[k], preferred_element_type=F32)
        half_out[k] = product_own[k, other, :].astype(BF16)
        send(remote(half_out.at[k], half_in.at[k], s_of["last"], r_of["last"], sibling))
    await_all("last", half_in)
    await_all("part", w_attend.at[0, :192])
    for dx in order:
        k = (x + dx) % NX
        columns = pl.ds(pl.multiple_of(k * 512, 512), 512)
        scan_part = scan_product[0, mine, :] + pre_in[0].astype(F32)
        if dx:
            scan_part = part_in[dx].astype(F32)
        out[:, columns] = (product_own[k, mine, :] + half_in[k].astype(F32) + scan_part).astype(BF16)
    for name, data in {
        "rows": rows_in.at[:2, :64],
        "half": rows_in.at[:2],
        "keyed": keyed_w.at[:1280],
        "values": drive_w.at[:448],
        "far_rows": rows_in.at[3, :64],
        "query": query_w.at[:1536],
        "packed": packed_in.at[:3],
        "right": w_attend.at[:2, :448],
        "left": w_attend.at[:2, :448],
        "offset": offset_in.at[:7],
        "state": state_in.at[:7],
        "scan": drive_w.at[:1920],
        "pre": pre_in,
        "part": w_attend.at[0, :192],
        "slice": w_attend.at[0, :384],
        "relay": w_attend.at[:3, :256],
        "hop": w_attend.at[0, :384],
        "attend": drive_w.at[:384],
        "last": half_in,
        "drive": drive_w.at[:256],
        "share": drive_w.at[:1344],
    }.items():
        remote(data, data, s_of[name], r_rows.at[0], sibling).wait_send()


def layer(*operands):
    return pl.pallas_call(
        layer_kernel,
        out_shape=pltpu.VMEM((64, 2048), BF16),
        in_specs=[pl.BlockSpec(memory_space=pl.ANY)] * 17,
        out_specs=VMEM,
        scratch_shapes=[
            *(
                pltpu.VMEM((NX, 512, 512) if k == 15 else operand.shape, operand.dtype)
                for k, operand in enumerate(operands)
            ),
            pltpu.SemaphoreType.DMA((17,)),
            pltpu.VMEM((64, 2048), BF16),
            pltpu.VMEM((NY, 128, 2048), BF16),
            pltpu.VMEM((2048, 256), BF16),
            pltpu.VMEM((2048, 128), BF16),
            pltpu.VMEM((2048, 128), BF16),
            pltpu.VMEM((NY, 16, 128), F32),
            pltpu.VMEM((NY, 16, 128), F32),
            pltpu.VMEM((NY, 128, 128), BF16),
            pltpu.VMEM((NY, 128, 128), BF16),
            pltpu.VMEM((NY, 128, 256), BF16),
            pltpu.VMEM((3, NY, 128, 256), BF16),
            pltpu.VMEM((3, NY, 128, 256), BF16),
            pltpu.VMEM((NY, 128, 256), BF16),
            pltpu.VMEM((8, 128), F32),
            pltpu.VMEM((NZ, 8, 128), F32),
            pltpu.VMEM((16, 128), F32),
            pltpu.VMEM((NZ, 16, 128), F32),
            pltpu.VMEM((NZ, 512, 128), F32),
            pltpu.VMEM((NZ, 512, 128), F32),
            pltpu.VMEM((256, 512), BF16),
            pltpu.VMEM((256, 2048), BF16),
            pltpu.VMEM((128, 2048), BF16),
            pltpu.VMEM((128, 1024), F32),
            pltpu.VMEM((128, 1024), F32),
            pltpu.VMEM((128, 1024), F32),
            pltpu.VMEM((128, 1024), F32),
            pltpu.VMEM((NY, 128, 1024), F32),
            pltpu.VMEM((NY, 8, 128), F32),
            pltpu.VMEM((NY, 128, 128), F32),
            pltpu.VMEM((NY, 128, 128), BF16),
            pltpu.VMEM((NY, 128, 128), BF16),
            pltpu.VMEM((128, 512), BF16),
            pltpu.VMEM((NX, NY, 128, 128), BF16),
            pltpu.VMEM((NX, 64, 512), BF16),
            pltpu.VMEM((NX, 64, 512), BF16),
            pltpu.VMEM((NX, 128, 512), F32),
            pltpu.VMEM((NX, 64, 512), BF16),
            pltpu.VMEM((NX, 64, 512), BF16),
            pltpu.VMEM((NX, 128, 512), F32),
            pltpu.VMEM((NX, 64, 512), BF16),
            pltpu.VMEM((NX, 64, 512), BF16),
            *(
                pltpu.SemaphoreType.DMA(shape)
                for shape in (
                    (len(SENT),), (len(TOGETHER),), (4,), (14,), (14,), (3,), (3, 2), (4,)
                )
            ),
        ],
        compiler_params=pltpu.CompilerParams(
            collective_id=0, has_side_effects=True, vmem_limit_bytes=60 << 20
        ),
        name="layer",
    )(*operands)


def on_device(
    tokens, norm_gain, drive_weight, query_weight, key_weight, value_weight, key_offset, log_step,
    lambda_real, lambda_imag, input_map, output_map, skip_gain, forget, initial_state,
    scan_out_weight, attend_out_weight,
):
    return layer(
        tokens[0],
        norm_gain[None],
        drive_weight,
        query_weight,
        key_weight,
        value_weight,
        key_offset[:, 0, :],
        log_step[None],
        lambda_real,
        lambda_imag,
        input_map.transpose(0, 1, 3, 2),
        output_map,
        skip_gain.reshape(NY, 128),
        forget.reshape(NY, 8, 128),
        initial_state[:, 0],
        attend_out_weight,
        scan_out_weight,
    )[None]


def solution(mesh):
    split = Mesh(
        mesh.devices.reshape(NZ, NY, mesh.shape["fs"], mesh.shape["tp"]),
        ("sp_0", "sp_1", "fs", "tp"),
    )
    in_specs = (
        P("fs", SP_TP, None),
        P(),
        P("fs", "tp"),
        P("fs", "tp"),
        P("fs", "tp"),
        P("fs", "tp"),
        P("tp", "fs", SP),
        P("tp"),
        P("tp", None),
        P("tp", None),
        P(None, "tp", None, None),
        P(None, "tp", None, None),
        P("tp"),
        P("tp", "fs", SP),
        P(None, "fs", "tp", None),
        P("tp", "fs"),
        P("tp", "fs"),
    )
    return jax.shard_map(
        on_device, mesh=split, in_specs=in_specs, out_specs=P("fs", SP_TP, None), check_vma=False
    )
```

```python
import math

import jax
import jax.numpy as jnp
from jax import lax
from jax.experimental import pallas as pl
from jax.experimental.pallas import tpu as pltpu
from jax.sharding import Mesh
from jax.sharding import PartitionSpec as P

SP_TP = ("sp_0", "sp_1", "tp")
SP = ("sp_0", "sp_1")
EPSILON = 1e-06
LOG2E = 1.4426950408889634
NZ, NY, NX, NT = 8, 4, 4, 2
BF16, F32 = jnp.bfloat16, jnp.float32
TOGETHER = (
    "half", "keyed", "query", "packed", "offset", "state", "scan", "pre", "part", "hop", "attend",
    "last", "share", "far_rows", "values",
)
SENT = TOGETHER + ("rows", "right", "left", "slice", "relay", "drive")
VMEM = pl.BlockSpec(memory_space=pltpu.VMEM)
MESH_ID = pl.DeviceIdType.MESH


def remote(src, dst, send_sem, recv_sem, where):
    return pltpu.make_async_remote_copy(
        src_ref=src, dst_ref=dst, send_sem=send_sem, recv_sem=recv_sem,
        device_id=where, device_id_type=MESH_ID,
    )


def greet(peers):
    barrier = pltpu.get_barrier_semaphore()
    for peer in peers:
        pl.semaphore_signal(barrier, inc=1, device_id=peer, device_id_type=MESH_ID)


def await_greetings(count):
    pl.semaphore_wait(pltpu.get_barrier_semaphore(), count)


def plane_peers(x, y, t):
    peers = [
        {"fs": (x + dx) % NX, "tp": (t + dt) % NT}
        for dx in range(NX) for dt in range(NT) if (dx, dt) != (0, 0)
    ]
    peers += [
        {"fs": (x + dx) % NX, "sp_1": (y + dy) % NY} for dx in range(NX) for dy in range(1, NY)
    ]
    return peers


def high_low(value):
    high = value.astype(BF16)
    return high, (value - high.astype(F32)).astype(BF16)


def attend_chunk(query, pairs, offset, ladder, visible=None):
    keys, values = pairs[:, :128], pairs[:, 128:]
    score = lax.dot_general(query, keys, (((1,), (1,)), ((), ())), preferred_element_type=F32)
    score = score + offset
    soft = jnp.maximum(score, LOG2E * jnp.log(1.0 + jnp.exp2(jnp.minimum(score, 126.0))))
    if visible is not None:
        soft = jnp.where(visible, soft, 0.0)
    soft = soft.astype(BF16)
    last = jnp.dot(soft[:, 256:], ladder[:, :256], preferred_element_type=F32)
    first = jnp.dot(soft[:, :256], ladder[:, :256], preferred_element_type=F32) + jnp.dot(
        soft[:, 256:], ladder[:, 256:], preferred_element_type=F32
    )
    weight = jnp.exp2(score + jnp.concatenate([first, last], axis=1))
    if visible is not None:
        weight = jnp.where(visible, weight, 0.0)
    return jnp.dot(weight.astype(BF16), values, preferred_element_type=F32), first[:, :128]


def turned(gain, state):
    return gain[0] * state + gain[1] * pltpu.roll(state, 64, 1)


def powers_times(left, right):
    return (
        left[0] * right[0] - left[1] * right[1],
        left[1] * right[0] + left[0] * right[1],
    )


def layer_kernel(
    *refs,
):
    operands, out, held_here, rest = refs[:17], refs[17], refs[18:35], refs[35:]
    run_layer(operands, out, held_here, *rest)


def run_layer(
    operands, out, held_here, s_operand,
    normed, rows_in, keyed_w, query_w, drive_w, packed, packed_in, driven_in, queries,
    own_in, right_in, left_in, far_in, offset_own, offset_in, state_own, state_in, acc, tot,
    ladder, into_map, out_map, fwd_p, fwd_q, inv_p, inv_q, held, ends, decay,
    attend_own, scan_own, attend_in, scan_in, part_out, part_in, product_own, half_out, half_in,
    scan_product, pre_out, pre_in,
    s_all, r_all, r_rows, r_right, r_left, r_slice, r_relay, r_drive,
):
    (
        tok, gain_ref, w_drive, w_query, w_key, w_value, key_offset, log_step_ref, lambda_real,
        lambda_imag, input_map, output_map, skip_ref, forget_ref, initial_ref, w_attend, w_scan,
    ) = held_here
    z, y, x, t = (lax.axis_index(a) for a in ("sp_0", "sp_1", "fs", "tp"))
    fetches = [
        pltpu.make_async_copy(src, dst.at[x] if k == 15 else dst, s_operand.at[k])
        for k, (src, dst) in enumerate(zip(operands, held_here))
    ]
    for fetch in fetches:
        fetch.start()
    greet(plane_peers(x, y, t) + [{"sp_0": (z + dz) % NZ} for dz in range(1, NZ)])
    row = lax.broadcasted_iota(jnp.int32, (128, 128), 0)
    lane = lax.broadcasted_iota(jnp.int32, (128, 128), 1)
    up, down = {"sp_0": (z + 1) % NZ}, {"sp_0": (z + NZ - 1) % NZ}
    s_of = {name: s_all.at[k] for k, name in enumerate(SENT)}
    r_of = {name: r_all.at[k] for k, name in enumerate(TOGETHER)}

    def send(copy):
        copy.start()
        return copy

    def await_all(name, data):
        remote(data, data, s_of[name], r_of[name], sibling).wait_recv()

    for k in (0, 1, 6, 13):
        fetches[k].wait()
    packed[:, :8, :] = forget_ref[...]
    packed[:, 8:, :] = jnp.zeros((NY, 8, 128), F32)
    offsets = key_offset[...].astype(F32) * LOG2E
    for k in range(NY):
        packed[k, 8:9, :] = offsets[k : k + 1]
    values = tok[...].astype(F32)
    scale = lax.rsqrt(jnp.mean(values * values, axis=1, keepdims=True) + EPSILON)
    normed[...] = (values * scale * gain_ref[...]).astype(BF16)
    for k in (2, 3, 4, 5, 15):
        fetches[k].wait()
    await_greetings(26)

    order = (0, 1, 3, 2)
    mine = pl.ds(pl.multiple_of(t * 64, 64), 64)
    sibling = {"tp": 1 - t}

    def quarter(half):
        return pl.ds(pl.multiple_of(t * 64 + half * 32, 32), 32)

    def row_copy(j, half):
        return remote(
            normed.at[pl.ds(half * 32, 32)], rows_in.at[j, quarter(half)], s_of["rows"],
            r_rows.at[2 * j - 2 + half], {"sp_1": (y + order[j]) % NY},
        )

    def far_row_copy(j):
        part = quarter(j - 1)
        return remote(
            rows_in.at[j, part], rows_in.at[3, part], s_of["far_rows"], r_of["far_rows"],
            {"sp_1": (y + order[j]) % NY},
        )

    def half_copy(j):
        return remote(
            rows_in.at[j, mine] if j else normed, rows_in.at[j, mine], s_of["half"], r_of["half"],
            sibling,
        )

    column = pl.ds(pl.multiple_of(y * 128, 128), 128)
    depth = pl.ds(pl.multiple_of(x * 512, 512), 512)
    sources = (w_key, w_value, w_query)
    targets = (keyed_w.at[depth, :128], keyed_w.at[depth, 128:], query_w.at[depth])

    def weight_copy(kind, dx):
        group = "query" if kind == 2 else "keyed"
        return remote(
            sources[kind].at[:, column], targets[kind], s_of[group], r_of[group],
            {"fs": (x + dx) % NX},
        )

    def eighth(k):
        return drive_w.at[pl.ds(pl.multiple_of(k * 512 + z * 64, 64), 64)]

    def drive_copy(dx):
        return remote(
            w_drive.at[pl.ds(pl.multiple_of(z * 64, 64), 64), column], eighth(x), s_of["drive"],
            r_drive.at[dx - 1], {"fs": (x + dx) % NX},
        )

    def value_eighth(k):
        return keyed_w.at[pl.ds(pl.multiple_of(k * 512 + z * 64, 64), 64), 128:]

    def value_copy():
        return remote(
            w_value.at[pl.ds(pl.multiple_of(z * 64, 64), 64), column], value_eighth(x),
            s_of["drive"], r_drive.at[3], {"fs": (x + 2) % NX},
        )

    def value_share_copy(dz):
        part = value_eighth((x + 2) % NX)
        return remote(part, part, s_of["values"], r_of["values"], {"sp_0": (z + dz) % NZ})

    def share_copy(dx, dz):
        part = eighth((x + NX - dx) % NX)
        return remote(
            part, part, s_of["share"], r_of["share"], {"sp_0": (z + dz) % NZ}
        )

    def slice_copy(dx):
        return remote(
            w_attend.at[x, column], w_attend.at[x, column], s_of["slice"], r_slice.at[dx - 1],
            {"fs": (x + dx) % NX},
        )

    def relay_copy(dx, dy):
        part = w_attend.at[(x + NX - dx) % NX, column]
        return remote(
            part, part, s_of["relay"], r_relay.at[dx - 1, dy // 2], {"sp_1": (y + dy) % NY}
        )

    def hop_copy(dx, dy):
        start = (y + NY - dy) % NY * 128 + dy // 2 * 64
        part = w_attend.at[
            (x + NX - dx) % NX, pl.ds(pl.multiple_of(start, 64), 64)
        ]
        return remote(part, part, s_of["hop"], r_of["hop"], {"sp_1": (y + dy) % NY})

    for dy in range(1, NY):
        send(
            remote(
                packed.at[(y + dy) % NY], packed_in.at[y], s_of["packed"], r_of["packed"],
                {"sp_1": (y + dy) % NY},
            )
        )
    send(half_copy(0))
    for half in (0, 1):
        send(row_copy(1, half))
        send(row_copy(2, 1 - half))
    send(value_copy())
    for dx in (2, 1, 3):
        send(drive_copy(dx))
    for dx in (2, 1, 3):
        send(weight_copy(0, dx))
    for dx in (1, 3):
        send(weight_copy(1, dx))
    for dx in (1, 3, 2):
        send(slice_copy(dx))
    for dx in (2, 1, 3):
        send(weight_copy(2, dx))
    packed_in[y] = packed[y]
    rows_in[0, mine] = normed[...]
    keyed_w[depth, :128] = w_key[:, column]
    keyed_w[depth, 128:] = w_value[:, column]
    query_w[depth] = w_query[:, column]
    drive_w[depth] = w_drive[:, column]

    for k in (7, 8, 9, 10, 11, 12, 14, 16):
        fetches[k].wait()
    sign = jnp.where(lane[:8] < 64, -1.0, 1.0)
    groups = pl.ds(pl.multiple_of(y * 8, 8), 8)

    def side_by_side(left, right):
        return jnp.concatenate([left, right], axis=1)

    lam_real = side_by_side(lambda_real[groups, :], lambda_real[groups, :])
    lam_imag = side_by_side(lambda_imag[groups, :], lambda_imag[groups, :])
    initial = side_by_side(initial_ref[0, groups, :], initial_ref[1, groups, :])
    spot = lax.broadcasted_iota(jnp.int32, (8, 32), 1) - lax.broadcasted_iota(
        jnp.int32, (8, 32), 0
    )
    step = jnp.exp(
        jnp.sum(jnp.where(spot == y * 8, log_step_ref[...], 0.0), axis=1, keepdims=True)
    )
    log_gain, rotate = lam_real * step, lam_imag * step
    cosine, sine, magnitude = jnp.cos(rotate), jnp.sin(rotate), jnp.exp(log_gain)
    bar_real, bar_imag = magnitude * cosine, magnitude * sine
    divisor = lam_real * lam_real + lam_imag * lam_imag
    shifted = bar_real - 1.0
    factor_real = (shifted * lam_real + bar_imag * lam_imag) / divisor
    factor_imag = (bar_imag * lam_real - shifted * lam_imag) / divisor * sign
    shrink = jnp.exp(-log_gain)
    gain = (bar_real, sign * bar_imag)
    inverse = (shrink * cosine, -sign * shrink * sine)
    gains, inverses = [gain], [inverse]
    for _ in range(9):
        gains.append(powers_times(gains[-1], gains[-1]))
    for _ in range(6):
        inverses.append(powers_times(inverses[-1], inverses[-1]))
    gain_block, gain_all = gains[7], gains[9]
    gain_last = powers_times(gain_block, inverse)
    into_map[...] = jnp.zeros_like(into_map)
    out_map[...] = jnp.zeros_like(out_map)
    for g in range(8):
        cols, swapped = pl.ds(g * 128, 128), pl.ds(1024 + g * 128, 128)
        raw = side_by_side(input_map[0, y * 8 + g], input_map[1, y * 8 + g])
        entry = factor_real[g : g + 1] * raw + factor_imag[g : g + 1] * pltpu.roll(raw, 64, 1)
        turned_entry = pltpu.roll(entry, 64, 1)
        for at in (g * 16, 128 + g * 16):
            into_map[at : at + 16, cols] = entry.astype(BF16)
            into_map[at : at + 16, swapped] = turned_entry.astype(BF16)
        raw = side_by_side(output_map[0, y * 8 + g], output_map[1, y * 8 + g])
        out_map[g * 16 : g * 16 + 16, cols] = (raw * -sign[:1]).astype(BF16)
        out_map[g * 16 : g * 16 + 16, swapped] = (pltpu.roll(raw, 64, 1) * -sign[:1]).astype(BF16)
        for table_p, table_q, steps in ((fwd_p, fwd_q, gains), (inv_p, inv_q, inverses)):
            real, imag = jnp.ones((8, 128), F32), jnp.zeros((8, 128), F32)
            for bit in range(3):
                by = tuple(part[g : g + 1] for part in steps[bit])
                new = powers_times((real, imag), by)
                chosen = (row[:8] & (1 << bit)) != 0
                real, imag = jnp.where(chosen, new[0], real), jnp.where(chosen, new[1], imag)
            table_p[:8, cols] = real
            table_q[:8, cols] = imag
            for bit in range(3, 7):
                n = 1 << bit
                by = tuple(part[g : g + 1] for part in steps[bit])
                new = powers_times((table_p[:n, cols], table_q[:n, cols]), by)
                table_p[n : 2 * n, cols] = new[0]
                table_q[n : 2 * n, cols] = new[1]
    ladder_row = lax.broadcasted_iota(jnp.int32, (256, 512), 0)
    ladder_lane = lax.broadcasted_iota(jnp.int32, (256, 512), 1)
    ladder[...] = jnp.where((ladder_lane >= 256) | (ladder_row >= ladder_lane), -1.0, 0.0).astype(
        BF16
    )

    def block_of(j):
        dy = j + j // 2 * (5 - 2 * j)
        return (y + NY - dy) % NY

    def right_copy(i, j):
        b = block_of(j)
        return remote(
            own_in.at[b] if i == 1 else right_in.at[i - 2, b],
            far_in.at[b] if i == 4 else right_in.at[i - 1, b],
            s_of["right"], r_right.at[4 * i - 4 + j], up,
        )

    def left_copy(i, j):
        b = block_of(j)
        return remote(
            own_in.at[b] if i == 1 else left_in.at[i - 2, b],
            far_in.at[b] if i == 4 else left_in.at[i - 1, b],
            s_of["left"], r_left.at[4 * i - 4 + j - (2 if i == 4 else 0)], down,
        )

    await_all("packed", packed_in.at[:3])
    for b in range(NY):
        offset_own[b : b + 1, :] = packed_in[b, 8:9, :]
        offset_in[0, b : b + 1, :] = packed_in[b, 8:9, :]
    offset_own[4:8, :] = jnp.zeros((4, 128), F32)
    for dz in range(1, NZ):
        send(
            remote(
                offset_own, offset_in.at[dz], s_of["offset"], r_of["offset"],
                {"sp_0": (z + dz) % NZ},
            )
        )
    value_copy().wait_recv()
    for dz in (4, 3, 5, 2, 6, 1, 7):
        send(value_share_copy(dz))
    for dx in (2, 1, 3):
        drive_copy(dx).wait_recv()
        for dz in (4, 3, 5, 2, 6, 1, 7):
            send(share_copy(dx, dz))
    until = jnp.where(lane <= row, 1.0, 0.0)
    until_half = until.astype(BF16)
    falls = []
    for b in range(NY):
        forget = packed_in[b, :8, :]
        spread = jnp.concatenate(
            [jnp.broadcast_to(forget[g : g + 1], (16, 128)) for g in range(8)], axis=0
        )
        decay[b] = lax.dot_general(
            until, spread, (((1,), (1,)), ((), ())), preferred_element_type=F32,
            precision=lax.Precision.HIGHEST,
        )
        falls.append(jnp.sum(forget, axis=1, keepdims=True))
    for half in (0, 1):
        row_copy(1, half).wait_recv()
        row_copy(2, 1 - half).wait_recv()
        for j in (1, 2):
            send(half_copy(j) if half else far_row_copy(j))
    await_all("far_rows", rows_in.at[3, :64])
    send(half_copy(3))
    await_all("keyed", keyed_w.at[:1280])
    await_all("values", drive_w.at[:448])
    await_all("half", rows_in.at[:2])
    product = jnp.dot(
        rows_in[...].reshape(512, 2048), keyed_w[...], preferred_element_type=F32
    ).astype(BF16)
    for j in range(NY):
        own_in[block_of(j)] = product[j * 128 : (j + 1) * 128]
        right_copy(1, j).start()
        left_copy(1, j).start()
    def arrive(i, blocks=range(NY)):
        for j in blocks:
            if i < 4 or j < 2:
                right_copy(i, j).wait_recv()
                if i < 3 or i == 3 and j < 2:
                    right_copy(i + 1, j).start()
            if i < 4 or j >= 2:
                left_copy(i, j).wait_recv()
                if i < 3 or i == 3 and j >= 2:
                    left_copy(i + 1, j).start()

    def offset_row(dz):
        return jnp.concatenate([offset_in[dz, b : b + 1, :] for b in range(NY)], axis=1)

    def attend_far(dz, pairs):
        @pl.when(z >= dz)
        def _():
            acc[dz], tot[dz] = attend_chunk(
                queries[...].reshape(512, 128), pairs[...].reshape(512, 256), offset_row(dz),
                ladder[...],
            )

    def join(near, far):
        @pl.when(z >= far)
        def _():
            fallen = tot[near, :, :1]
            acc[near] += jnp.exp2(fallen) * acc[far]
            tot[near, :, :1] = fallen + tot[far, :, :1]

    def attend_step(i):
        attend_far(i, right_in.at[i - 1])
        attend_far(8 - i, left_in.at[i - 1])

    def pass_slice(dx):
        slice_copy(dx).wait_recv()
        for dy in (1, 3):
            send(relay_copy(dx, dy))

    def pass_on(dx):
        for dy in (1, 3):
            relay_copy(dx, dy).wait_recv()
            send(hop_copy(dx, dy))

    pass_slice(1)
    await_all("share", drive_w.at[:1344])
    product = jnp.dot(
        rows_in[...].reshape(512, 2048), drive_w[...], preferred_element_type=F32
    ).astype(BF16)
    for j in range(NY):
        driven_in[block_of(j)] = product[j * 128 : (j + 1) * 128]
    local = jnp.zeros((8, 128), F32)
    fall_all = jnp.zeros((8, 1), F32)
    for b in range(NY):
        driven = driven_in[b].astype(F32) * jnp.exp(-decay[b])
        entered = jnp.dot(
            jnp.concatenate(high_low(driven), axis=1), into_map[...], preferred_element_type=F32
        )
        unturned = entered[:, :1024] * inv_p[...] + entered[:, 1024:] * inv_q[...]
        high, low = high_low(unturned)
        held[b] = jnp.dot(until_half, high, preferred_element_type=F32) + jnp.dot(
            until_half, low, preferred_element_type=F32
        )
        for g in range(8):
            ends[b, g : g + 1, :] = held[b, 127:128, g * 128 : (g + 1) * 128]
        fall_all = fall_all + falls[b]
        falls[b] = jnp.exp(falls[b])
        ends[b] = falls[b] * turned(gain_last, ends[b])
        local = falls[b] * turned(gain_block, local) + ends[b]
        if b == 1:
            pass_slice(3)
            pass_slice(2)
        if b < 3:
            arrive(1, (b,))
    state_own[:8, :] = local
    state_own[8:, :] = jnp.broadcast_to(fall_all, (8, 128))
    for dz in range(1, NZ):
        send(
            remote(
                state_own, state_in.at[dz], s_of["state"], r_of["state"],
                {"sp_0": (z + dz) % NZ},
            )
        )

    arrive(1, (3,))
    arrive(2, (0,))
    pass_on(1)
    arrive(2, (1,))
    await_all("query", query_w.at[:1536])
    product = jnp.dot(
        rows_in[...].reshape(512, 2048), query_w[...], preferred_element_type=F32
    )
    product = (product * (LOG2E * 128**-0.5)).astype(BF16)
    for j in range(NY):
        queries[block_of(j)] = product[j * 128 : (j + 1) * 128]

    arrive(2, (2,))
    acc[0], tot[0] = attend_chunk(
        queries[...].reshape(512, 128), own_in[...].reshape(512, 256), offset_row(0), ladder[...],
        lax.broadcasted_iota(jnp.int32, (512, 512), 1)
        < lax.broadcasted_iota(jnp.int32, (512, 512), 0),
    )
    await_all("offset", offset_in.at[:7])
    pass_on(3)
    pass_on(2)
    arrive(2, (3,))

    await_all("state", state_in.at[:7])
    carry = initial
    for source in range(NZ - 1):
        arrived = state_in[jnp.maximum(z - source, 1)]
        moved = jnp.exp(arrived[8:]) * turned(gain_all, carry) + arrived[:8]
        carry = jnp.where(source < z, moved, carry)
    for b in range(NY):
        entering = turned(gain, carry)
        whole = jnp.concatenate(
            [held[b, :, g * 128 : (g + 1) * 128] + entering[g : g + 1] for g in range(8)], axis=1
        )
        turned_states = jnp.concatenate(
            [(whole * fwd_p[...]).astype(BF16), (whole * fwd_q[...]).astype(BF16)], axis=1
        )
        read = lax.dot_general(
            turned_states, out_map[...], (((1,), (1,)), ((), ())), preferred_element_type=F32
        )
        read = read * jnp.exp(decay[b]) + skip_ref[pl.ds(y, 1), :] * driven_in[b].astype(F32)
        inner = math.sqrt(2.0 / math.pi) * (read + 0.044715 * (read * read * read))
        scan_own[b] = (0.5 * read * (1.0 + jnp.tanh(inner))).astype(BF16)
        carry = falls[b] * turned(gain_block, carry) + ends[b]

    for dx in (2, 1, 3, 0):
        for dy in (2, 1, 3, 0):
            if (dx, dy) != (0, 0):
                send(
                    remote(
                        scan_own.at[(y + dy) % NY], scan_in.at[dx, :, column], s_of["scan"],
                        r_of["scan"], {"fs": (x + dx) % NX, "sp_1": (y + dy) % NY},
                    )
                )
    scan_in[0, :, column] = scan_own[y]
    arrive(3, (0,))
    attend_far(1, right_in.at[0])
    join(0, 1)
    arrive(3, (1,))
    attend_far(7, left_in.at[0])
    arrive(3, (2,))
    attend_far(2, right_in.at[1])
    join(0, 2)
    arrive(3, (3,))
    attend_far(6, left_in.at[1])
    attend_step(3)

    join(0, 3)
    for dz in (6, 7):
        join(5, dz)
    other = pl.ds(pl.multiple_of((1 - t) * 64, 64), 64)
    await_all("scan", drive_w.at[:1920])
    for dx in order:
        scan_product[dx] = jnp.dot(scan_in[dx], w_scan[...], preferred_element_type=F32)
        pre_out[dx] = scan_product[dx, other, :].astype(BF16)
        send(remote(pre_out.at[dx], pre_in.at[dx], s_of["pre"], r_of["pre"], sibling))
    arrive(4)
    attend_far(4, far_in)
    for dz in (4, 5):
        join(0, dz)
    attend_own[...] = acc[0].astype(BF16).reshape(NY, 128, 128)
    for dy in (2, 1, 3):
        send(
            remote(
                attend_own.at[(y + dy) % NY], attend_in.at[:, column], s_of["attend"],
                r_of["attend"], {"sp_1": (y + dy) % NY},
            )
        )
    attend_in[:, column] = attend_own[y]
    await_all("pre", pre_in)
    for dx in (2, 1, 3):
        part_out[dx] = (scan_product[dx, mine, :] + pre_in[dx].astype(F32)).astype(BF16)
        send(
            remote(
                part_out.at[dx], part_in.at[dx], s_of["part"], r_of["part"],
                {"fs": (x + NX - dx) % NX},
            )
        )
    await_all("hop", w_attend.at[0, :384])
    await_all("attend", drive_w.at[:384])
    for k in range(NX):
        product_own[k] = jnp.dot(attend_in[...], w_attend[k], preferred_element_type=F32)
        half_out[k] = product_own[k, other, :].astype(BF16)
        send(remote(half_out.at[k], half_in.at[k], s_of["last"], r_of["last"], sibling))
    await_all("last", half_in)
    await_all("part", w_attend.at[0, :192])
    for dx in order:
        k = (x + dx) % NX
        columns = pl.ds(pl.multiple_of(k * 512, 512), 512)
        scan_part = scan_product[0, mine, :] + pre_in[0].astype(F32)
        if dx:
            scan_part = part_in[dx].astype(F32)
        out[:, columns] = (product_own[k, mine, :] + half_in[k].astype(F32) + scan_part).astype(BF16)
    for name, data in {
        "rows": rows_in.at[:2, :64],
        "half": rows_in.at[:2],
        "keyed": keyed_w.at[:1280],
        "values": drive_w.at[:448],
        "far_rows": rows_in.at[3, :64],
        "query": query_w.at[:1536],
        "packed": packed_in.at[:3],
        "right": w_attend.at[:2, :448],
        "left": w_attend.at[:2, :448],
        "offset": offset_in.at[:7],
        "state": state_in.at[:7],
        "scan": drive_w.at[:1920],
        "pre": pre_in,
        "part": w_attend.at[0, :192],
        "slice": w_attend.at[0, :384],
        "relay": w_attend.at[:3, :256],
        "hop": w_attend.at[0, :384],
        "attend": drive_w.at[:384],
        "last": half_in,
        "drive": drive_w.at[:256],
        "share": drive_w.at[:1344],
    }.items():
        remote(data, data, s_of[name], r_rows.at[0], sibling).wait_send()


def layer(*operands):
    return pl.pallas_call(
        layer_kernel,
        out_shape=pltpu.VMEM((64, 2048), BF16),
        in_specs=[pl.BlockSpec(memory_space=pl.ANY)] * 17,
        out_specs=VMEM,
        scratch_shapes=[
            *(
                pltpu.VMEM((NX, 512, 512) if k == 15 else operand.shape, operand.dtype)
                for k, operand in enumerate(operands)
            ),
            pltpu.SemaphoreType.DMA((17,)),
            pltpu.VMEM((64, 2048), BF16),
            pltpu.VMEM((NY, 128, 2048), BF16),
            pltpu.VMEM((2048, 256), BF16),
            pltpu.VMEM((2048, 128), BF16),
            pltpu.VMEM((2048, 128), BF16),
            pltpu.VMEM((NY, 16, 128), F32),
            pltpu.VMEM((NY, 16, 128), F32),
            pltpu.VMEM((NY, 128, 128), BF16),
            pltpu.VMEM((NY, 128, 128), BF16),
            pltpu.VMEM((NY, 128, 256), BF16),
            pltpu.VMEM((3, NY, 128, 256), BF16),
            pltpu.VMEM((3, NY, 128, 256), BF16),
            pltpu.VMEM((NY, 128, 256), BF16),
            pltpu.VMEM((8, 128), F32),
            pltpu.VMEM((NZ, 8, 128), F32),
            pltpu.VMEM((16, 128), F32),
            pltpu.VMEM((NZ, 16, 128), F32),
            pltpu.VMEM((NZ, 512, 128), F32),
            pltpu.VMEM((NZ, 512, 128), F32),
            pltpu.VMEM((256, 512), BF16),
            pltpu.VMEM((256, 2048), BF16),
            pltpu.VMEM((128, 2048), BF16),
            pltpu.VMEM((128, 1024), F32),
            pltpu.VMEM((128, 1024), F32),
            pltpu.VMEM((128, 1024), F32),
            pltpu.VMEM((128, 1024), F32),
            pltpu.VMEM((NY, 128, 1024), F32),
            pltpu.VMEM((NY, 8, 128), F32),
            pltpu.VMEM((NY, 128, 128), F32),
            pltpu.VMEM((NY, 128, 128), BF16),
            pltpu.VMEM((NY, 128, 128), BF16),
            pltpu.VMEM((128, 512), BF16),
            pltpu.VMEM((NX, 128, 512), BF16),
            pltpu.VMEM((NX, 64, 512), BF16),
            pltpu.VMEM((NX, 64, 512), BF16),
            pltpu.VMEM((NX, 128, 512), F32),
            pltpu.VMEM((NX, 64, 512), BF16),
            pltpu.VMEM((NX, 64, 512), BF16),
            pltpu.VMEM((NX, 128, 512), F32),
            pltpu.VMEM((NX, 64, 512), BF16),
            pltpu.VMEM((NX, 64, 512), BF16),
            *(
                pltpu.SemaphoreType.DMA(shape)
                for shape in (
                    (len(SENT),), (len(TOGETHER),), (4,), (14,), (14,), (3,), (3, 2), (4,)
                )
            ),
        ],
        compiler_params=pltpu.CompilerParams(
            collective_id=0, has_side_effects=True, vmem_limit_bytes=60 << 20
        ),
        name="layer",
    )(*operands)


def on_device(
    tokens, norm_gain, drive_weight, query_weight, key_weight, value_weight, key_offset, log_step,
    lambda_real, lambda_imag, input_map, output_map, skip_gain, forget, initial_state,
    scan_out_weight, attend_out_weight,
):
    return layer(
        tokens[0],
        norm_gain[None],
        drive_weight,
        query_weight,
        key_weight,
        value_weight,
        key_offset[:, 0, :],
        log_step[None],
        lambda_real,
        lambda_imag,
        input_map.transpose(0, 1, 3, 2),
        output_map,
        skip_gain.reshape(NY, 128),
        forget.reshape(NY, 8, 128),
        initial_state[:, 0],
        attend_out_weight,
        scan_out_weight,
    )[None]


def solution(mesh):
    split = Mesh(
        mesh.devices.reshape(NZ, NY, mesh.shape["fs"], mesh.shape["tp"]),
        ("sp_0", "sp_1", "fs", "tp"),
    )
    in_specs = (
        P("fs", SP_TP, None),
        P(),
        P("fs", "tp"),
        P("fs", "tp"),
        P("fs", "tp"),
        P("fs", "tp"),
        P("tp", "fs", SP),
        P("tp"),
        P("tp", None),
        P("tp", None),
        P(None, "tp", None, None),
        P(None, "tp", None, None),
        P("tp"),
        P("tp", "fs", SP),
        P(None, "fs", "tp", None),
        P("tp", "fs"),
        P("tp", "fs"),
    )
    return jax.shard_map(
        on_device, mesh=split, in_specs=in_specs, out_specs=P("fs", SP_TP, None), check_vma=False
    )
```
